256 devices in a mesh: sp: 32 (over z, x), tp: 8 (over y, core).
Axes of the slice: x: 4, y: 4, z: 8, core: 2. Of those that a mesh axis runs over, the one named last changes fastest.
Arguments:
- tokens: bfloat16 [16384, 2048], P(('sp', 'tp')), may hold values from -6 to 6
- norm_gain: float32 [2048], replicated, may hold values from 0.1 to 1.9
- w_query: bfloat16 [2048, 1024], P(None, 'tp'), may hold values from -16 to 16
- w_key: bfloat16 [2048, 1024], P(None, 'tp'), may hold values from -16 to 16
- w_value: bfloat16 [2048, 1024], P(None, 'tp'), may hold values from -0.125 to 0.125
- conv_in: bfloat16 [2048, 2048], P(None, 'tp'), may hold values from -0.125 to 0.125
- conv_gate: bfloat16 [2048, 2048], P(None, 'tp'), may hold values from -0.125 to 0.125
- conv_taps: float32 [31, 2048], P(None, 'tp'), may hold values from -3.7 to 3.7
- conv_gain: float32 [2048], P('tp'), may hold values from 0.1 to 1.9
- cum_gate: float32 [16, 16384], P('tp'), may hold values from -2050 to 0, as said below
- out_attn: bfloat16 [1024, 2048], P('tp'), may hold values from -0.75 to 0.75
- out_conv: bfloat16 [2048, 2048], P('tp'), may hold values from -0.125 to 0.125
Outputs:
- mixed: bfloat16 [16384, 2048], P(('sp', 'tp'))
- log_total: float32 [16, 16384], P('tp', 'sp')
The draws below stay inside these ranges and needn't reach their ends.
Inputs may be any that keep to these rules, and one draw needn't show every extreme that they name: `cum_gate`: for each head the values never rise from one position to the next and are at most 0.
All inputs are finite; a program needn't handle non-finite values.
Results may differ from the reference program's by a relative error of at most 0.014.
Values may be sent and summed in bfloat16 or wider, within the bound.
A program may use at most 128 MiB of HBM per device.

```python
import math
import jax
import jax.numpy as jnp
from jax import lax

D = 2048
HEAD_COUNT = 16
HEAD = 64
KERNEL = 31
TOK_DEV = 512
TOKEN_COUNT = 16384
ATT_WIDTH = 1024
CONV = 2048
N_SP = 32
N_TP = 8


def query_key_pair(key):
    random_split_keys = jax.random.split(jax.random.fold_in(key, 11), 3)
    fan_scale = D ** (-0.5)
    key_weight = jnp.clip(jax.random.normal(random_split_keys[0], (D, HEAD_COUNT * HEAD), jnp.float32), -6.0, 6.0) * fan_scale
    query_weight = jnp.clip(jax.random.normal(random_split_keys[2], (D, HEAD_COUNT * HEAD), jnp.float32), -6.0, 6.0) * (2.25 * fan_scale)
    return (query_weight, key_weight)


def draw_w_query(key, part):
    return query_key_pair(key)[0].astype(jnp.bfloat16)


def draw_w_key(key, part):
    return query_key_pair(key)[1].astype(jnp.bfloat16)


def draw_conv_taps(key, part):
    random_split_keys = jax.random.split(jax.random.fold_in(key, 23), 1)
    sequence_positions = jnp.arange(CONV, dtype=jnp.float32) / (CONV - 1)
    raw_taps = jnp.clip(jax.random.normal(random_split_keys[0], (KERNEL, CONV), jnp.float32), -4.0, 4.0)
    channel_ramp = 10.0 ** (sequence_positions - 0.5)
    return raw_taps * KERNEL ** (-0.5) * channel_ramp[None, :]


def draw_cum_gate(key, part):
    random_split_keys = jax.random.split(jax.random.fold_in(key, 37), 7)
    head_order = jax.random.permutation(random_split_keys[0], HEAD_COUNT)
    slow_count = HEAD_COUNT // 2
    slow_heads = (head_order < slow_count)[:, None]
    slow_total = jax.random.uniform(random_split_keys[1], (HEAD_COUNT, 1), jnp.float32, 0.5, 1.0)
    fast_rate = 1.0 / jax.random.uniform(random_split_keys[2], (HEAD_COUNT, 1), jnp.float32, 30.0, 100.0)
    baseline_forget_rate = jnp.where(slow_heads, slow_total / TOKEN_COUNT, fast_rate)
    block_multiplier = jnp.exp(jax.random.uniform(random_split_keys[3], (HEAD_COUNT, N_SP), jnp.float32, math.log(0.5), math.log(2.0)))
    block_multiplier = jnp.repeat(block_multiplier, TOK_DEV, axis=1)
    roughness_multiplier = jax.random.uniform(random_split_keys[4], (HEAD_COUNT, TOKEN_COUNT), jnp.float32, 0.2, 1.8)
    spike_location = jax.random.randint(random_split_keys[5], (HEAD_COUNT, 2), 0, TOKEN_COUNT)
    spike_penalty = -jnp.log(jax.random.uniform(random_split_keys[6], (HEAD_COUNT, 2), jnp.float32, 0.6, 0.8))
    sequence_positions = jnp.arange(TOKEN_COUNT, dtype=jnp.int32)
    spike_events = jnp.sum(jnp.where(sequence_positions[None, None, :] == spike_location[:, :, None], spike_penalty[:, :, None], 0.0), axis=1)
    forget_rate_grid = baseline_forget_rate * block_multiplier * roughness_multiplier + spike_events
    return -jnp.cumsum(forget_rate_grid, axis=1)


def shard_levels(rng, dims, cuts, low, largest):
    gain = 1.0
    for axis_at, shards_of in cuts:
        draws = jax.random.uniform(jax.random.fold_in(jax.random.fold_in(rng, 6), axis_at), (shards_of,), jnp.float32, low / len(cuts), largest / len(cuts))
        gain = gain * jnp.repeat(jnp.exp(draws), dims[axis_at] // shards_of).reshape((-1,) + (1,) * (len(dims) - 1 - axis_at))
    return gain


def centred(key, dims, scale, bound, cuts=(), kind=jnp.bfloat16):
    drawn = scale * jax.random.normal(key, dims, jnp.float32)
    if cuts:
        drawn = drawn * shard_levels(key, dims, cuts, -0.22, 0.18)
    return jnp.clip(drawn, -bound, bound).astype(kind)


def setup_inputs(seed: int = 0) -> dict:
    seeds = jax.random.split(jax.random.key(seed), 13)
    tokens = centred(seeds[0], (TOKEN_COUNT, D), 1.0, 6.0, ((0, 256),))
    norm_gain = jnp.clip(1.0 + 0.18 * jax.random.normal(seeds[1], (D,), jnp.float32), 0.1, 1.9)
    w_query = draw_w_query(jax.random.fold_in(seeds[12], 71), 0)
    w_key = draw_w_key(jax.random.fold_in(seeds[12], 71), 0)
    w_value = centred(seeds[4], (D, ATT_WIDTH), D ** -0.5, 0.125, ((1, 8),))
    conv_in = centred(seeds[5], (D, CONV), D ** -0.5, 0.125, ((1, 8),))
    conv_gate = centred(seeds[6], (D, CONV), D ** -0.5, 0.125, ((1, 8),))
    conv_taps = draw_conv_taps(jax.random.fold_in(seeds[12], 71), 0)
    conv_gain = jnp.clip(1.0 + 0.18 * jax.random.normal(seeds[8], (CONV,), jnp.float32), 0.1, 1.9)
    cum_gate = draw_cum_gate(jax.random.fold_in(seeds[12], 71), 0)
    out_attn = centred(seeds[10], (ATT_WIDTH, D), (ATT_WIDTH // 16) ** -0.5, 0.75, ((0, 8),))
    out_conv = centred(seeds[11], (CONV, D), CONV ** -0.5, 0.125, ((0, 8),))
    return dict(tokens=tokens, norm_gain=norm_gain, w_query=w_query, w_key=w_key, w_value=w_value, conv_in=conv_in, conv_gate=conv_gate, conv_taps=conv_taps, conv_gain=conv_gain, cum_gate=cum_gate, out_attn=out_attn, out_conv=out_conv)


def by_heads(matrix):
    return matrix.reshape(TOKEN_COUNT, HEAD_COUNT, HEAD).transpose(1, 0, 2)

def head_attention(operands):
    query_head, key_head, value_head, cum_head = operands
    key_place = jnp.arange(TOKEN_COUNT, dtype=jnp.int32)

    def one_block(block_index):
        begin_row = (block_index * TOK_DEV).astype(jnp.int32)
        query_block = lax.dynamic_slice_in_dim(query_head, begin_row, TOK_DEV, 0)
        cum_block = lax.dynamic_slice_in_dim(cum_head, begin_row, TOK_DEV, 0)
        query_place = begin_row + jnp.arange(TOK_DEV, dtype=jnp.int32)
        scores = jnp.dot(query_block, key_head.T, preferred_element_type=jnp.float32)
        scores = scores + cum_block[:, None] - cum_head[None, :]
        visible = key_place[None, :] <= query_place[:, None]
        scores = jnp.where(visible, scores, -1e+30)
        row_max = lax.optimization_barrier(jnp.max(scores, axis=1))
        weights = jnp.where(visible, jnp.exp(scores - row_max[:, None]), 0.0)
        row_sum = lax.optimization_barrier(jnp.sum(weights, axis=1))
        result = jnp.dot(weights.astype(jnp.bfloat16), value_head, preferred_element_type=jnp.float32)
        result = (result / row_sum[:, None]).astype(jnp.bfloat16)
        return (result, row_max + jnp.log(row_sum))
    blocks_out, totals = lax.map(one_block, jnp.arange(N_SP, dtype=jnp.int32))
    return (blocks_out.reshape(TOKEN_COUNT, HEAD), totals.reshape(TOKEN_COUNT))

def reference(tokens, norm_gain, w_query, w_key, w_value, conv_in, conv_gate, conv_taps, conv_gain, cum_gate, out_attn, out_conv):
    wide = tokens.astype(jnp.float32)
    normed = (wide * lax.rsqrt(lax.optimization_barrier(jnp.mean(wide * wide, axis=1, keepdims=True)) + 1e-06) * norm_gain[None, :]).astype(jnp.bfloat16)
    query = (jnp.dot(normed, w_query, preferred_element_type=jnp.float32) * HEAD ** (-0.5)).astype(jnp.bfloat16)
    keyed = jnp.dot(normed, w_key, preferred_element_type=jnp.float32).astype(jnp.bfloat16)
    valued = jnp.dot(normed, w_value, preferred_element_type=jnp.float32).astype(jnp.bfloat16)
    attended, log_total = lax.map(head_attention, (by_heads(query), by_heads(keyed), by_heads(valued), cum_gate))
    attended = attended.transpose(1, 0, 2).reshape(TOKEN_COUNT, ATT_WIDTH)
    opened = jnp.dot(normed, conv_in, preferred_element_type=jnp.float32)
    gating = jnp.dot(normed, conv_gate, preferred_element_type=jnp.float32)
    gated = (opened * jax.nn.sigmoid(gating)).astype(jnp.bfloat16)
    padded = jnp.concatenate([jnp.zeros((KERNEL - 1, CONV), jnp.bfloat16), gated], axis=0).astype(jnp.float32)
    convolved = jnp.zeros((TOKEN_COUNT, CONV), jnp.float32)
    for tap_index in range(KERNEL):
        convolved = convolved + conv_taps[tap_index][None, :] * padded[tap_index:tap_index + TOKEN_COUNT]
    channel_square = lax.optimization_barrier(jnp.mean(convolved * convolved, axis=1, keepdims=True))
    conv_out = jax.nn.silu(convolved * lax.rsqrt(channel_square + 1e-06) * conv_gain[None, :]).astype(jnp.bfloat16)
    group_att = ATT_WIDTH // N_TP
    group_conv = CONV // N_TP
    mixed = jnp.zeros((TOKEN_COUNT, D), jnp.float32)
    for group in range(N_TP):
        group_part = jnp.dot(attended[:, group * group_att:(group + 1) * group_att], out_attn[group * group_att:(group + 1) * group_att], preferred_element_type=jnp.float32)
        group_part = group_part + jnp.dot(conv_out[:, group * group_conv:(group + 1) * group_conv], out_conv[group * group_conv:(group + 1) * group_conv], preferred_element_type=jnp.float32)
        group_part = lax.optimization_barrier(group_part.astype(jnp.bfloat16)).astype(jnp.float32)
        mixed = mixed + group_part
    return (mixed.astype(jnp.bfloat16), log_total)
```

```python
import functools

import jax
import jax.numpy as jnp
from jax import lax
from jax.experimental import pallas as pl
from jax.experimental.pallas import tpu as pltpu
from jax.sharding import PartitionSpec as P

MESH = pl.DeviceIdType.MESH
F32 = jnp.float32
BF16 = jnp.bfloat16
HEAD = 64
NX = 4
NY = 4
LOW = -1e30
LOG2E = 1.4426950408889634
VROWS = 80


def kernel(
    tokens,
    norm_gain,
    w_query,
    w_key,
    w_value,
    conv_in,
    conv_gate,
    conv_taps,
    conv_gain,
    cum_gate,
    out_attn,
    out_conv,
    mixed,
    log_total,
    nt,
    wall,
    wout,
    qp,
    ks,
    vs,
    kp,
    vp,
    cpad,
    mrow,
    acc,
    obuf,
    orecv,
    sbuf,
    srecv,
    gb,
    rim,
    cg,
    cv,
    sq,
    csq,
    xs,
    sb,
    rb,
    po,
    t2,
    r2r,
    r2l,
    sr,
    sl,
    frl,
    frr,
    wsem,
    gsend,
    grecv,
    ksend,
    krecv,
    vsend,
    vrecv,
    qsend,
    qrecv,
    msend,
    mrecv,
    osend,
    orecv_sem,
    csend,
    crecv,
    xsend,
    xrecv,
):
    s_me = lax.axis_index("sp")
    t_me = lax.axis_index("tp")
    nsp = lax.axis_size("sp")
    nz = nsp // NX
    z = s_me // NX
    x = s_me % NX
    y = t_me // 2
    c = t_me % 2
    rows = tokens.shape[0]
    half = rows // 2
    depth = tokens.shape[1]
    tok = rows * 8

    def at_tp(t):
        return (s_me, t)

    def at_sp(s):
        return (s, t_me)

    def rcopy(src, dst, ssem, rsem, dev):
        return pltpu.make_async_remote_copy(
            src_ref=src,
            dst_ref=dst,
            send_sem=ssem,
            recv_sem=rsem,
            device_id=dev,
            device_id_type=MESH,
        )

    wcopies = []
    at = 0
    for i, w in enumerate((w_query, w_key, w_value, conv_in, conv_gate)):
        n = w.shape[1]
        wcopies.append(pltpu.make_async_copy(w, wall.at[:, pl.ds(at, n)], wsem.at[i]))
        at += n
    at = 0
    ocopies = []
    for i, w in enumerate((out_attn, out_conv)):
        n = w.shape[0]
        ocopies.append(pltpu.make_async_copy(w, wout.at[pl.ds(at, n), :], wsem.at[5 + i]))
        at += n
    for w in wcopies + ocopies:
        w.start()

    barrier = pltpu.get_barrier_semaphore()
    for d in range(1, 8):
        pl.semaphore_signal(
            barrier, inc=1, device_id=at_tp((t_me + d) % 8), device_id_type=MESH
        )
    for d in range(1, NX):
        pl.semaphore_signal(
            barrier, inc=1, device_id=at_sp(z * NX + (x + d) % NX), device_id_type=MESH
        )
    for d in (1, nz - 1):
        pl.semaphore_signal(
            barrier, inc=1, device_id=at_sp(((z + d) % nz) * NX + x), device_id_type=MESH
        )
    for d in (1, nsp - 1):
        pl.semaphore_signal(
            barrier, inc=1, device_id=at_sp((s_me + d) % nsp), device_id_type=MESH
        )

    wide = tokens[...].astype(F32)
    factor = lax.rsqrt(jnp.mean(wide * wide, axis=1, keepdims=True) + 1e-06)
    nt[t_me] = (wide * factor * norm_gain[...]).astype(BF16)
    qp[:, 0, HEAD:, :] = jnp.ones((NX, HEAD, tok), BF16)
    qp[:, 1, :HEAD, :] = jnp.ones((NX, HEAD, tok), BF16)
    vp[:, HEAD:, :] = jnp.ones((2, VROWS - HEAD, tok), BF16)
    cpad[...] = jnp.zeros_like(cpad)
    mrow[...] = jnp.full_like(mrow, LOW)
    acc[...] = jnp.zeros_like(acc)

    pl.semaphore_wait(barrier, 7 + NX - 1 + 4)

    sib = y * 2 + (1 - c)
    tr = ((y + 1) % NY) * 2 + c
    tl = ((y + NY - 1) % NY) * 2 + c
    to = ((y + 2) % NY) * 2 + c
    lo, hi = pl.ds(0, half), pl.ds(half, half)

    def gcopy(k, src, part, dev):
        ref = nt.at[src] if part is None else nt.at[src, part]
        return rcopy(ref, ref, gsend.at[k], grecv.at[k], at_tp(dev))

    g = [
        gcopy(0, t_me, None, sib),
        gcopy(1, t_me, lo, tr),
        gcopy(2, t_me, hi, tr),
        gcopy(3, t_me, hi, tl),
        gcopy(4, t_me, lo, tl),
        gcopy(5, tl, None, sib),
        gcopy(6, tr, None, sib),
        gcopy(7, tl, lo, tr),
        gcopy(8, tr, hi, tl),
        gcopy(9, to, lo, sib),
        gcopy(10, to, hi, sib),
    ]
    for k in (1, 3, 2, 4, 0):
        g[k].start()
    for w in wcopies:
        w.wait()

    def project(i, carry):
        @pl.when(i == 0)
        def _():
            g[0].wait_recv()

        @pl.when(i == 1)
        def _():
            g[1].wait_recv()
            g[7].start()
            g[3].wait_recv()
            g[8].start()
            g[2].wait_recv()
            g[5].start()
            g[4].wait_recv()
            g[6].start()
            g[5].wait_recv()

        @pl.when(i == 2)
        def _():
            g[6].wait_recv()

        @pl.when(i == 3)
        def _():
            g[7].wait_recv()
            g[9].start()
            g[8].wait_recv()
            g[10].start()
            g[9].wait_recv()
            g[10].wait_recv()

        p = (y + 2 * NY - (2 * (i % 2) - 1) * ((i + 1) // 2)) % NY
        lhs = nt[pl.ds(2 * p, 2)].reshape(2 * rows, depth)
        res = jnp.dot(lhs, wall[...], preferred_element_type=F32)
        here = pl.ds(pl.multiple_of(p * 2 * rows, 2 * rows), 2 * rows)
        qt = (res[:, :128] * HEAD ** (-0.5)).T.astype(BF16)
        qp[x, 0, :HEAD, here] = qt[:HEAD]
        qp[x, 1, HEAD:, here] = qt[HEAD:]
        ks[z, here, :] = res[:, 128:256].astype(BF16)
        vs[z, :, here] = res[:, 256:384].T.astype(BF16)
        opened = res[:, 384:640]
        gating = res[:, 640:896]
        gate = (opened / (1.0 + jnp.exp(-gating))).astype(BF16)
        gb[here, :] = gate
        cg[pl.ds(pl.multiple_of(p * 2 * rows + 32, 32), 2 * rows), :] = gate.astype(F32)
        return carry

    lax.fori_loop(0, NY, project, 0)

    def sp_of(zz):
        return at_sp(zz * NX + x)

    def kcopy(zb, t, zt):
        return rcopy(ks.at[zb], ks.at[zb], ksend.at[t], krecv.at[t], sp_of(zt))

    def vcopy(zb, t, zt):
        return rcopy(vs.at[zb], vs.at[zb], vsend.at[t], vrecv.at[t], sp_of(zt))

    for t, zt in ((1, (z + 1) % nz), (2, (z + nz - 1) % nz)):
        kcopy(z, t, zt).start()
        vcopy(z, t, zt).start()

    def qcopies(src, d):
        dev = at_sp(z * NX + (x + d) % NX)
        a = qp.at[src, 0, pl.ds(0, HEAD)]
        b = qp.at[src, 1, pl.ds(HEAD, HEAD)]
        return (
            rcopy(a, a, qsend.at[2 * d - 2], qrecv.at[2 * d - 2], dev),
            rcopy(b, b, qsend.at[2 * d - 1], qrecv.at[2 * d - 1], dev),
        )

    for d in (1, 3, 2):
        for q in qcopies(x, d):
            q.start()
    rcopy_rim = rcopy(
        gb.at[pl.ds(tok - 32, 32)], rim, msend.at[0], mrecv.at[0], at_sp((s_me + 1) % nsp)
    )
    rcopy_rim.start()

    rcopy_rim.wait_recv()
    first = jnp.where(s_me > 0, 1.0, 0.0).astype(F32)
    cg[0:32, :] = rim[...].astype(F32) * first

    def conv_rows(i, carry):
        r0 = pl.multiple_of(i * 64, 64)
        win = cg[pl.ds(r0, 96), :]
        total = jnp.zeros((64, win.shape[1]), F32)
        for b in range(8):
            turned = win if b == 0 else pltpu.roll(win, 96 - b, 0)
            for a in range(5):
                k = 8 * a + b - 2
                if 0 <= k < 31:
                    total = total + conv_taps[k : k + 1, :] * turned[8 * a : 8 * a + 64]
        cv[pl.ds(r0, 64), :] = total
        square = total * total
        sq[pl.ds(r0, 64), :] = square[:, :128] + square[:, 128:]
        return carry

    lax.fori_loop(0, tok // 64, conv_rows, 0)
    part = jnp.sum(sq[...].T, axis=0, keepdims=True)
    csq[t_me] = jnp.broadcast_to(part, (8, tok))
    ccopies = []
    for d in range(1, 8):
        cc = rcopy(
            csq.at[t_me], csq.at[t_me], csend.at[d], crecv.at[d], at_tp((t_me + d) % 8)
        )
        cc.start()
        ccopies.append(cc)

    cref = cum_gate[:, pl.ds(pl.multiple_of(z * NX * tok, 128), 128)][:, :1]

    def prepare(zb):
        ck = cum_gate[:, pl.ds(pl.multiple_of((zb * NX + x) * tok, 128), tok)]
        bias = cref - ck
        high = bias.astype(BF16).astype(F32)
        left = bias - high
        mid = left.astype(BF16).astype(F32)
        low = left - mid
        rowid = lax.broadcasted_iota(jnp.int32, (8, tok), 0)
        for h, r0 in ((0, HEAD), (1, 0)):
            tile = jnp.where(
                rowid == 0,
                high[h : h + 1],
                jnp.where(
                    rowid == 1, mid[h : h + 1], jnp.where(rowid == 2, low[h : h + 1], 0.0)
                ),
            )
            cpad[r0 : r0 + 8, :] = tile
        extra = cpad[...].T
        kf = ks[zb].astype(F32)
        lane = lax.broadcasted_iota(jnp.int32, (tok, 2 * HEAD), 1)
        kp[0] = jnp.where(lane < HEAD, kf, extra).astype(BF16)
        kp[1] = jnp.where(lane < HEAD, extra, kf).astype(BF16)
        vp[0, :HEAD, :] = vs[zb, :HEAD, :]
        vp[1, :HEAD, :] = vs[zb, HEAD:, :]

    def chunk(j, masked):
        for h in range(2):
            sc = jnp.dot(kp[h], qp[j, h], preferred_element_type=F32)
            if masked:
                kpos = lax.broadcasted_iota(jnp.int32, sc.shape, 0)
                qpos = lax.broadcasted_iota(jnp.int32, sc.shape, 1)
                sc = jnp.where(kpos <= qpos, sc, LOW)
            old = mrow[j, h]
            new = jnp.maximum(old, jnp.max(sc, axis=0, keepdims=True))
            wts = jnp.exp2((sc - new) * LOG2E).astype(BF16)
            shrink = jnp.exp2((old - new) * LOG2E)
            mrow[j, h] = new
            acc[j, h] = acc[j, h] * shrink + jnp.dot(vp[h], wts, preferred_element_type=F32)

    def full(j, carry):
        chunk(j, False)
        return carry

    prepare(z)
    chunk(x, True)
    for d in range(1, NX):
        for q in qcopies((x + NX - d) % NX, d):
            q.wait_recv()
    lax.fori_loop(x + 1, NX, full, 0)

    def arrival(t, carry):
        dr = 2 * (t % 2) - 1
        zb = (z + nz - dr * ((t + 1) // 2)) % nz
        zt = (z + nz + dr) % nz
        kcopy(zb, t, zt).wait_recv()

        @pl.when(t <= 5)
        def _():
            kcopy(zb, t + 2, zt).start()

        vcopy(zb, t, zt).wait_recv()

        @pl.when((t <= 4) | (t == 6))
        def _():
            vcopy(zb, t + 2 - t // 6, zt).start()

        @pl.when(zb < z)
        def _():
            prepare(zb)
            lax.fori_loop(0, NX, full, 0)

        return carry

    lax.fori_loop(1, nz, arrival, 0)

    xcopies = []
    for d in (1, 3, 2):
        j = (x + d) % NX
        for h in range(2):
            obuf[d - 1, h * HEAD : (h + 1) * HEAD, :] = acc[j, h, :HEAD, :].astype(BF16)
            sbuf[d - 1, h : h + 1, :] = mrow[j, h]
            sbuf[d - 1, 2 + h : 3 + h, :] = acc[j, h, HEAD : HEAD + 1, :]
        dev = at_sp(z * NX + j)
        oc = rcopy(
            obuf.at[d - 1], orecv.at[d - 1], osend.at[2 * d - 2], orecv_sem.at[2 * d - 2], dev
        )
        st = rcopy(
            sbuf.at[d - 1], srecv.at[d - 1], osend.at[2 * d - 1], orecv_sem.at[2 * d - 1], dev
        )
        st.start()
        oc.start()
        xcopies += [oc, st]

    for cc in ccopies:
        cc.wait_recv()
    total = csq[0, 0:1, :]
    for t in range(1, 8):
        total = total + csq[t, 0:1, :]
    scale = lax.rsqrt(total / (8.0 * conv_gain.shape[1]) + 1e-06)
    sq[...] = jnp.broadcast_to(scale, (128, tok)).T
    for i in range(8):
        r = pl.ds(i * rows, rows)
        factor = sq[r, :]
        for b in range(2):
            lanes = pl.ds(b * 128, 128)
            v = cv[r, lanes] * factor * conv_gain[:, lanes]
            v = v / (1.0 + jnp.exp(-v))
            xs[i % 2, i // 2, :, pl.ds(128 + b * 128, 128)] = v.astype(BF16)
    for w in ocopies:
        w.wait()

    for cp in xcopies:
        cp.wait_recv()
    offset = pl.multiple_of(s_me * tok, 128)
    for h in range(2):
        best = mrow[x, h]
        for d in range(1, NX):
            best = jnp.maximum(best, srecv[d - 1, h : h + 1, :])
        share = jnp.exp2((mrow[x, h] - best) * LOG2E)
        summed = acc[x, h, HEAD : HEAD + 1, :] * share
        value = acc[x, h, :HEAD, :] * share
        for d in range(1, NX):
            share = jnp.exp2((srecv[d - 1, h : h + 1, :] - best) * LOG2E)
            summed = summed + srecv[d - 1, 2 + h : 3 + h, :] * share
            value = value + orecv[d - 1, h * HEAD : (h + 1) * HEAD, :].astype(F32) * share
        own = cum_gate[:, pl.ds(offset, tok)][h : h + 1] - cref[h : h + 1]
        log_total[h : h + 1, :] = best + jnp.log(summed) + own
        cpad[h * HEAD : (h + 1) * HEAD, :] = value / summed
    att = cpad[...].T.astype(BF16)
    for i in range(8):
        xs[i % 2, i // 2, :, 0:128] = att[i * rows : (i + 1) * rows]

    def project_out(which, emit):
        lhs = xs[which].reshape(NY * rows, 384)

        def columns(n, carry):
            cols = pl.ds(pl.multiple_of(n * 512, 512), 512)
            res = jnp.dot(lhs, wout[:, cols], preferred_element_type=F32)
            emit(cols, res)
            return carry

        lax.fori_loop(0, depth // 512, columns, 0)

    def emit_sib(cols, res):
        sb[:, :, cols] = res.astype(BF16).reshape(NY, rows, 512)

    def emit_own(cols, res):
        po[:, :, cols] = res.reshape(NY, rows, 512)

    project_out(1 - c, emit_sib)
    ybits = [(y + k) % NY for k in range(NY)]

    def xcopy(k, src, dst, dev):
        return rcopy(src, dst, xsend.at[k], xrecv.at[k], at_tp(dev))

    bcopies = [xcopy(k, sb.at[ybits[k]], rb.at[ybits[k]], sib) for k in range(NY)]
    for k in (2, 1, 3, 0):
        bcopies[k].start()
    project_out(c, emit_own)

    bcopies[2].wait_recv()
    t2[...] = (po[ybits[2]] + rb[ybits[2]].astype(F32)).astype(BF16)
    far_r = xcopy(4, t2.at[lo], r2r, tr)
    far_l = xcopy(5, t2.at[hi], r2l, tl)
    far_r.start()
    far_l.start()
    bcopies[1].wait_recv()
    sr[hi, :] = (po[ybits[1], hi] + rb[ybits[1], hi].astype(F32)).astype(BF16)
    near_r = xcopy(6, sr.at[hi], frl.at[hi], tr)
    near_r.start()
    bcopies[3].wait_recv()
    sl[lo, :] = (po[ybits[3], lo] + rb[ybits[3], lo].astype(F32)).astype(BF16)
    near_l = xcopy(7, sl.at[lo], frr.at[lo], tl)
    near_l.start()
    far_r.wait_recv()
    sr[lo, :] = (po[ybits[1], lo] + rb[ybits[1], lo].astype(F32) + r2r[...].astype(F32)).astype(BF16)
    both_r = xcopy(8, sr.at[lo], frl.at[lo], tr)
    both_r.start()
    far_l.wait_recv()
    sl[hi, :] = (po[ybits[3], hi] + rb[ybits[3], hi].astype(F32) + r2l[...].astype(F32)).astype(BF16)
    both_l = xcopy(9, sl.at[hi], frr.at[hi], tl)
    both_l.start()
    bcopies[0].wait_recv()
    po[ybits[0]] = po[ybits[0]] + rb[ybits[0]].astype(F32)
    near_r.wait_recv()
    near_l.wait_recv()
    both_r.wait_recv()
    both_l.wait_recv()
    mixed[...] = (po[y] + frl[...].astype(F32) + frr[...].astype(F32)).astype(BF16)

    for cp in g:
        cp.wait_send()
    for t in range(1, 8):
        kcopy(z, t, (z + 1) % nz).wait_send()
        vcopy(z, t, (z + 1) % nz).wait_send()
    for d in range(1, NX):
        for q in qcopies(x, d):
            q.wait_send()
    rcopy_rim.wait_send()
    for cp in ccopies + xcopies + bcopies:
        cp.wait_send()
    for cp in (far_r, far_l, near_r, near_l, both_r, both_l):
        cp.wait_send()


def per_device(*args):
    tokens = args[0]
    rows, depth = tokens.shape
    tok = rows * 8
    nz = lax.axis_size("sp") // NX
    att = args[2].shape[1]
    ch = args[5].shape[1]
    wide = 3 * att + 2 * ch
    ops = list(args)
    ops[1] = args[1][None]
    ops[8] = args[8][None]
    vmem = pl.BlockSpec(memory_space=pltpu.VMEM)
    hbm = pl.BlockSpec(memory_space=pltpu.HBM)
    specs = [vmem, vmem, hbm, hbm, hbm, hbm, hbm, vmem, vmem, vmem, hbm, hbm]
    dma = pltpu.SemaphoreType.DMA
    scratch = [
        pltpu.VMEM((8, rows, depth), BF16),
        pltpu.VMEM((depth, wide), BF16),
        pltpu.VMEM((att + ch, depth), BF16),
        pltpu.VMEM((NX, 2, att, tok), BF16),
        pltpu.VMEM((nz, tok, att), BF16),
        pltpu.VMEM((nz, att, tok), BF16),
        pltpu.VMEM((2, tok, att), BF16),
        pltpu.VMEM((2, VROWS, tok), BF16),
        pltpu.VMEM((att, tok), F32),
        pltpu.VMEM((NX, 2, 1, tok), F32),
        pltpu.VMEM((NX, 2, VROWS, tok), F32),
        pltpu.VMEM((NX - 1, att, tok), BF16),
        pltpu.VMEM((NX - 1, att, tok), BF16),
        pltpu.VMEM((NX - 1, 8, tok), F32),
        pltpu.VMEM((NX - 1, 8, tok), F32),
        pltpu.VMEM((tok, ch), BF16),
        pltpu.VMEM((32, ch), BF16),
        pltpu.VMEM((tok + 32, ch), F32),
        pltpu.VMEM((tok, ch), F32),
        pltpu.VMEM((tok, 128), F32),
        pltpu.VMEM((8, 8, tok), F32),
        pltpu.VMEM((2, NY, rows, att + ch), BF16),
        pltpu.VMEM((NY, rows, depth), BF16),
        pltpu.VMEM((NY, rows, depth), BF16),
        pltpu.VMEM((NY, rows, depth), F32),
        pltpu.VMEM((rows, depth), BF16),
        pltpu.VMEM((rows // 2, depth), BF16),
        pltpu.VMEM((rows // 2, depth), BF16),
        pltpu.VMEM((rows, depth), BF16),
        pltpu.VMEM((rows, depth), BF16),
        pltpu.VMEM((rows, depth), BF16),
        pltpu.VMEM((rows, depth), BF16),
        dma((7,)),
        dma((11,)),
        dma((11,)),
        dma((8,)),
        dma((8,)),
        dma((8,)),
        dma((8,)),
        dma((6,)),
        dma((6,)),
        dma((1,)),
        dma((1,)),
        dma((6,)),
        dma((6,)),
        dma((8,)),
        dma((8,)),
        dma((10,)),
        dma((10,)),
    ]
    return pl.pallas_call(
        kernel,
        out_shape=(
            jax.ShapeDtypeStruct((rows, depth), BF16),
            jax.ShapeDtypeStruct((2, tok), F32),
        ),
        in_specs=specs,
        out_specs=(vmem, vmem),
        scratch_shapes=scratch,
        compiler_params=pltpu.CompilerParams(
            collective_id=0, has_side_effects=True, vmem_limit_bytes=60 * 1024 * 1024
        ),
        name="layer",
    )(*ops)


def solution(mesh):
    in_specs = (
        P(("sp", "tp"), None),
        P(),
        P(None, "tp"),
        P(None, "tp"),
        P(None, "tp"),
        P(None, "tp"),
        P(None, "tp"),
        P(None, "tp"),
        P("tp"),
        P("tp", None),
        P("tp", None),
        P("tp", None),
    )
    out_specs = (P(("sp", "tp"), None), P("tp", "sp"))
    return jax.shard_map(
        per_device, mesh=mesh, in_specs=in_specs, out_specs=out_specs, check_vma=False
    )
```

```python
import functools

import jax
import jax.numpy as jnp
from jax import lax
from jax.experimental import pallas as pl
from jax.experimental.pallas import tpu as pltpu
from jax.sharding import PartitionSpec as P

MESH = pl.DeviceIdType.MESH
F32 = jnp.float32
BF16 = jnp.bfloat16
HEAD = 64
NX = 4
NY = 4
LOW = -1e30
LOG2E = 1.4426950408889634
VROWS = 80
AT_ONCE = 4


def kernel(
    tokens,
    norm_gain,
    w_query,
    w_key,
    w_value,
    conv_in,
    conv_gate,
    conv_taps,
    conv_gain,
    cum_gate,
    out_attn,
    out_conv,
    mixed,
    log_total,
    nt,
    wall,
    wo,
    wconv,
    qp,
    qb,
    ks,
    vs,
    kp,
    vp,
    cpad,
    mrow,
    acc,
    obuf,
    orecv,
    sbuf,
    srecv,
    gb,
    rim,
    cg,
    cv,
    sq,
    csq,
    xs,
    sb,
    rb,
    po,
    t2,
    r2r,
    r2l,
    sr,
    sl,
    frl,
    frr,
    at_out,
    at_in,
    lt_out,
    lt_in,
    wsem,
    gsend,
    grecv,
    wosend,
    worecv,
    ksend,
    krecv,
    vsend,
    vrecv,
    qsend,
    qrecv,
    qbsend,
    qbrecv,
    qrsend,
    qrrecv,
    msend,
    mrecv,
    osend,
    orecv_sem,
    csend,
    crecv,
    xsend,
    xrecv,
    asend,
    arecv,
    lsend,
    lrecv,
):
    s_me = lax.axis_index("sp")
    t_me = lax.axis_index("tp")
    nsp = lax.axis_size("sp")
    nz = nsp // NX
    z = s_me // NX
    x = s_me % NX
    y = t_me // 2
    c = t_me % 2
    rows = tokens.shape[0]
    half = rows // 2
    depth = tokens.shape[1]
    tok = rows * 8
    mid_tok = tok // 2
    zbar = nz - 1 - z

    def at_tp(t):
        return (s_me, t)

    def at_sp(s):
        return (s, t_me)

    def rcopy(src, dst, ssem, rsem, dev):
        return pltpu.make_async_remote_copy(
            src_ref=src,
            dst_ref=dst,
            send_sem=ssem,
            recv_sem=rsem,
            device_id=dev,
            device_id_type=MESH,
        )

    wcopies = []
    at = 0
    for i, w in enumerate((w_query, w_key, w_value, conv_in, conv_gate)):
        n = w.shape[1]
        wcopies.append(pltpu.make_async_copy(w, wall.at[:, pl.ds(at, n)], wsem.at[i]))
        at += n
    ocopies = [
        pltpu.make_async_copy(out_attn, wo.at[t_me], wsem.at[5]),
        pltpu.make_async_copy(out_conv, wconv, wsem.at[6]),
    ]
    for w in wcopies + ocopies:
        w.start()

    barrier = pltpu.get_barrier_semaphore()
    for d in range(1, 8):
        pl.semaphore_signal(
            barrier, inc=1, device_id=at_tp((t_me + d) % 8), device_id_type=MESH
        )
    for d in range(1, NX):
        pl.semaphore_signal(
            barrier, inc=1, device_id=at_sp(z * NX + (x + d) % NX), device_id_type=MESH
        )
    for d in (1, nz - 1):
        pl.semaphore_signal(
            barrier, inc=1, device_id=at_sp(((z + d) % nz) * NX + x), device_id_type=MESH
        )
    for d in (1, nsp - 1):
        pl.semaphore_signal(
            barrier, inc=1, device_id=at_sp((s_me + d) % nsp), device_id_type=MESH
        )

    for t in range(8):
        pl.semaphore_signal(
            barrier, inc=1, device_id=(zbar * NX + x, t), device_id_type=MESH
        )

    wide = tokens[...].astype(F32)
    factor = lax.rsqrt(jnp.mean(wide * wide, axis=1, keepdims=True) + 1e-06)
    nt[t_me] = (wide * factor * norm_gain[...]).astype(BF16)
    qp[:, 0, HEAD:, :] = jnp.ones((NX, HEAD, tok), BF16)
    qp[:, 1, :HEAD, :] = jnp.ones((NX, HEAD, tok), BF16)
    vp[:, HEAD:, :] = jnp.ones((2, VROWS - HEAD, tok), BF16)
    cpad[...] = jnp.zeros_like(cpad)
    mrow[...] = jnp.full_like(mrow, LOW)
    acc[...] = jnp.zeros_like(acc)

    pl.semaphore_wait(barrier, 7 + NX - 1 + 4 + 8)

    sib = y * 2 + (1 - c)
    tr = ((y + 1) % NY) * 2 + c
    tl = ((y + NY - 1) % NY) * 2 + c
    to = ((y + 2) % NY) * 2 + c
    lo, hi = pl.ds(0, half), pl.ds(half, half)

    def gather_over_tp(buf, ssem, rsem):
        n = buf.shape[1] // 2
        first, last = pl.ds(0, n), pl.ds(n, n)

        def gcopy(k, src, part, dev):
            ref = buf.at[src] if part is None else buf.at[src, part]
            return rcopy(ref, ref, ssem.at[k], rsem.at[k], at_tp(dev))

        return [
            gcopy(0, t_me, None, sib),
            gcopy(1, t_me, first, tr),
            gcopy(2, t_me, last, tr),
            gcopy(3, t_me, last, tl),
            gcopy(4, t_me, first, tl),
            gcopy(5, tl, None, sib),
            gcopy(6, tr, None, sib),
            gcopy(7, tl, first, tr),
            gcopy(8, tr, last, tl),
            gcopy(9, to, first, sib),
            gcopy(10, to, last, sib),
        ]

    g = gather_over_tp(nt, gsend, grecv)
    gw = gather_over_tp(wo, wosend, worecv)
    for k in (1, 3, 2, 4, 0):
        g[k].start()

    def sp_of(zz):
        return at_sp(zz * NX + x)

    def kcopy(zb, t, zt, part=None):
        ref = ks.at[zb] if part is None else ks.at[zb, part]
        return rcopy(ref, ref, ksend.at[t], krecv.at[t], sp_of(zt))

    def vcopy(zb, t, zt, part=None):
        ref = vs.at[zb] if part is None else vs.at[zb, :, part]
        return rcopy(ref, ref, vsend.at[t], vrecv.at[t], sp_of(zt))

    low_half, high_half = pl.ds(0, mid_tok), pl.ds(mid_tok, mid_tok)

    def qcopies(src, d, lanes, ssem, rsem):
        dev = at_sp(z * NX + (x + d) % NX)
        a = qp.at[src, 0, pl.ds(0, HEAD), lanes]
        b = qp.at[src, 1, pl.ds(HEAD, HEAD), lanes]
        return (
            rcopy(a, a, ssem.at[2 * d - 2], rsem.at[2 * d - 2], dev),
            rcopy(b, b, ssem.at[2 * d - 1], rsem.at[2 * d - 1], dev),
        )

    def qbcopies(src, lanes):
        dev = sp_of(zbar)
        return (
            rcopy(
                qb.at[pl.ds(0, HEAD), src],
                qp.at[x, 0, pl.ds(0, HEAD), lanes],
                qbsend.at[0],
                qbrecv.at[0],
                dev,
            ),
            rcopy(
                qb.at[pl.ds(HEAD, HEAD), src],
                qp.at[x, 1, pl.ds(HEAD, HEAD), lanes],
                qbsend.at[1],
                qbrecv.at[1],
                dev,
            ),
        )

    rcopy_rim = rcopy(
        gb.at[pl.ds(tok - 32, 32)], rim, msend.at[0], mrecv.at[0], at_sp((s_me + 1) % nsp)
    )
    for w in wcopies:
        w.wait()

    def project(i, carry):
        @pl.when(i == 0)
        def _():
            g[0].wait_recv()

        @pl.when(i == 1)
        def _():
            g[1].wait_recv()
            g[7].start()
            g[3].wait_recv()
            g[8].start()
            g[2].wait_recv()
            g[5].start()
            g[4].wait_recv()
            g[6].start()
            g[5].wait_recv()

        @pl.when(i == 2)
        def _():
            g[6].wait_recv()

        @pl.when(i == 3)
        def _():
            g[7].wait_recv()
            g[9].start()
            g[8].wait_recv()
            g[10].start()
            g[9].wait_recv()
            g[10].wait_recv()
            ocopies[0].wait()
            gw[1].start()
            gw[3].start()

        p = (y + 2 * NY - (2 * (i % 2) - 1) * ((i + 1) // 2)) % NY
        lhs = nt[pl.ds(2 * p, 2)].reshape(2 * rows, depth)
        res = jnp.dot(lhs, wall[...], preferred_element_type=F32)
        here = pl.ds(pl.multiple_of(p * 2 * rows, 2 * rows), 2 * rows)
        opened = res[:, 384:640]
        gating = res[:, 640:896]
        gate = (opened / (1.0 + jnp.exp(-gating))).astype(BF16)
        gb[here, :] = gate
        cg[pl.ds(pl.multiple_of(p * 2 * rows + 32, 32), 2 * rows), :] = gate.astype(F32)
        ks[z, here, :] = res[:, 128:256].astype(BF16)
        vs[z, :, here] = res[:, 256:384].T.astype(BF16)
        qt = (res[:, :128] * HEAD ** (-0.5)).T.astype(BF16)

        @pl.when(p < NY // 2)
        def _():
            qp[x, 0, :HEAD, here] = qt[:HEAD]
            qp[x, 1, HEAD:, here] = qt[HEAD:]

        qb[:, here] = qt

        @pl.when(p == NY - 1)
        def _():
            rcopy_rim.start()

        for t, zt in ((1, (z + 1) % nz), (2, (z + nz - 1) % nz)):
            kcopy(z, t, zt, here).start()
            vcopy(z, t, zt, here).start()

        @pl.when(p < NY // 2)
        def _():
            for d in (1, 3, 2):
                for q in qcopies(x, d, here, qsend, qrecv):
                    q.start()

        @pl.when(p >= NY // 2)
        def _():
            for q in qbcopies(here, here):
                q.start()

        return carry

    lax.fori_loop(0, NY, project, 0)

    rcopy_rim.wait_recv()
    first = jnp.where(s_me > 0, 1.0, 0.0).astype(F32)
    cg[0:32, :] = rim[...].astype(F32) * first

    def conv_rows(i, carry):
        r0 = pl.multiple_of(i * 64, 64)
        win = cg[pl.ds(r0, 96), :]
        total = jnp.zeros((64, win.shape[1]), F32)
        for b in range(8):
            turned = win if b == 0 else pltpu.roll(win, 96 - b, 0)
            for a in range(5):
                k = 8 * a + b - 2
                if 0 <= k < 31:
                    total = total + conv_taps[k : k + 1, :] * turned[8 * a : 8 * a + 64]
        cv[pl.ds(r0, 64), :] = total
        square = total * total
        sq[pl.ds(r0, 64), :] = square[:, :128] + square[:, 128:]
        return carry

    lax.fori_loop(0, tok // 64, conv_rows, 0)
    part = jnp.sum(sq[...].T, axis=0, keepdims=True)
    csq[t_me] = part
    ccopies = []
    for d in range(1, 8):
        cc = rcopy(
            csq.at[t_me], csq.at[t_me], csend.at[d], crecv.at[d], at_tp((t_me + d) % 8)
        )
        cc.start()
        ccopies.append(cc)
    for k in (2, 4, 0):
        gw[k].start()

    cref = cum_gate[:, pl.ds(pl.multiple_of(z * NX * tok, 128), 128)][:, :1]

    def prepare(zb):
        ck = cum_gate[:, pl.ds(pl.multiple_of((zb * NX + x) * tok, 128), tok)]
        bias = cref - ck
        high = bias.astype(BF16).astype(F32)
        left = bias - high
        mid = left.astype(BF16).astype(F32)
        low = left - mid
        rowid = lax.broadcasted_iota(jnp.int32, (8, tok), 0)
        for h, r0 in ((0, HEAD), (1, 0)):
            tile = jnp.where(
                rowid == 0,
                high[h : h + 1],
                jnp.where(
                    rowid == 1, mid[h : h + 1], jnp.where(rowid == 2, low[h : h + 1], 0.0)
                ),
            )
            cpad[r0 : r0 + 8, :] = tile
        extra = cpad[...].T
        kf = ks[zb].astype(F32)
        lane = lax.broadcasted_iota(jnp.int32, (tok, 2 * HEAD), 1)
        kp[0] = jnp.where(lane < HEAD, kf, extra).astype(BF16)
        kp[1] = jnp.where(lane < HEAD, extra, kf).astype(BF16)
        vp[0, :HEAD, :] = vs[zb, :HEAD, :]
        vp[1, :HEAD, :] = vs[zb, HEAD:, :]

    def chunks(js, g, masked):
        lanes = pl.ds(pl.multiple_of(g * mid_tok, mid_tok), mid_tok)
        units = [(j, h) for j in js for h in range(2)]
        old = [mrow[j, h, :, lanes] for j, h in units]
        held = [acc[j, h, :, lanes] for j, h in units]
        sc = [jnp.dot(kp[h], qp[j, h, :, lanes], preferred_element_type=F32) for j, h in units]
        if masked:
            kpos = lax.broadcasted_iota(jnp.int32, sc[0].shape, 0)
            qpos = lax.broadcasted_iota(jnp.int32, sc[0].shape, 1) + g * mid_tok
            sc = [jnp.where(kpos <= qpos, v, LOW) for v in sc]
        new = [jnp.maximum(o, jnp.max(v, axis=0, keepdims=True)) for o, v in zip(old, sc)]
        wts = [jnp.exp2((v - n) * LOG2E).astype(BF16) for n, v in zip(new, sc)]
        shrink = [jnp.exp2((o - n) * LOG2E) for o, n in zip(old, new)]
        out = [
            a * k + jnp.dot(vp[h], w, preferred_element_type=F32)
            for a, k, w, (_, h) in zip(held, shrink, wts, units)
        ]
        for n, o, (j, h) in zip(new, out, units):
            mrow[j, h, :, lanes] = n
            acc[j, h, :, lanes] = o

    def place(t):
        dr = 2 * (t % 2) - 1
        return dr, (z + nz - dr * ((t + 1) // 2)) % nz

    def ocopies_of(d, lanes, k):
        dev = at_sp(z * NX + (x + d) % NX)
        return (
            rcopy(
                obuf.at[d - 1, :, lanes],
                orecv.at[d - 1, :, lanes],
                osend.at[2 * k + 4 * (d - 1)],
                orecv_sem.at[2 * k + 4 * (d - 1)],
                dev,
            ),
            rcopy(
                sbuf.at[d - 1, :, lanes],
                srecv.at[d - 1, :, lanes],
                osend.at[2 * k + 4 * (d - 1) + 1],
                orecv_sem.at[2 * k + 4 * (d - 1) + 1],
                dev,
            ),
        )

    def final_at(zz, gg):
        zq = nz - 1 - zz if gg else zz
        order = [(zz - (2 * (t % 2) - 1) * ((t + 1) // 2)) % nz for t in range(nz)]
        return max(t for t in range(nz) if order[t] <= zq)

    def finish(t, g):
        done = False
        for zz in range(nz):
            for gg in range(2):
                done = done | ((z == zz) & (g == gg) & (t == final_at(zz, gg)))

        @pl.when(done)
        def _():
            lanes = pl.ds(pl.multiple_of(g * mid_tok, mid_tok), mid_tok)
            for d in (2, 1, 3):
                j = (x + d) % NX
                for h in range(2):
                    obuf[d - 1, h * HEAD : (h + 1) * HEAD, lanes] = acc[j, h, :HEAD, lanes].astype(
                        BF16
                    )
                    sbuf[d - 1, h : h + 1, lanes] = mrow[j, h, :, lanes]
                    sbuf[d - 1, 2 + h : 3 + h, lanes] = acc[j, h, HEAD : HEAD + 1, lanes]
                for cp in ocopies_of(d, lanes, g):
                    cp.start()

    def whole(g):
        def some(i, carry):
            chunks(tuple(i * AT_ONCE + k for k in range(AT_ONCE)), g, False)
            return carry

        lax.fori_loop(0, NX // AT_ONCE, some, 0)

    def diagonal(g):
        chunks((x,), g, True)

        def one(j, carry):
            chunks((j,), g, False)
            return carry

        lax.fori_loop(x + 1, NX, one, 0)

    def tile(t):
        _, zb = place(t)

        @pl.when((zb <= z) | (zb <= zbar))
        def _():
            prepare(zb)

            def group(i, carry):
                g = i + (z // (nz // 2)) * (1 - 2 * i)
                zq = z + g * (nz - 1 - 2 * z)

                @pl.when(zb < zq)
                def _():
                    whole(g)

                @pl.when(zb == zq)
                def _():
                    diagonal(g)

                @pl.when(zb <= zq)
                def _():
                    finish(t, g)

                return carry

            lax.fori_loop(0, 2, group, 0)

    def forward(t):
        dr, zb = place(t)
        zt = (z + nz + dr) % nz
        kcopy(zb, t, zt).wait_recv()
        if t <= 5:
            kcopy(zb, t + 2, zt).start()
        vcopy(zb, t, zt).wait_recv()
        if t <= 4 or t == 6:
            vcopy(zb, t + 2 - t // 6, zt).start()

    for d in range(1, NX):
        for q in qcopies(x, d, low_half, qsend, qrecv):
            q.wait_recv()
    prepare(z)
    diagonal(0)
    finish(0, 0)
    forward(1)
    forward(2)

    for q in qbcopies(high_half, high_half):
        q.wait_recv()
    for d in (1, 3, 2):
        for q in qcopies(x, d, high_half, qrsend, qrrecv):
            q.start()

    def project_out(which, emit):
        lhs = xs[which].reshape(NY * rows, xs.shape[3])

        def columns(n, carry):
            cols = pl.ds(pl.multiple_of(n * 512, 512), 512)
            res = jnp.dot(lhs, wconv[:, cols], preferred_element_type=F32)
            emit(cols, res)
            return carry

        lax.fori_loop(0, depth // 512, columns, 0)

    def emit_sib(cols, res):
        sb[:, :, cols] = res.astype(BF16).reshape(NY, rows, 512)

    def emit_own(cols, res):
        po[:, :, cols] = res.reshape(NY, rows, 512)

    ybits = [(y + k) % NY for k in range(NY)]

    def xcopy(k, src, dst, dev):
        return rcopy(src, dst, xsend.at[k], xrecv.at[k], at_tp(dev))

    bcopies = [xcopy(k, sb.at[ybits[k]], rb.at[ybits[k]], sib) for k in range(NY)]

    def conv_part():
        for cc in ccopies:
            cc.wait_recv()
        total = csq[0]
        for t in range(1, 8):
            total = total + csq[t]
        scale = lax.rsqrt(total / (8.0 * conv_gain.shape[1]) + 1e-06)
        sq[...] = jnp.broadcast_to(scale, (128, tok)).T
        for i in range(8):
            r = pl.ds(i * rows, rows)
            factor = sq[r, :]
            for b in range(2):
                lanes = pl.ds(b * 128, 128)
                v = cv[r, lanes] * factor * conv_gain[:, lanes]
                v = v / (1.0 + jnp.exp(-v))
                xs[i % 2, i // 2, :, lanes] = v.astype(BF16)
        ocopies[1].wait()

        project_out(1 - c, emit_sib)
        for k in (2, 1, 3, 0):
            bcopies[k].start()
        project_out(c, emit_own)

    far_r = xcopy(4, t2.at[lo], r2r, tr)
    far_l = xcopy(5, t2.at[hi], r2l, tl)
    near_r = xcopy(6, sr.at[hi], frl.at[hi], tr)
    near_l = xcopy(7, sl.at[lo], frr.at[lo], tl)
    both_r = xcopy(8, sr.at[lo], frl.at[lo], tr)
    both_l = xcopy(9, sl.at[hi], frr.at[hi], tl)

    def scatter_first():
        bcopies[2].wait_recv()
        t2[...] = (po[ybits[2]] + rb[ybits[2]].astype(F32)).astype(BF16)
        far_r.start()
        far_l.start()
        bcopies[1].wait_recv()
        sr[hi, :] = (po[ybits[1], hi] + rb[ybits[1], hi].astype(F32)).astype(BF16)
        near_r.start()
        bcopies[3].wait_recv()
        sl[lo, :] = (po[ybits[3], lo] + rb[ybits[3], lo].astype(F32)).astype(BF16)
        near_l.start()

    def scatter_second():
        far_r.wait_recv()
        sr[lo, :] = (
            po[ybits[1], lo] + rb[ybits[1], lo].astype(F32) + r2r[...].astype(F32)
        ).astype(BF16)
        both_r.start()
        far_l.wait_recv()
        sl[hi, :] = (
            po[ybits[3], hi] + rb[ybits[3], hi].astype(F32) + r2l[...].astype(F32)
        ).astype(BF16)
        both_l.start()
        bcopies[0].wait_recv()
        po[y] = po[y] + rb[y].astype(F32)

    def weights_on():
        for got, on in ((1, 7), (3, 8), (2, 5), (4, 6)):
            gw[got].wait_recv()
            gw[on].start()

    def weights_last():
        for got, on in ((7, 9), (8, 10)):
            gw[got].wait_recv()
            gw[on].start()

    conv_part()
    forward(3)
    forward(4)
    for d in range(1, NX):
        for q in qcopies(x, d, high_half, qrsend, qrrecv):
            q.wait_recv()

    @pl.when(z < zbar)
    def _():
        whole(1)

    def step(t, carry):
        tile(t)

        @pl.when(t == 1)
        def _():
            scatter_first()

        @pl.when(t == 3)
        def _():
            forward(5)
            forward(6)
            scatter_second()

        @pl.when(t == 4)
        def _():
            weights_on()

        @pl.when(t == 6)
        def _():
            forward(7)

        return carry

    lax.fori_loop(1, nz, step, 0)

    weights_last()

    for d in range(1, NX):
        for k, lanes in enumerate((low_half, high_half)):
            for cp in ocopies_of(d, lanes, k):
                cp.wait_recv()
    for h in range(2):
        best = mrow[x, h]
        for d in range(1, NX):
            best = jnp.maximum(best, srecv[d - 1, h : h + 1, :])
        share = jnp.exp2((mrow[x, h] - best) * LOG2E)
        summed = acc[x, h, HEAD : HEAD + 1, :] * share
        value = acc[x, h, :HEAD, :] * share
        for d in range(1, NX):
            share = jnp.exp2((srecv[d - 1, h : h + 1, :] - best) * LOG2E)
            summed = summed + srecv[d - 1, 2 + h : 3 + h, :] * share
            value = value + orecv[d - 1, h * HEAD : (h + 1) * HEAD, :].astype(F32) * share
        cpad[h * HEAD : (h + 1) * HEAD, :] = value / summed
        level = best + jnp.log(summed) - cref[h : h + 1]
        for zz, lanes, dst in ((z, low_half, log_total), (zbar, high_half, lt_out)):
            at = pl.multiple_of((zz * NX + x) * tok + lanes.start, 128)
            dst[h : h + 1, 0:mid_tok] = (
                level[:, lanes.start : lanes.start + mid_tok]
                + cum_gate[:, pl.ds(at, mid_tok)][h : h + 1]
            )
    at_out[...] = cpad[...].T.astype(BF16).reshape(8, rows, 2 * HEAD)

    mine = at_in.at[:, pl.ds(pl.multiple_of(t_me * 2 * HEAD, 2 * HEAD), 2 * HEAD)]
    lcopy = rcopy(lt_out, lt_in, lsend.at[0], lrecv.at[0], sp_of(zbar))

    def acopy(r):
        zz = z if r < 4 else zbar
        return rcopy(at_out.at[r], mine, asend.at[r], arecv.at[t_me], (zz * NX + x, r))

    for r in (4, 5, 6, 7):
        acopy(r).start()
    for r in (0, 1, 2, 3):

        @pl.when(t_me != r)
        def _(r=r):
            acopy(r).start()

    lcopy.start()

    @pl.when(t_me < 4)
    def _():
        mine[...] = at_out[t_me]

    for k in (0, 5, 6, 9, 10):
        gw[k].wait_recv()
    near_r.wait_recv()
    near_l.wait_recv()
    both_r.wait_recv()
    both_l.wait_recv()
    po[y] = po[y] + frl[...].astype(F32) + frr[...].astype(F32)
    for t in range(8):

        @pl.when((t_me >= 4) | (t_me != t))
        def _(t=t):
            rcopy(
                at_out.at[0],
                at_in.at[:, pl.ds(t * 2 * HEAD, 2 * HEAD)],
                asend.at[0],
                arecv.at[t],
                sp_of(zbar),
            ).wait_recv()

    lhs = at_in[...]

    def last(n, carry):
        cols = pl.ds(pl.multiple_of(n * 512, 512), 512)
        w = wo[:, :, cols].reshape(lhs.shape[1], 512)
        res = jnp.dot(lhs, w, preferred_element_type=F32)
        mixed[:, cols] = (po[y, :, cols] + res).astype(BF16)
        return carry

    lax.fori_loop(0, depth // 512, last, 0)
    lcopy.wait_recv()
    log_total[:, mid_tok:] = lt_in[0:2, :]

    for cp in g + gw:
        cp.wait_send()
    for t in range(1, 8):
        kcopy(z, t, (z + 1) % nz).wait_send()
        vcopy(z, t, (z + 1) % nz).wait_send()
    for d in range(1, NX):
        for q in qcopies(x, d, low_half, qsend, qrecv) + qcopies(x, d, high_half, qrsend, qrrecv):
            q.wait_send()
    for q in qbcopies(high_half, high_half):
        q.wait_send()
    rcopy_rim.wait_send()
    for d in range(1, NX):
        for k, lanes in enumerate((low_half, high_half)):
            for cp in ocopies_of(d, lanes, k):
                cp.wait_send()
    for cp in ccopies + bcopies:
        cp.wait_send()
    for cp in (far_r, far_l, near_r, near_l, both_r, both_l, lcopy):
        cp.wait_send()
    for r in (4, 5, 6, 7):
        acopy(r).wait_send()
    for r in (0, 1, 2, 3):

        @pl.when(t_me != r)
        def _(r=r):
            acopy(r).wait_send()


def per_device(*args):
    tokens = args[0]
    rows, depth = tokens.shape
    tok = rows * 8
    nz = lax.axis_size("sp") // NX
    att = args[2].shape[1]
    ch = args[5].shape[1]
    wide = 3 * att + 2 * ch
    ops = list(args)
    ops[1] = args[1][None]
    ops[8] = args[8][None]
    vmem = pl.BlockSpec(memory_space=pltpu.VMEM)
    hbm = pl.BlockSpec(memory_space=pltpu.HBM)
    specs = [vmem, vmem, hbm, hbm, hbm, hbm, hbm, vmem, vmem, vmem, hbm, hbm]
    dma = pltpu.SemaphoreType.DMA
    scratch = [
        pltpu.VMEM((8, rows, depth), BF16),
        pltpu.VMEM((depth, wide), BF16),
        pltpu.VMEM((8, att, depth), BF16),
        pltpu.VMEM((ch, depth), BF16),
        pltpu.VMEM((NX, 2, att, tok), BF16),
        pltpu.VMEM((att, tok), BF16),
        pltpu.VMEM((nz, tok, att), BF16),
        pltpu.VMEM((nz, att, tok), BF16),
        pltpu.VMEM((2, tok, att), BF16),
        pltpu.VMEM((2, VROWS, tok), BF16),
        pltpu.VMEM((att, tok), F32),
        pltpu.VMEM((NX, 2, 1, tok), F32),
        pltpu.VMEM((NX, 2, VROWS, tok), F32),
        pltpu.VMEM((NX - 1, att, tok), BF16),
        pltpu.VMEM((NX - 1, att, tok), BF16),
        pltpu.VMEM((NX - 1, 8, tok), F32),
        pltpu.VMEM((NX - 1, 8, tok), F32),
        pltpu.VMEM((tok, ch), BF16),
        pltpu.VMEM((32, ch), BF16),
        pltpu.VMEM((tok + 32, ch), F32),
        pltpu.VMEM((tok, ch), F32),
        pltpu.VMEM((tok, 128), F32),
        pltpu.VMEM((8, 1, tok), F32),
        pltpu.VMEM((2, NY, rows, ch), BF16),
        pltpu.VMEM((NY, rows, depth), BF16),
        pltpu.VMEM((NY, rows, depth), BF16),
        pltpu.VMEM((NY, rows, depth), F32),
        pltpu.VMEM((rows, depth), BF16),
        pltpu.VMEM((rows // 2, depth), BF16),
        pltpu.VMEM((rows // 2, depth), BF16),
        pltpu.VMEM((rows, depth), BF16),
        pltpu.VMEM((rows, depth), BF16),
        pltpu.VMEM((rows, depth), BF16),
        pltpu.VMEM((rows, depth), BF16),
        pltpu.VMEM((8, rows, att), BF16),
        pltpu.VMEM((rows, 8 * att), BF16),
        pltpu.VMEM((8, tok // 2), F32),
        pltpu.VMEM((8, tok // 2), F32),
    ] + [dma((n,)) for n in (7, 11, 11, 11, 11, 8, 8, 8, 8, 6, 6, 2, 2, 6, 6, 1, 1, 12, 12, 8, 8, 10, 10, 8, 8, 1, 1)]
    return pl.pallas_call(
        kernel,
        out_shape=(
            jax.ShapeDtypeStruct((rows, depth), BF16),
            jax.ShapeDtypeStruct((2, tok), F32),
        ),
        in_specs=specs,
        out_specs=(vmem, vmem),
        scratch_shapes=scratch,
        compiler_params=pltpu.CompilerParams(
            collective_id=0, has_side_effects=True, vmem_limit_bytes=58 * 1024 * 1024
        ),
        name="layer",
    )(*ops)


def solution(mesh):
    in_specs = (
        P(("sp", "tp"), None),
        P(),
        P(None, "tp"),
        P(None, "tp"),
        P(None, "tp"),
        P(None, "tp"),
        P(None, "tp"),
        P(None, "tp"),
        P("tp"),
        P("tp", None),
        P("tp", None),
        P("tp", None),
    )
    out_specs = (P(("sp", "tp"), None), P("tp", "sp"))
    return jax.shard_map(
        per_device, mesh=mesh, in_specs=in_specs, out_specs=out_specs, check_vma=False
    )
```

```python
import functools

import jax
import jax.numpy as jnp
from jax import lax
from jax.experimental import pallas as pl
from jax.experimental.pallas import tpu as pltpu
from jax.sharding import PartitionSpec as P

MESH = pl.DeviceIdType.MESH
F32 = jnp.float32
BF16 = jnp.bfloat16
HEAD = 64
NX = 4
NY = 4
LOW = -1e30
LOG2E = 1.4426950408889634
VROWS = 80
AT_ONCE = 4


def kernel(
    tokens,
    norm_gain,
    w_query,
    w_key,
    w_value,
    conv_in,
    conv_gate,
    conv_taps,
    conv_gain,
    cum_gate,
    out_attn,
    out_conv,
    mixed,
    log_total,
    nt,
    wall,
    wo,
    wconv,
    qp,
    qb,
    ks,
    vs,
    kp,
    vp,
    cpad,
    mrow,
    acc,
    obuf,
    orecv,
    sbuf,
    srecv,
    gb,
    rim,
    cg,
    cv,
    sq,
    csq,
    xs,
    sb,
    rb,
    po,
    t2,
    r2r,
    r2l,
    sr,
    sl,
    frl,
    frr,
    at_out,
    at_in,
    lt_out,
    lt_in,
    wsem,
    gsend,
    grecv,
    wosend,
    worecv,
    ksend,
    krecv,
    vsend,
    vrecv,
    qsend,
    qrecv,
    qbsend,
    qbrecv,
    qrsend,
    qrrecv,
    msend,
    mrecv,
    osend,
    orecv_sem,
    csend,
    crecv,
    xsend,
    xrecv,
    asend,
    arecv,
    lsend,
    lrecv,
):
    s_me = lax.axis_index("sp")
    t_me = lax.axis_index("tp")
    nsp = lax.axis_size("sp")
    nz = nsp // NX
    z = s_me // NX
    x = s_me % NX
    y = t_me // 2
    c = t_me % 2
    rows = tokens.shape[0]
    half = rows // 2
    depth = tokens.shape[1]
    tok = rows * 8
    mid_tok = tok // 2
    zbar = nz - 1 - z
    hb = y // (NY // 2)
    ha = 1 - hb

    def at_tp(t):
        return (s_me, t)

    def at_sp(s):
        return (s, t_me)

    def rcopy(src, dst, ssem, rsem, dev):
        return pltpu.make_async_remote_copy(
            src_ref=src,
            dst_ref=dst,
            send_sem=ssem,
            recv_sem=rsem,
            device_id=dev,
            device_id_type=MESH,
        )

    wcopies = []
    at = 0
    for i, w in enumerate((w_query, w_key, w_value, conv_in, conv_gate)):
        n = w.shape[1]
        wcopies.append(pltpu.make_async_copy(w, wall.at[:, pl.ds(at, n)], wsem.at[i]))
        at += n
    ocopies = [
        pltpu.make_async_copy(out_attn, wo.at[t_me], wsem.at[5]),
        pltpu.make_async_copy(out_conv, wconv, wsem.at[6]),
    ]
    for w in wcopies + ocopies:
        w.start()

    barrier = pltpu.get_barrier_semaphore()
    for d in range(1, 8):
        pl.semaphore_signal(
            barrier, inc=1, device_id=at_tp((t_me + d) % 8), device_id_type=MESH
        )
    for d in range(1, NX):
        pl.semaphore_signal(
            barrier, inc=1, device_id=at_sp(z * NX + (x + d) % NX), device_id_type=MESH
        )
    for d in (1, nz - 1):
        pl.semaphore_signal(
            barrier, inc=1, device_id=at_sp(((z + d) % nz) * NX + x), device_id_type=MESH
        )
    for d in (1, nsp - 1):
        pl.semaphore_signal(
            barrier, inc=1, device_id=at_sp((s_me + d) % nsp), device_id_type=MESH
        )

    for t in range(8):
        pl.semaphore_signal(
            barrier, inc=1, device_id=(zbar * NX + x, t), device_id_type=MESH
        )

    wide = tokens[...].astype(F32)
    factor = lax.rsqrt(jnp.mean(wide * wide, axis=1, keepdims=True) + 1e-06)
    nt[t_me] = (wide * factor * norm_gain[...]).astype(BF16)
    qp[:, 0, HEAD:, :] = jnp.ones((NX, HEAD, tok), BF16)
    qp[:, 1, :HEAD, :] = jnp.ones((NX, HEAD, tok), BF16)
    vp[:, HEAD:, :] = jnp.ones((2, VROWS - HEAD, tok), BF16)
    cpad[...] = jnp.zeros_like(cpad)
    mrow[...] = jnp.full_like(mrow, LOW)
    acc[...] = jnp.zeros_like(acc)

    pl.semaphore_wait(barrier, 7 + NX - 1 + 4 + 8)

    sib = y * 2 + (1 - c)
    tr = ((y + 1) % NY) * 2 + c
    tl = ((y + NY - 1) % NY) * 2 + c
    to = ((y + 2) % NY) * 2 + c
    lo, hi = pl.ds(0, half), pl.ds(half, half)

    def gather_over_tp(buf, ssem, rsem):
        n = buf.shape[1] // 2
        first, last = pl.ds(0, n), pl.ds(n, n)

        def gcopy(k, src, part, dev):
            ref = buf.at[src] if part is None else buf.at[src, part]
            return rcopy(ref, ref, ssem.at[k], rsem.at[k], at_tp(dev))

        return [
            gcopy(0, t_me, None, sib),
            gcopy(1, t_me, first, tr),
            gcopy(2, t_me, last, tr),
            gcopy(3, t_me, last, tl),
            gcopy(4, t_me, first, tl),
            gcopy(5, tl, None, sib),
            gcopy(6, tr, None, sib),
            gcopy(7, tl, first, tr),
            gcopy(8, tr, last, tl),
            gcopy(9, to, first, sib),
            gcopy(10, to, last, sib),
        ]

    g = gather_over_tp(nt, gsend, grecv)
    gw = gather_over_tp(wo, wosend, worecv)
    for k in (1, 3, 2, 4, 0):
        g[k].start()

    def sp_of(zz):
        return at_sp(zz * NX + x)

    def kcopy(zb, t, zt, part=None):
        ref = ks.at[zb] if part is None else ks.at[zb, part]
        return rcopy(ref, ref, ksend.at[t], krecv.at[t], sp_of(zt))

    def vcopy(zb, t, zt, part=None):
        ref = vs.at[zb] if part is None else vs.at[zb, :, part]
        return rcopy(ref, ref, vsend.at[t], vrecv.at[t], sp_of(zt))

    low_half, high_half = pl.ds(0, mid_tok), pl.ds(mid_tok, mid_tok)

    def qcopies(src, d, lanes, ssem, rsem):
        dev = at_sp(z * NX + (x + d) % NX)
        a = qp.at[src, 0, pl.ds(0, HEAD), lanes]
        b = qp.at[src, 1, pl.ds(HEAD, HEAD), lanes]
        return (
            rcopy(a, a, ssem.at[2 * d - 2], rsem.at[2 * d - 2], dev),
            rcopy(b, b, ssem.at[2 * d - 1], rsem.at[2 * d - 1], dev),
        )

    def qbcopies(src, lanes):
        dev = sp_of(zbar)
        return (
            rcopy(
                qb.at[pl.ds(0, HEAD), src],
                qp.at[x, 0, pl.ds(0, HEAD), lanes],
                qbsend.at[0],
                qbrecv.at[0],
                dev,
            ),
            rcopy(
                qb.at[pl.ds(HEAD, HEAD), src],
                qp.at[x, 1, pl.ds(HEAD, HEAD), lanes],
                qbsend.at[1],
                qbrecv.at[1],
                dev,
            ),
        )

    rcopy_rim = rcopy(
        gb.at[pl.ds(tok - 32, 32)], rim, msend.at[0], mrecv.at[0], at_sp((s_me + 1) % nsp)
    )
    for w in wcopies:
        w.wait()

    def project(i, carry):
        @pl.when(i == 0)
        def _():
            g[0].wait_recv()

        @pl.when(i == 1)
        def _():
            g[1].wait_recv()
            g[7].start()
            g[3].wait_recv()
            g[8].start()
            g[2].wait_recv()
            g[5].start()
            g[4].wait_recv()
            g[6].start()
            g[5].wait_recv()

        @pl.when(i == 2)
        def _():
            g[6].wait_recv()

        @pl.when(i == 3)
        def _():
            g[7].wait_recv()
            g[9].start()
            g[8].wait_recv()
            g[10].start()
            g[9].wait_recv()
            g[10].wait_recv()

        p = (y + 2 * NY - (2 * (i % 2) - 1) * ((i + 1) // 2)) % NY
        lhs = nt[pl.ds(2 * p, 2)].reshape(2 * rows, depth)
        res = jnp.dot(lhs, wall[...], preferred_element_type=F32)
        here = pl.ds(pl.multiple_of(p * 2 * rows, 2 * rows), 2 * rows)
        opened = res[:, 384:640]
        gating = res[:, 640:896]
        gate = (opened / (1.0 + jnp.exp(-gating))).astype(BF16)
        gb[here, :] = gate
        cg[pl.ds(pl.multiple_of(p * 2 * rows + 32, 32), 2 * rows), :] = gate.astype(F32)
        ks[z, here, :] = res[:, 128:256].astype(BF16)
        vs[z, :, here] = res[:, 256:384].T.astype(BF16)
        qt = (res[:, :128] * HEAD ** (-0.5)).T.astype(BF16)

        spot = pl.ds(pl.multiple_of((p % 2) * 2 * rows, 2 * rows), 2 * rows)
        over = pl.ds(pl.multiple_of((p % 2) * 2 * rows + mid_tok, 2 * rows), 2 * rows)

        @pl.when(p // 2 == hb)
        def _():
            qb[:, spot] = qt
            for q in qbcopies(spot, over):
                q.start()

        @pl.when(p == NY - 1)
        def _():
            rcopy_rim.start()

        for t, zt in ((1, (z + 1) % nz), (2, (z + nz - 1) % nz)):
            kcopy(z, t, zt, here).start()
            vcopy(z, t, zt, here).start()

        @pl.when(p // 2 == ha)
        def _():
            qp[x, 0, :HEAD, spot] = qt[:HEAD]
            qp[x, 1, HEAD:, spot] = qt[HEAD:]
            for d in (1, 3, 2):
                for q in qcopies(x, d, spot, qsend, qrecv):
                    q.start()

        return carry

    lax.fori_loop(0, NY, project, 0)

    def conv_rows(i, carry):
        r0 = pl.multiple_of(i * 64, 64)
        win = cg[pl.ds(r0, 96), :]
        total = jnp.zeros((64, win.shape[1]), F32)
        for b in range(8):
            turned = win if b == 0 else pltpu.roll(win, 96 - b, 0)
            for a in range(5):
                k = 8 * a + b - 2
                if 0 <= k < 31:
                    total = total + conv_taps[k : k + 1, :] * turned[8 * a : 8 * a + 64]
        cv[pl.ds(r0, 64), :] = total
        square = total * total
        sq[pl.ds(r0, 64), :] = square[:, :128] + square[:, 128:]
        return carry

    lax.fori_loop(1, tok // 64, conv_rows, 0)

    cref = cum_gate[:, pl.ds(pl.multiple_of(z * NX * tok, 128), 128)][:, :1]

    def prepare(zb):
        ck = cum_gate[:, pl.ds(pl.multiple_of((zb * NX + x) * tok, 128), tok)]
        bias = cref - ck
        high = bias.astype(BF16).astype(F32)
        left = bias - high
        mid = left.astype(BF16).astype(F32)
        low = left - mid
        rowid = lax.broadcasted_iota(jnp.int32, (8, tok), 0)
        for h, r0 in ((0, HEAD), (1, 0)):
            tile = jnp.where(
                rowid == 0,
                high[h : h + 1],
                jnp.where(
                    rowid == 1, mid[h : h + 1], jnp.where(rowid == 2, low[h : h + 1], 0.0)
                ),
            )
            cpad[r0 : r0 + 8, :] = tile
        extra = cpad[...].T
        kf = ks[zb].astype(F32)
        lane = lax.broadcasted_iota(jnp.int32, (tok, 2 * HEAD), 1)
        kp[0] = jnp.where(lane < HEAD, kf, extra).astype(BF16)
        kp[1] = jnp.where(lane < HEAD, extra, kf).astype(BF16)
        vp[0, :HEAD, :] = vs[zb, :HEAD, :]
        vp[1, :HEAD, :] = vs[zb, HEAD:, :]

    def chunks(js, g, masked):
        lanes = pl.ds(pl.multiple_of(g * mid_tok, mid_tok), mid_tok)
        units = [(j, h) for j in js for h in range(2)]
        old = [mrow[j, h, :, lanes] for j, h in units]
        held = [acc[j, h, :, lanes] for j, h in units]
        sc = [jnp.dot(kp[h], qp[j, h, :, lanes], preferred_element_type=F32) for j, h in units]
        if masked:
            kpos = lax.broadcasted_iota(jnp.int32, sc[0].shape, 0)
            qpos = lax.broadcasted_iota(jnp.int32, sc[0].shape, 1)
            qpos = qpos + (ha + g * (hb - ha)) * mid_tok
            sc = [jnp.where(kpos <= qpos, v, LOW) for v in sc]
        new = [jnp.maximum(o, jnp.max(v, axis=0, keepdims=True)) for o, v in zip(old, sc)]
        wts = [jnp.exp2((v - n) * LOG2E).astype(BF16) for n, v in zip(new, sc)]
        shrink = [jnp.exp2((o - n) * LOG2E) for o, n in zip(old, new)]
        out = [
            a * k + jnp.dot(vp[h], w, preferred_element_type=F32)
            for a, k, w, (_, h) in zip(held, shrink, wts, units)
        ]
        for n, o, (j, h) in zip(new, out, units):
            mrow[j, h, :, lanes] = n
            acc[j, h, :, lanes] = o

    def place(t):
        dr = 2 * (t % 2) - 1
        return dr, (z + nz - dr * ((t + 1) // 2)) % nz

    def ocopies_of(d, lanes, k):
        dev = at_sp(z * NX + (x + d) % NX)
        return (
            rcopy(
                obuf.at[d - 1, :, lanes],
                orecv.at[d - 1, :, lanes],
                osend.at[2 * k + 4 * (d - 1)],
                orecv_sem.at[2 * k + 4 * (d - 1)],
                dev,
            ),
            rcopy(
                sbuf.at[d - 1, :, lanes],
                srecv.at[d - 1, :, lanes],
                osend.at[2 * k + 4 * (d - 1) + 1],
                orecv_sem.at[2 * k + 4 * (d - 1) + 1],
                dev,
            ),
        )

    def final_at(zz, gg):
        zq = nz - 1 - zz if gg else zz
        order = [(zz - (2 * (t % 2) - 1) * ((t + 1) // 2)) % nz for t in range(nz)]
        return max(t for t in range(nz) if order[t] <= zq)

    def finish(t, g):
        done = False
        for zz in range(nz):
            for gg in range(2):
                done = done | ((z == zz) & (g == gg) & (t == final_at(zz, gg)))

        @pl.when(done)
        def _():
            lanes = pl.ds(pl.multiple_of(g * mid_tok, mid_tok), mid_tok)
            for d in (2, 1, 3):
                j = (x + d) % NX
                for h in range(2):
                    obuf[d - 1, h * HEAD : (h + 1) * HEAD, lanes] = acc[j, h, :HEAD, lanes].astype(
                        BF16
                    )
                    sbuf[d - 1, h : h + 1, lanes] = mrow[j, h, :, lanes]
                    sbuf[d - 1, 2 + h : 3 + h, lanes] = acc[j, h, HEAD : HEAD + 1, lanes]
                for cp in ocopies_of(d, lanes, g):
                    cp.start()

    def whole(g):
        def some(i, carry):
            chunks(tuple(i * AT_ONCE + k for k in range(AT_ONCE)), g, False)
            return carry

        lax.fori_loop(0, NX // AT_ONCE, some, 0)

    def diagonal(g):
        chunks((x,), g, True)

        def one(j, carry):
            chunks((j,), g, False)
            return carry

        lax.fori_loop(x + 1, NX, one, 0)

    def tile(t):
        _, zb = place(t)

        @pl.when((zb <= z) | (zb <= zbar))
        def _():
            prepare(zb)

            def group(i, carry):
                g = i + (z // (nz // 2)) * (1 - 2 * i)
                zq = z + g * (nz - 1 - 2 * z)

                @pl.when(zb < zq)
                def _():
                    whole(g)

                @pl.when(zb == zq)
                def _():
                    diagonal(g)

                @pl.when(zb <= zq)
                def _():
                    finish(t, g)

                return carry

            lax.fori_loop(0, 2, group, 0)

    def keys_on(t):
        dr, zb = place(t)
        zt = (z + nz + dr) % nz
        kcopy(zb, t, zt).wait_recv()
        if t <= 5:
            kcopy(zb, t + 2, zt).start()

    def values_on(t):
        dr, zb = place(t)
        zt = (z + nz + dr) % nz
        vcopy(zb, t, zt).wait_recv()
        if t <= 4 or t == 6:
            vcopy(zb, t + 2 - t // 6, zt).start()

    keys_on(1)
    keys_on(2)
    values_on(1)
    values_on(2)

    for q in qbcopies(low_half, high_half):
        q.wait_recv()
    for d in (1, 3, 2):
        for q in qcopies(x, d, high_half, qrsend, qrrecv):
            q.start()

    def project_out(which, emit):
        lhs = xs[which].reshape(NY * rows, xs.shape[3])

        def columns(n, carry):
            cols = pl.ds(pl.multiple_of(n * 512, 512), 512)
            res = jnp.dot(lhs, wconv[:, cols], preferred_element_type=F32)
            emit(cols, res)
            return carry

        lax.fori_loop(0, depth // 512, columns, 0)

    def emit_sib(cols, res):
        sb[:, :, cols] = res.astype(BF16).reshape(NY, rows, 512)

    def emit_own(cols, res):
        po[:, :, cols] = res.reshape(NY, rows, 512)

    ybits = [(y + k) % NY for k in range(NY)]

    def xcopy(k, src, dst, dev):
        return rcopy(src, dst, xsend.at[k], xrecv.at[k], at_tp(dev))

    bcopies = [xcopy(k, sb.at[ybits[k]], rb.at[ybits[k]], sib) for k in range(NY)]

    def conv_part():
        for cc in ccopies:
            cc.wait_recv()
        total = csq[0]
        for t in range(1, 8):
            total = total + csq[t]
        scale = lax.rsqrt(total / (8.0 * conv_gain.shape[1]) + 1e-06)
        sq[...] = jnp.broadcast_to(scale, (128, tok)).T
        for i in range(8):
            r = pl.ds(i * rows, rows)
            factor = sq[r, :]
            for b in range(2):
                lanes = pl.ds(b * 128, 128)
                v = cv[r, lanes] * factor * conv_gain[:, lanes]
                v = v / (1.0 + jnp.exp(-v))
                xs[i % 2, i // 2, :, lanes] = v.astype(BF16)
        ocopies[1].wait()

        project_out(1 - c, emit_sib)
        for k in (2, 1, 3, 0):
            bcopies[k].start()
        project_out(c, emit_own)

    far_r = xcopy(4, t2.at[lo], r2r, tr)
    far_l = xcopy(5, t2.at[hi], r2l, tl)
    near_r = xcopy(6, sr.at[hi], frl.at[hi], tr)
    near_l = xcopy(7, sl.at[lo], frr.at[lo], tl)
    both_r = xcopy(8, sr.at[lo], frl.at[lo], tr)
    both_l = xcopy(9, sl.at[hi], frr.at[hi], tl)

    def scatter_first():
        bcopies[2].wait_recv()
        t2[...] = (po[ybits[2]] + rb[ybits[2]].astype(F32)).astype(BF16)
        far_r.start()
        far_l.start()
        bcopies[1].wait_recv()
        sr[hi, :] = (po[ybits[1], hi] + rb[ybits[1], hi].astype(F32)).astype(BF16)
        near_r.start()
        bcopies[3].wait_recv()
        sl[lo, :] = (po[ybits[3], lo] + rb[ybits[3], lo].astype(F32)).astype(BF16)
        near_l.start()

    def scatter_second():
        far_r.wait_recv()
        sr[lo, :] = (
            po[ybits[1], lo] + rb[ybits[1], lo].astype(F32) + r2r[...].astype(F32)
        ).astype(BF16)
        both_r.start()
        far_l.wait_recv()
        sl[hi, :] = (
            po[ybits[3], hi] + rb[ybits[3], hi].astype(F32) + r2l[...].astype(F32)
        ).astype(BF16)
        both_l.start()
        bcopies[0].wait_recv()
        po[y] = po[y] + rb[y].astype(F32)

    def weights_on():
        for got, on in ((1, 7), (3, 8), (2, 5), (4, 6)):
            gw[got].wait_recv()
            gw[on].start()

    def weights_last():
        for got, on in ((7, 9), (8, 10)):
            gw[got].wait_recv()
            gw[on].start()

    rcopy_rim.wait_recv()
    first = jnp.where(s_me > 0, 1.0, 0.0).astype(F32)
    cg[0:32, :] = rim[...].astype(F32) * first
    conv_rows(0, 0)
    part = jnp.sum(sq[...].T, axis=0, keepdims=True)
    csq[t_me] = part
    ccopies = []
    for d in range(1, 8):
        cc = rcopy(
            csq.at[t_me], csq.at[t_me], csend.at[d], crecv.at[d], at_tp((t_me + d) % 8)
        )
        cc.start()
        ccopies.append(cc)
    ocopies[0].wait()
    for k in (1, 3, 2, 4, 0):
        gw[k].start()

    for d in range(1, NX):
        for q in qcopies(x, d, low_half, qsend, qrecv):
            q.wait_recv()
    prepare(z)
    diagonal(0)
    finish(0, 0)
    keys_on(3)
    keys_on(4)
    for d in range(1, NX):
        for q in qcopies(x, d, high_half, qrsend, qrrecv):
            q.wait_recv()

    @pl.when(z < zbar)
    def _():
        whole(1)

    swap = ((z + 4) // nz) * ((2 * nz - 2 - z) // nz)

    def step(i, carry):
        early = (i // 2 % 2) * (1 - i // 4)
        is_two, is_three = early * (1 - i % 2), early * (i % 2)
        t = i + swap * (is_two - is_three)
        tile(t)

        @pl.when(i == 1)
        def _():
            values_on(3)
            values_on(4)
            conv_part()
            keys_on(5)
            keys_on(6)

        @pl.when(i == 2)
        def _():
            values_on(5)
            values_on(6)
            scatter_first()

        @pl.when(i == 4)
        def _():
            weights_on()

        @pl.when(i == 5)
        def _():
            scatter_second()

        @pl.when(i == 6)
        def _():
            keys_on(7)
            values_on(7)

        return carry

    lax.fori_loop(1, nz, step, 0)


    for d in range(1, NX):
        for k, lanes in enumerate((low_half, high_half)):
            for cp in ocopies_of(d, lanes, k):
                cp.wait_recv()
    for h in range(2):
        best = mrow[x, h]
        for d in range(1, NX):
            best = jnp.maximum(best, srecv[d - 1, h : h + 1, :])
        share = jnp.exp2((mrow[x, h] - best) * LOG2E)
        summed = acc[x, h, HEAD : HEAD + 1, :] * share
        value = acc[x, h, :HEAD, :] * share
        for d in range(1, NX):
            share = jnp.exp2((srecv[d - 1, h : h + 1, :] - best) * LOG2E)
            summed = summed + srecv[d - 1, 2 + h : 3 + h, :] * share
            value = value + orecv[d - 1, h * HEAD : (h + 1) * HEAD, :].astype(F32) * share
        cpad[h * HEAD : (h + 1) * HEAD, :] = value / summed
        level = best + jnp.log(summed) - cref[h : h + 1]
        for zz, part, lanes, dst, at in (
            (z, ha, low_half, log_total, pl.multiple_of(ha * mid_tok, mid_tok)),
            (zbar, hb, high_half, lt_out, 0),
        ):
            here = pl.multiple_of((zz * NX + x) * tok + part * mid_tok, 128)
            dst[h : h + 1, pl.ds(at, mid_tok)] = (
                level[:, lanes.start : lanes.start + mid_tok]
                + cum_gate[:, pl.ds(here, mid_tok)][h : h + 1]
            )
    at_out[...] = cpad[...].T.astype(BF16).reshape(8, rows, 2 * HEAD)

    mine = at_in.at[:, pl.ds(pl.multiple_of(t_me * 2 * HEAD, 2 * HEAD), 2 * HEAD)]
    lcopy = rcopy(lt_out, lt_in, lsend.at[0], lrecv.at[0], sp_of(zbar))

    def acopy(k):
        zz, owner = (z, 4 * ha + k) if k < 4 else (zbar, 4 * hb + k - 4)
        return rcopy(at_out.at[k], mine, asend.at[k], arecv.at[t_me], (zz * NX + x, owner))

    for k in (4, 5, 6, 7, 0, 1, 2, 3):
        acopy(k).start()
    lcopy.start()

    weights_last()
    for k in (0, 5, 6, 9, 10):
        gw[k].wait_recv()
    near_r.wait_recv()
    near_l.wait_recv()
    both_r.wait_recv()
    both_l.wait_recv()
    po[y] = po[y] + frl[...].astype(F32) + frr[...].astype(F32)
    for t in range(8):
        rcopy(
            at_out.at[0],
            at_in.at[:, pl.ds(t * 2 * HEAD, 2 * HEAD)],
            asend.at[0],
            arecv.at[t],
            sp_of(zbar),
        ).wait_recv()

    lhs = at_in[...]

    def last(n, carry):
        cols = pl.ds(pl.multiple_of(n * 512, 512), 512)
        w = wo[:, :, cols].reshape(lhs.shape[1], 512)
        res = jnp.dot(lhs, w, preferred_element_type=F32)
        mixed[:, cols] = (po[y, :, cols] + res).astype(BF16)
        return carry

    lax.fori_loop(0, depth // 512, last, 0)
    lcopy.wait_recv()
    log_total[:, pl.ds(pl.multiple_of(hb * mid_tok, mid_tok), mid_tok)] = lt_in[0:2, :]

    for cp in g + gw:
        cp.wait_send()
    for t in range(1, 8):
        kcopy(z, t, (z + 1) % nz).wait_send()
        vcopy(z, t, (z + 1) % nz).wait_send()
    for d in range(1, NX):
        for q in qcopies(x, d, low_half, qsend, qrecv) + qcopies(x, d, high_half, qrsend, qrrecv):
            q.wait_send()
    for q in qbcopies(low_half, high_half):
        q.wait_send()
    rcopy_rim.wait_send()
    for d in range(1, NX):
        for k, lanes in enumerate((low_half, high_half)):
            for cp in ocopies_of(d, lanes, k):
                cp.wait_send()
    for cp in ccopies + bcopies:
        cp.wait_send()
    for cp in (far_r, far_l, near_r, near_l, both_r, both_l, lcopy):
        cp.wait_send()
    for k in range(8):
        acopy(k).wait_send()


def per_device(*args):
    tokens = args[0]
    rows, depth = tokens.shape
    tok = rows * 8
    nz = lax.axis_size("sp") // NX
    att = args[2].shape[1]
    ch = args[5].shape[1]
    wide = 3 * att + 2 * ch
    ops = list(args)
    ops[1] = args[1][None]
    ops[8] = args[8][None]
    vmem = pl.BlockSpec(memory_space=pltpu.VMEM)
    hbm = pl.BlockSpec(memory_space=pltpu.HBM)
    specs = [vmem, vmem, hbm, hbm, hbm, hbm, hbm, vmem, vmem, vmem, hbm, hbm]
    dma = pltpu.SemaphoreType.DMA
    scratch = [
        pltpu.VMEM((8, rows, depth), BF16),
        pltpu.VMEM((depth, wide), BF16),
        pltpu.VMEM((8, att, depth), BF16),
        pltpu.VMEM((ch, depth), BF16),
        pltpu.VMEM((NX, 2, att, tok), BF16),
        pltpu.VMEM((att, tok // 2), BF16),
        pltpu.VMEM((nz, tok, att), BF16),
        pltpu.VMEM((nz, att, tok), BF16),
        pltpu.VMEM((2, tok, att), BF16),
        pltpu.VMEM((2, VROWS, tok), BF16),
        pltpu.VMEM((att, tok), F32),
        pltpu.VMEM((NX, 2, 1, tok), F32),
        pltpu.VMEM((NX, 2, VROWS, tok), F32),
        pltpu.VMEM((NX - 1, att, tok), BF16),
        pltpu.VMEM((NX - 1, att, tok), BF16),
        pltpu.VMEM((NX - 1, 8, tok), F32),
        pltpu.VMEM((NX - 1, 8, tok), F32),
        pltpu.VMEM((tok, ch), BF16),
        pltpu.VMEM((32, ch), BF16),
        pltpu.VMEM((tok + 32, ch), F32),
        pltpu.VMEM((tok, ch), F32),
        pltpu.VMEM((tok, 128), F32),
        pltpu.VMEM((8, 1, tok), F32),
        pltpu.VMEM((2, NY, rows, ch), BF16),
        pltpu.VMEM((NY, rows, depth), BF16),
        pltpu.VMEM((NY, rows, depth), BF16),
        pltpu.VMEM((NY, rows, depth), F32),
        pltpu.VMEM((rows, depth), BF16),
        pltpu.VMEM((rows // 2, depth), BF16),
        pltpu.VMEM((rows // 2, depth), BF16),
        pltpu.VMEM((rows, depth), BF16),
        pltpu.VMEM((rows, depth), BF16),
        pltpu.VMEM((rows, depth), BF16),
        pltpu.VMEM((rows, depth), BF16),
        pltpu.VMEM((8, rows, att), BF16),
        pltpu.VMEM((rows, 8 * att), BF16),
        pltpu.VMEM((8, tok // 2), F32),
        pltpu.VMEM((8, tok // 2), F32),
    ] + [dma((n,)) for n in (7, 11, 11, 11, 11, 8, 8, 8, 8, 6, 6, 2, 2, 6, 6, 1, 1, 12, 12, 8, 8, 10, 10, 8, 8, 1, 1)]
    return pl.pallas_call(
        kernel,
        out_shape=(
            jax.ShapeDtypeStruct((rows, depth), BF16),
            jax.ShapeDtypeStruct((2, tok), F32),
        ),
        in_specs=specs,
        out_specs=(vmem, vmem),
        scratch_shapes=scratch,
        compiler_params=pltpu.CompilerParams(
            collective_id=0, has_side_effects=True, vmem_limit_bytes=58 * 1024 * 1024
        ),
        name="layer",
    )(*ops)


def solution(mesh):
    in_specs = (
        P(("sp", "tp"), None),
        P(),
        P(None, "tp"),
        P(None, "tp"),
        P(None, "tp"),
        P(None, "tp"),
        P(None, "tp"),
        P(None, "tp"),
        P("tp"),
        P("tp", None),
        P("tp", None),
        P("tp", None),
    )
    out_specs = (P(("sp", "tp"), None), P("tp", "sp"))
    return jax.shard_map(
        per_device, mesh=mesh, in_specs=in_specs, out_specs=out_specs, check_vma=False
    )
```

```python
import functools

import jax
import jax.numpy as jnp
from jax import lax
from jax.experimental import pallas as pl
from jax.experimental.pallas import tpu as pltpu
from jax.sharding import PartitionSpec as P

MESH = pl.DeviceIdType.MESH
F32 = jnp.float32
BF16 = jnp.bfloat16
HEAD = 64
NX = 4
NY = 4
LOW = -1e30
LOG2E = 1.4426950408889634
VROWS = 80
AT_ONCE = 4


def kernel(
    tokens,
    norm_gain,
    w_query,
    w_key,
    w_value,
    conv_in,
    conv_gate,
    taps_hbm,
    gain_hbm,
    cum_hbm,
    out_attn,
    out_conv,
    mixed_hbm,
    log_hbm,
    mixed,
    log_total,
    conv_taps,
    conv_gain,
    cum_gate,
    nt,
    wall,
    wo,
    wconv,
    qp,
    qb,
    ks,
    vs,
    kp,
    vp,
    cpad,
    mrow,
    acc,
    obuf,
    orecv,
    sbuf,
    srecv,
    gb,
    rim,
    cg,
    cv,
    sq,
    csq,
    xs,
    sb,
    rb,
    po,
    t2,
    r2r,
    r2l,
    sr,
    sl,
    frl,
    frr,
    at_out,
    at_in,
    lt_out,
    lt_in,
    wsem,
    gsend,
    grecv,
    wosend,
    worecv,
    ksend,
    krecv,
    vsend,
    vrecv,
    qsend,
    qrecv,
    qbsend,
    qbrecv,
    qrsend,
    qrrecv,
    msend,
    mrecv,
    osend,
    orecv_sem,
    csend,
    crecv,
    xsend,
    xrecv,
    asend,
    arecv,
    lsend,
    lrecv,
):
    s_me = lax.axis_index("sp")
    t_me = lax.axis_index("tp")
    nsp = lax.axis_size("sp")
    nz = nsp // NX
    z = s_me // NX
    x = s_me % NX
    y = t_me // 2
    c = t_me % 2
    rows = tokens.shape[0]
    half = rows // 2
    depth = tokens.shape[1]
    tok = rows * 8
    mid_tok = tok // 2
    zbar = nz - 1 - z
    hb = y // (NY // 2)
    ha = 1 - hb

    def at_tp(t):
        return (s_me, t)

    def at_sp(s):
        return (s, t_me)

    def rcopy(src, dst, ssem, rsem, dev):
        return pltpu.make_async_remote_copy(
            src_ref=src,
            dst_ref=dst,
            send_sem=ssem,
            recv_sem=rsem,
            device_id=dev,
            device_id_type=MESH,
        )

    wcopies = []
    at = 0
    for i, w in enumerate((w_query, w_key, w_value, conv_in, conv_gate)):
        n = w.shape[1]
        wcopies.append(pltpu.make_async_copy(w, wall.at[:, pl.ds(at, n)], wsem.at[i]))
        at += n
    ocopies = [
        pltpu.make_async_copy(out_attn, wo.at[t_me], wsem.at[5]),
        pltpu.make_async_copy(out_conv, wconv, wsem.at[6]),
    ]
    scopies = [
        pltpu.make_async_copy(src, dst, wsem.at[7 + i])
        for i, (src, dst) in enumerate(
            ((taps_hbm, conv_taps), (gain_hbm, conv_gain), (cum_hbm, cum_gate))
        )
    ]
    for w in wcopies + ocopies + scopies:
        w.start()

    barrier = pltpu.get_barrier_semaphore()
    for d in range(1, 8):
        pl.semaphore_signal(
            barrier, inc=1, device_id=at_tp((t_me + d) % 8), device_id_type=MESH
        )
    for d in range(1, NX):
        pl.semaphore_signal(
            barrier, inc=1, device_id=at_sp(z * NX + (x + d) % NX), device_id_type=MESH
        )
    for d in (1, nz - 1):
        pl.semaphore_signal(
            barrier, inc=1, device_id=at_sp(((z + d) % nz) * NX + x), device_id_type=MESH
        )
    for d in (1, nsp - 1):
        pl.semaphore_signal(
            barrier, inc=1, device_id=at_sp((s_me + d) % nsp), device_id_type=MESH
        )

    for t in range(8):
        pl.semaphore_signal(
            barrier, inc=1, device_id=(zbar * NX + x, t), device_id_type=MESH
        )

    wide = tokens[...].astype(F32)
    factor = lax.rsqrt(jnp.mean(wide * wide, axis=1, keepdims=True) + 1e-06)
    nt[t_me] = (wide * factor * norm_gain[...]).astype(BF16)
    qp[:, 0, HEAD:, :] = jnp.ones((NX, HEAD, tok), BF16)
    qp[:, 1, :HEAD, :] = jnp.ones((NX, HEAD, tok), BF16)
    vp[:, HEAD:, :] = jnp.ones((2, VROWS - HEAD, tok), BF16)
    cpad[...] = jnp.zeros_like(cpad)
    mrow[...] = jnp.full_like(mrow, LOW)
    acc[...] = jnp.zeros_like(acc)

    pl.semaphore_wait(barrier, 7 + NX - 1 + 4 + 8)

    sib = y * 2 + (1 - c)
    tr = ((y + 1) % NY) * 2 + c
    tl = ((y + NY - 1) % NY) * 2 + c
    to = ((y + 2) % NY) * 2 + c
    lo, hi = pl.ds(0, half), pl.ds(half, half)

    def gather_over_tp(buf, ssem, rsem):
        n = buf.shape[1] // 2
        first, last = pl.ds(0, n), pl.ds(n, n)

        def gcopy(k, src, part, dev):
            ref = buf.at[src] if part is None else buf.at[src, part]
            return rcopy(ref, ref, ssem.at[k], rsem.at[k], at_tp(dev))

        return [
            gcopy(0, t_me, None, sib),
            gcopy(1, t_me, first, tr),
            gcopy(2, t_me, last, tr),
            gcopy(3, t_me, last, tl),
            gcopy(4, t_me, first, tl),
            gcopy(5, tl, None, sib),
            gcopy(6, tr, None, sib),
            gcopy(7, tl, first, tr),
            gcopy(8, tr, last, tl),
            gcopy(9, to, first, sib),
            gcopy(10, to, last, sib),
        ]

    g = gather_over_tp(nt, gsend, grecv)
    gw = gather_over_tp(wo, wosend, worecv)
    for k in (1, 3, 2, 4, 0):
        g[k].start()

    def sp_of(zz):
        return at_sp(zz * NX + x)

    def kcopy(zb, t, zt, part=None):
        ref = ks.at[zb] if part is None else ks.at[zb, part]
        return rcopy(ref, ref, ksend.at[t], krecv.at[t], sp_of(zt))

    def vcopy(zb, t, zt, part=None):
        ref = vs.at[zb] if part is None else vs.at[zb, :, part]
        return rcopy(ref, ref, vsend.at[t], vrecv.at[t], sp_of(zt))

    def delivered(kind, t):
        up, s = t % 2 == 1, (t + 1) // 2
        if t == nz - 1:
            up = kind == "k"
        last = nz // 2 if up == (kind == "k") else nz // 2 - 1
        rows_at = []
        for zz in range(nz):
            zb = (zz - s if up else zz + s) % nz
            behind = [(zz + k if up else zz - k) % nz for k in range(last - s + 1)]
            if any(zb <= max(r, nz - 1 - r) for r in behind):
                rows_at.append(zz)
        return rows_at

    def among(kind, t, zz):
        found = False
        for r in delivered(kind, t):
            found = found | (zz == r)
        return found

    low_half, high_half = pl.ds(0, mid_tok), pl.ds(mid_tok, mid_tok)

    def qcopies(src, d, lanes, ssem, rsem):
        dev = at_sp(z * NX + (x + d) % NX)
        a = qp.at[src, 0, pl.ds(0, HEAD), lanes]
        b = qp.at[src, 1, pl.ds(HEAD, HEAD), lanes]
        return (
            rcopy(a, a, ssem.at[2 * d - 2], rsem.at[2 * d - 2], dev),
            rcopy(b, b, ssem.at[2 * d - 1], rsem.at[2 * d - 1], dev),
        )

    def qbcopies(src, lanes):
        dev = sp_of(zbar)
        return (
            rcopy(
                qb.at[pl.ds(0, HEAD), src],
                qp.at[x, 0, pl.ds(0, HEAD), lanes],
                qbsend.at[0],
                qbrecv.at[0],
                dev,
            ),
            rcopy(
                qb.at[pl.ds(HEAD, HEAD), src],
                qp.at[x, 1, pl.ds(HEAD, HEAD), lanes],
                qbsend.at[1],
                qbrecv.at[1],
                dev,
            ),
        )

    rcopy_rim = rcopy(
        gb.at[pl.ds(tok - 32, 32)], rim, msend.at[0], mrecv.at[0], at_sp((s_me + 1) % nsp)
    )
    for w in wcopies + scopies:
        w.wait()

    def project(i, carry):
        @pl.when(i == 0)
        def _():
            g[0].wait_recv()

        @pl.when(i == 1)
        def _():
            g[1].wait_recv()
            g[7].start()
            g[3].wait_recv()
            g[8].start()
            g[2].wait_recv()
            g[5].start()
            g[4].wait_recv()
            g[6].start()
            g[5].wait_recv()

        @pl.when(i == 2)
        def _():
            g[6].wait_recv()

        @pl.when(i == 3)
        def _():
            g[7].wait_recv()
            g[9].start()
            g[8].wait_recv()
            g[10].start()
            g[9].wait_recv()
            g[10].wait_recv()

        p = (y + 2 * NY - (2 * (i % 2) - 1) * ((i + 1) // 2)) % NY
        lhs = nt[pl.ds(2 * p, 2)].reshape(2 * rows, depth)
        res = jnp.dot(lhs, wall[...], preferred_element_type=F32)
        here = pl.ds(pl.multiple_of(p * 2 * rows, 2 * rows), 2 * rows)
        opened = res[:, 384:640]
        gating = res[:, 640:896]
        gate = (opened / (1.0 + jnp.exp(-gating))).astype(BF16)
        gb[here, :] = gate
        cg[pl.ds(pl.multiple_of(p * 2 * rows + 32, 32), 2 * rows), :] = gate.astype(F32)
        ks[z, here, :] = res[:, 128:256].astype(BF16)
        vs[z, :, here] = res[:, 256:384].T.astype(BF16)
        qt = (res[:, :128] * HEAD ** (-0.5)).T.astype(BF16)

        spot = pl.ds(pl.multiple_of((p % 2) * 2 * rows, 2 * rows), 2 * rows)
        over = pl.ds(pl.multiple_of((p % 2) * 2 * rows + mid_tok, 2 * rows), 2 * rows)

        @pl.when(p // 2 == hb)
        def _():
            qb[:, spot] = qt
            for q in qbcopies(spot, over):
                q.start()

        @pl.when(p == NY - 1)
        def _():
            rcopy_rim.start()

        for t, zt in ((1, (z + 1) % nz), (2, (z + nz - 1) % nz)):

            @pl.when(among("k", t, zt))
            def _(t=t, zt=zt):
                kcopy(z, t, zt, here).start()

            @pl.when(among("v", t, zt))
            def _(t=t, zt=zt):
                vcopy(z, t, zt, here).start()

        @pl.when(p // 2 == ha)
        def _():
            qp[x, 0, :HEAD, spot] = qt[:HEAD]
            qp[x, 1, HEAD:, spot] = qt[HEAD:]
            for d in (1, 3, 2):
                for q in qcopies(x, d, spot, qsend, qrecv):
                    q.start()

        return carry

    lax.fori_loop(0, NY, project, 0)

    def conv_rows(i, carry):
        r0 = pl.multiple_of(i * 64, 64)
        win = cg[pl.ds(r0, 96), :]
        total = jnp.zeros((64, win.shape[1]), F32)
        for b in range(8):
            turned = win if b == 0 else pltpu.roll(win, 96 - b, 0)
            for a in range(5):
                k = 8 * a + b - 2
                if 0 <= k < 31:
                    total = total + conv_taps[k : k + 1, :] * turned[8 * a : 8 * a + 64]
        cv[pl.ds(r0, 64), :] = total
        square = total * total
        sq[pl.ds(r0, 64), :] = square[:, :128] + square[:, 128:]
        return carry

    lax.fori_loop(1, tok // 64, conv_rows, 0)

    cref = cum_gate[:, pl.ds(pl.multiple_of(z * NX * tok, 128), 128)][:, :1]

    def prepare(zb):
        ck = cum_gate[:, pl.ds(pl.multiple_of((zb * NX + x) * tok, 128), tok)]
        bias = cref - ck
        high = bias.astype(BF16).astype(F32)
        left = bias - high
        mid = left.astype(BF16).astype(F32)
        low = left - mid
        rowid = lax.broadcasted_iota(jnp.int32, (8, tok), 0)
        for h, r0 in ((0, HEAD), (1, 0)):
            tile = jnp.where(
                rowid == 0,
                high[h : h + 1],
                jnp.where(
                    rowid == 1, mid[h : h + 1], jnp.where(rowid == 2, low[h : h + 1], 0.0)
                ),
            )
            cpad[r0 : r0 + 8, :] = tile
        extra = cpad[...].T
        kf = ks[zb].astype(F32)
        lane = lax.broadcasted_iota(jnp.int32, (tok, 2 * HEAD), 1)
        kp[0] = jnp.where(lane < HEAD, kf, extra).astype(BF16)
        kp[1] = jnp.where(lane < HEAD, extra, kf).astype(BF16)
        vp[0, :HEAD, :] = vs[zb, :HEAD, :]
        vp[1, :HEAD, :] = vs[zb, HEAD:, :]

    def chunks(js, g, masked):
        lanes = pl.ds(pl.multiple_of(g * mid_tok, mid_tok), mid_tok)
        units = [(j, h) for j in js for h in range(2)]
        old = [mrow[j, h, :, lanes] for j, h in units]
        held = [acc[j, h, :, lanes] for j, h in units]
        sc = [jnp.dot(kp[h], qp[j, h, :, lanes], preferred_element_type=F32) for j, h in units]
        if masked:
            kpos = lax.broadcasted_iota(jnp.int32, sc[0].shape, 0)
            qpos = lax.broadcasted_iota(jnp.int32, sc[0].shape, 1)
            ahead = kpos - qpos - (ha + g * (hb - ha)) * mid_tok
            sc = [jnp.where(ahead <= (j - x) * tok, v, LOW) for v, (j, _) in zip(sc, units)]
        new = [jnp.maximum(o, jnp.max(v, axis=0, keepdims=True)) for o, v in zip(old, sc)]
        wts = [jnp.exp2((v - n) * LOG2E).astype(BF16) for n, v in zip(new, sc)]
        shrink = [jnp.exp2((o - n) * LOG2E) for o, n in zip(old, new)]
        out = [
            a * k + jnp.dot(vp[h], w, preferred_element_type=F32)
            for a, k, w, (_, h) in zip(held, shrink, wts, units)
        ]
        for n, o, (j, h) in zip(new, out, units):
            mrow[j, h, :, lanes] = n
            acc[j, h, :, lanes] = o

    def place(t):
        dr = 2 * (t % 2) - 1
        return dr, (z + nz - dr * ((t + 1) // 2)) % nz

    def ocopies_of(d, lanes, k):
        dev = at_sp(z * NX + (x + d) % NX)
        return (
            rcopy(
                obuf.at[d - 1, :, lanes],
                orecv.at[d - 1, :, lanes],
                osend.at[2 * k + 4 * (d - 1)],
                orecv_sem.at[2 * k + 4 * (d - 1)],
                dev,
            ),
            rcopy(
                sbuf.at[d - 1, :, lanes],
                srecv.at[d - 1, :, lanes],
                osend.at[2 * k + 4 * (d - 1) + 1],
                orecv_sem.at[2 * k + 4 * (d - 1) + 1],
                dev,
            ),
        )

    def final_at(zz, gg):
        zq = nz - 1 - zz if gg else zz
        order = [(zz - (2 * (t % 2) - 1) * ((t + 1) // 2)) % nz for t in range(nz)]
        return max(t for t in range(nz) if order[t] <= zq)

    def finish(t, g):
        done = False
        for zz in range(nz):
            for gg in range(2):
                done = done | ((z == zz) & (g == gg) & (t == final_at(zz, gg)))

        @pl.when(done)
        def _():
            lanes = pl.ds(pl.multiple_of(g * mid_tok, mid_tok), mid_tok)
            for d in (2, 1, 3):
                j = (x + d) % NX
                for h in range(2):
                    obuf[d - 1, h * HEAD : (h + 1) * HEAD, lanes] = acc[j, h, :HEAD, lanes].astype(
                        BF16
                    )
                    sbuf[d - 1, h : h + 1, lanes] = mrow[j, h, :, lanes]
                    sbuf[d - 1, 2 + h : 3 + h, lanes] = acc[j, h, HEAD : HEAD + 1, lanes]
                for cp in ocopies_of(d, lanes, g):
                    cp.start()

    def whole(g):
        def some(i, carry):
            chunks(tuple(i * AT_ONCE + k for k in range(AT_ONCE)), g, False)
            return carry

        lax.fori_loop(0, NX // AT_ONCE, some, 0)

    def diagonal(g):
        chunks(tuple(range(NX)), g, True)

    def tile(t):
        _, zb = place(t)

        @pl.when((zb <= z) | (zb <= zbar))
        def _():
            prepare(zb)

            def group(i, carry):
                g = i + (z // (nz // 2)) * (1 - 2 * i)
                zq = z + g * (nz - 1 - 2 * z)

                @pl.when(zb < zq)
                def _():
                    whole(g)

                @pl.when(zb == zq)
                def _():
                    diagonal(g)

                @pl.when(zb <= zq)
                def _():
                    finish(t, g)

                return carry

            lax.fori_loop(0, 2, group, 0)

    def keys_on(t):
        dr, zb = place(t)
        zt = (z + nz + dr) % nz

        @pl.when(among("k", t, z))
        def _():
            kcopy(zb, t, zt).wait_recv()

        if t <= 5:

            @pl.when(among("k", t + 2, zt))
            def _():
                kcopy(zb, t + 2, zt).start()

    def values_on(t):
        dr, zb = place(t)
        zt = (z + nz + dr) % nz

        @pl.when(among("v", t, z))
        def _():
            vcopy(zb, t, zt).wait_recv()

        if t <= 4 or t == 6:
            on = t + 2 - t // 6

            @pl.when(among("v", on, zt))
            def _():
                vcopy(zb, on, zt).start()

    keys_on(1)
    keys_on(2)
    values_on(1)
    values_on(2)

    for q in qbcopies(low_half, high_half):
        q.wait_recv()
    for d in (1, 3, 2):
        for q in qcopies(x, d, high_half, qrsend, qrrecv):
            q.start()

    def project_out(which, emit):
        lhs = xs[which].reshape(NY * rows, xs.shape[3])

        def columns(n, carry):
            cols = pl.ds(pl.multiple_of(n * 512, 512), 512)
            res = jnp.dot(lhs, wconv[:, cols], preferred_element_type=F32)
            emit(cols, res)
            return carry

        lax.fori_loop(0, depth // 512, columns, 0)

    def emit_sib(cols, res):
        sb[:, :, cols] = res.astype(BF16).reshape(NY, rows, 512)

    def emit_own(cols, res):
        po[:, :, cols] = res.reshape(NY, rows, 512)

    ybits = [(y + k) % NY for k in range(NY)]

    def xcopy(k, src, dst, dev):
        return rcopy(src, dst, xsend.at[k], xrecv.at[k], at_tp(dev))

    bcopies = [xcopy(k, sb.at[ybits[k]], rb.at[ybits[k]], sib) for k in range(NY)]

    def conv_part():
        for cc in ccopies:
            cc.wait_recv()
        total = csq[0]
        for t in range(1, 8):
            total = total + csq[t]
        scale = lax.rsqrt(total / (8.0 * conv_gain.shape[1]) + 1e-06)
        sq[...] = jnp.broadcast_to(scale, (128, tok)).T
        for i in range(8):
            r = pl.ds(i * rows, rows)
            factor = sq[r, :]
            for b in range(2):
                lanes = pl.ds(b * 128, 128)
                v = cv[r, lanes] * factor * conv_gain[:, lanes]
                v = v / (1.0 + jnp.exp(-v))
                xs[i % 2, i // 2, :, lanes] = v.astype(BF16)
        ocopies[1].wait()

        project_out(1 - c, emit_sib)
        for k in (2, 1, 3, 0):
            bcopies[k].start()
        project_out(c, emit_own)

    far_r = xcopy(4, t2.at[lo], r2r, tr)
    far_l = xcopy(5, t2.at[hi], r2l, tl)
    near_r = xcopy(6, sr.at[hi], frl.at[hi], tr)
    near_l = xcopy(7, sl.at[lo], frr.at[lo], tl)
    both_r = xcopy(8, sr.at[lo], frl.at[lo], tr)
    both_l = xcopy(9, sl.at[hi], frr.at[hi], tl)

    def scatter_first():
        bcopies[2].wait_recv()
        t2[...] = (po[ybits[2]] + rb[ybits[2]].astype(F32)).astype(BF16)
        far_r.start()
        far_l.start()
        bcopies[1].wait_recv()
        sr[hi, :] = (po[ybits[1], hi] + rb[ybits[1], hi].astype(F32)).astype(BF16)
        near_r.start()
        bcopies[3].wait_recv()
        sl[lo, :] = (po[ybits[3], lo] + rb[ybits[3], lo].astype(F32)).astype(BF16)
        near_l.start()

    def scatter_second():
        far_r.wait_recv()
        sr[lo, :] = (
            po[ybits[1], lo] + rb[ybits[1], lo].astype(F32) + r2r[...].astype(F32)
        ).astype(BF16)
        both_r.start()
        far_l.wait_recv()
        sl[hi, :] = (
            po[ybits[3], hi] + rb[ybits[3], hi].astype(F32) + r2l[...].astype(F32)
        ).astype(BF16)
        both_l.start()
        bcopies[0].wait_recv()
        po[y] = po[y] + rb[y].astype(F32)

    def weights_on():
        for got, on in ((1, 7), (3, 8), (2, 5), (4, 6)):
            gw[got].wait_recv()
            gw[on].start()

    def weights_last():
        for got, on in ((7, 9), (8, 10)):
            gw[got].wait_recv()
            gw[on].start()

    rcopy_rim.wait_recv()
    first = jnp.where(s_me > 0, 1.0, 0.0).astype(F32)
    cg[0:32, :] = rim[...].astype(F32) * first
    conv_rows(0, 0)
    part = jnp.sum(sq[...].T, axis=0, keepdims=True)
    csq[t_me] = part
    ccopies = []
    for d in range(1, 8):
        cc = rcopy(
            csq.at[t_me], csq.at[t_me], csend.at[d], crecv.at[d], at_tp((t_me + d) % 8)
        )
        cc.start()
        ccopies.append(cc)
    ocopies[0].wait()
    for k in (1, 3, 2, 4, 0):
        gw[k].start()

    for d in range(1, NX):
        for q in qcopies(x, d, low_half, qsend, qrecv):
            q.wait_recv()
    prepare(z)
    diagonal(0)
    finish(0, 0)
    keys_on(3)
    keys_on(4)
    for d in range(1, NX):
        for q in qcopies(x, d, high_half, qrsend, qrrecv):
            q.wait_recv()

    @pl.when(z < zbar)
    def _():
        whole(1)

    swap = ((z + 4) // nz) * ((2 * nz - 2 - z) // nz)

    def step(i, carry):
        early = (i // 2 % 2) * (1 - i // 4)
        is_two, is_three = early * (1 - i % 2), early * (i % 2)
        t = i + swap * (is_two - is_three)
        tile(t)

        @pl.when(i == 1)
        def _():
            values_on(3)
            values_on(4)
            conv_part()
            keys_on(5)
            keys_on(6)

        @pl.when(i == 2)
        def _():
            values_on(5)
            values_on(6)
            scatter_first()

        @pl.when(i == 4)
        def _():
            weights_on()

        @pl.when(i == 6)
        def _():
            keys_on(7)
            values_on(7)
            scatter_second()

        return carry

    lax.fori_loop(1, nz, step, 0)


    for d in range(1, NX):
        for k, lanes in enumerate((low_half, high_half)):
            for cp in ocopies_of(d, lanes, k):
                cp.wait_recv()
    for h in range(2):
        best = mrow[x, h]
        for d in range(1, NX):
            best = jnp.maximum(best, srecv[d - 1, h : h + 1, :])
        share = jnp.exp2((mrow[x, h] - best) * LOG2E)
        summed = acc[x, h, HEAD : HEAD + 1, :] * share
        value = acc[x, h, :HEAD, :] * share
        for d in range(1, NX):
            share = jnp.exp2((srecv[d - 1, h : h + 1, :] - best) * LOG2E)
            summed = summed + srecv[d - 1, 2 + h : 3 + h, :] * share
            value = value + orecv[d - 1, h * HEAD : (h + 1) * HEAD, :].astype(F32) * share
        cpad[h * HEAD : (h + 1) * HEAD, :] = value / summed
        level = best + jnp.log(summed) - cref[h : h + 1]
        for zz, part, lanes, dst, at in (
            (z, ha, low_half, log_total, pl.multiple_of(ha * mid_tok, mid_tok)),
            (zbar, hb, high_half, lt_out, 0),
        ):
            here = pl.multiple_of((zz * NX + x) * tok + part * mid_tok, 128)
            dst[h : h + 1, pl.ds(at, mid_tok)] = (
                level[:, lanes.start : lanes.start + mid_tok]
                + cum_gate[:, pl.ds(here, mid_tok)][h : h + 1]
            )
    at_out[...] = cpad[...].T.astype(BF16).reshape(8, rows, 2 * HEAD)

    mine = at_in.at[:, pl.ds(pl.multiple_of(t_me * 2 * HEAD, 2 * HEAD), 2 * HEAD)]
    lcopy = rcopy(lt_out, lt_in, lsend.at[0], lrecv.at[0], sp_of(zbar))

    def acopy(k):
        zz, owner = (z, 4 * ha + k) if k < 4 else (zbar, 4 * hb + k - 4)
        return rcopy(at_out.at[k], mine, asend.at[k], arecv.at[t_me], (zz * NX + x, owner))

    for k in (4, 5, 6, 7, 0, 1, 2, 3):
        acopy(k).start()
    lcopy.start()

    weights_last()
    for k in (0, 5, 6, 9, 10):
        gw[k].wait_recv()
    near_r.wait_recv()
    near_l.wait_recv()
    both_r.wait_recv()
    both_l.wait_recv()
    po[y] = po[y] + frl[...].astype(F32) + frr[...].astype(F32)
    for t in range(8):
        rcopy(
            at_out.at[0],
            at_in.at[:, pl.ds(t * 2 * HEAD, 2 * HEAD)],
            asend.at[0],
            arecv.at[t],
            sp_of(zbar),
        ).wait_recv()

    lhs = at_in[...]

    lcopy.wait_recv()
    log_total[:, pl.ds(pl.multiple_of(hb * mid_tok, mid_tok), mid_tok)] = lt_in[0:2, :]
    log_put = pltpu.make_async_copy(log_total, log_hbm, wsem.at[10])
    log_put.start()

    def put(cols):
        return pltpu.make_async_copy(mixed.at[:, cols], mixed_hbm.at[:, cols], wsem.at[11])

    def last(n, carry):
        cols = pl.ds(pl.multiple_of(n * 512, 512), 512)
        w = wo[:, :, cols].reshape(lhs.shape[1], 512)
        res = jnp.dot(lhs, w, preferred_element_type=F32)
        mixed[:, cols] = (po[y, :, cols] + res).astype(BF16)
        put(cols).start()
        return carry

    lax.fori_loop(0, depth // 512, last, 0)

    for cp in g + gw:
        cp.wait_send()
    for t in range(1, 8):
        above, below = (z + 1) % nz, (z + nz - 1) % nz

        @pl.when(among("k", t, above if t % 2 else below))
        def _(t=t, above=above):
            kcopy(z, t, above).wait_send()

        @pl.when(among("v", t, above if t % 2 and t < nz - 1 else below))
        def _(t=t, above=above):
            vcopy(z, t, above).wait_send()

    for d in range(1, NX):
        for q in qcopies(x, d, low_half, qsend, qrecv) + qcopies(x, d, high_half, qrsend, qrrecv):
            q.wait_send()
    for q in qbcopies(low_half, high_half):
        q.wait_send()
    rcopy_rim.wait_send()
    for d in range(1, NX):
        for k, lanes in enumerate((low_half, high_half)):
            for cp in ocopies_of(d, lanes, k):
                cp.wait_send()
    for cp in ccopies + bcopies:
        cp.wait_send()
    for cp in (far_r, far_l, near_r, near_l, both_r, both_l, lcopy):
        cp.wait_send()
    for k in range(8):
        acopy(k).wait_send()
    log_put.wait()
    put(pl.ds(0, depth)).wait()


def per_device(*args):
    tokens = args[0]
    rows, depth = tokens.shape
    tok = rows * 8
    nz = lax.axis_size("sp") // NX
    att = args[2].shape[1]
    ch = args[5].shape[1]
    wide = 3 * att + 2 * ch
    ops = list(args)
    ops[1] = args[1][None]
    ops[8] = args[8][None]
    vmem = pl.BlockSpec(memory_space=pltpu.VMEM)
    hbm = pl.BlockSpec(memory_space=pltpu.HBM)
    specs = [vmem, vmem] + [hbm] * 10
    dma = pltpu.SemaphoreType.DMA
    scratch = [
        pltpu.VMEM((rows, depth), BF16),
        pltpu.VMEM((2, tok), F32),
        pltpu.VMEM(args[7].shape, F32),
        pltpu.VMEM((1, ch), F32),
        pltpu.VMEM(args[9].shape, F32),
        pltpu.VMEM((8, rows, depth), BF16),
        pltpu.VMEM((depth, wide), BF16),
        pltpu.VMEM((8, att, depth), BF16),
        pltpu.VMEM((ch, depth), BF16),
        pltpu.VMEM((NX, 2, att, tok), BF16),
        pltpu.VMEM((att, tok // 2), BF16),
        pltpu.VMEM((nz, tok, att), BF16),
        pltpu.VMEM((nz, att, tok), BF16),
        pltpu.VMEM((2, tok, att), BF16),
        pltpu.VMEM((2, VROWS, tok), BF16),
        pltpu.VMEM((att, tok), F32),
        pltpu.VMEM((NX, 2, 1, tok), F32),
        pltpu.VMEM((NX, 2, VROWS, tok), F32),
        pltpu.VMEM((NX - 1, att, tok), BF16),
        pltpu.VMEM((NX - 1, att, tok), BF16),
        pltpu.VMEM((NX - 1, 8, tok), F32),
        pltpu.VMEM((NX - 1, 8, tok), F32),
        pltpu.VMEM((tok, ch), BF16),
        pltpu.VMEM((32, ch), BF16),
        pltpu.VMEM((tok + 32, ch), F32),
        pltpu.VMEM((tok, ch), F32),
        pltpu.VMEM((tok, 128), F32),
        pltpu.VMEM((8, 1, tok), F32),
        pltpu.VMEM((2, NY, rows, ch), BF16),
        pltpu.VMEM((NY, rows, depth), BF16),
        pltpu.VMEM((NY, rows, depth), BF16),
        pltpu.VMEM((NY, rows, depth), F32),
        pltpu.VMEM((rows, depth), BF16),
        pltpu.VMEM((rows // 2, depth), BF16),
        pltpu.VMEM((rows // 2, depth), BF16),
        pltpu.VMEM((rows, depth), BF16),
        pltpu.VMEM((rows, depth), BF16),
        pltpu.VMEM((rows, depth), BF16),
        pltpu.VMEM((rows, depth), BF16),
        pltpu.VMEM((8, rows, att), BF16),
        pltpu.VMEM((rows, 8 * att), BF16),
        pltpu.VMEM((8, tok // 2), F32),
        pltpu.VMEM((8, tok // 2), F32),
    ] + [dma((n,)) for n in (12, 11, 11, 11, 11, 8, 8, 8, 8, 6, 6, 2, 2, 6, 6, 1, 1, 12, 12, 8, 8, 10, 10, 8, 8, 1, 1)]
    return pl.pallas_call(
        kernel,
        out_shape=(
            jax.ShapeDtypeStruct((rows, depth), BF16),
            jax.ShapeDtypeStruct((2, tok), F32),
        ),
        in_specs=specs,
        out_specs=(hbm, hbm),
        scratch_shapes=scratch,
        compiler_params=pltpu.CompilerParams(
            collective_id=0, has_side_effects=True, vmem_limit_bytes=58 * 1024 * 1024
        ),
        name="layer",
    )(*ops)


def solution(mesh):
    in_specs = (
        P(("sp", "tp"), None),
        P(),
        P(None, "tp"),
        P(None, "tp"),
        P(None, "tp"),
        P(None, "tp"),
        P(None, "tp"),
        P(None, "tp"),
        P("tp"),
        P("tp", None),
        P("tp", None),
        P("tp", None),
    )
    out_specs = (P(("sp", "tp"), None), P("tp", "sp"))
    return jax.shard_map(
        per_device, mesh=mesh, in_specs=in_specs, out_specs=out_specs, check_vma=False
    )
```

```python
import functools

import jax
import jax.numpy as jnp
from jax import lax
from jax.experimental import pallas as pl
from jax.experimental.pallas import tpu as pltpu
from jax.sharding import PartitionSpec as P

MESH = pl.DeviceIdType.MESH
F32 = jnp.float32
BF16 = jnp.bfloat16
HEAD = 64
NX = 4
NY = 4
LOW = -1e30
LOG2E = 1.4426950408889634
VROWS = 80
AT_ONCE = 4


def kernel(
    tokens,
    norm_gain,
    w_query,
    w_key,
    w_value,
    conv_in,
    conv_gate,
    taps_hbm,
    gain_hbm,
    cum_hbm,
    out_attn,
    out_conv,
    mixed,
    log_total,
    conv_taps,
    conv_gain,
    cum_gate,
    nt,
    wall,
    wo,
    wconv,
    qp,
    qb,
    ks,
    vs,
    kp,
    vp,
    cpad,
    mrow,
    acc,
    obuf,
    orecv,
    sbuf,
    srecv,
    gb,
    rim,
    cg,
    cv,
    sq,
    csq,
    xs,
    sb,
    rb,
    po,
    t2,
    r2r,
    r2l,
    sr,
    sl,
    frl,
    frr,
    at_out,
    at_in,
    lt_out,
    lt_in,
    wsem,
    gsend,
    grecv,
    wosend,
    worecv,
    ksend,
    krecv,
    vsend,
    vrecv,
    qsend,
    qrecv,
    qbsend,
    qbrecv,
    qrsend,
    qrrecv,
    msend,
    mrecv,
    osend,
    orecv_sem,
    csend,
    crecv,
    xsend,
    xrecv,
    asend,
    arecv,
    lsend,
    lrecv,
):
    s_me = lax.axis_index("sp")
    t_me = lax.axis_index("tp")
    nsp = lax.axis_size("sp")
    nz = nsp // NX
    z = s_me // NX
    x = s_me % NX
    y = t_me // 2
    c = t_me % 2
    rows = tokens.shape[0]
    half = rows // 2
    depth = tokens.shape[1]
    tok = rows * 8
    mid_tok = tok // 2
    zbar = nz - 1 - z
    hb = y // (NY // 2)
    ha = 1 - hb

    def at_tp(t):
        return (s_me, t)

    def at_sp(s):
        return (s, t_me)

    def rcopy(src, dst, ssem, rsem, dev):
        return pltpu.make_async_remote_copy(
            src_ref=src,
            dst_ref=dst,
            send_sem=ssem,
            recv_sem=rsem,
            device_id=dev,
            device_id_type=MESH,
        )

    wcopies = []
    at = 0
    for i, w in enumerate((w_query, w_key, w_value, conv_in, conv_gate)):
        n = w.shape[1]
        wcopies.append(pltpu.make_async_copy(w, wall.at[:, pl.ds(at, n)], wsem.at[i]))
        at += n
    ocopies = [
        pltpu.make_async_copy(out_attn, wo.at[t_me], wsem.at[5]),
        pltpu.make_async_copy(out_conv, wconv, wsem.at[6]),
    ]
    scopies = [
        pltpu.make_async_copy(src, dst, wsem.at[7 + i])
        for i, (src, dst) in enumerate(
            ((taps_hbm, conv_taps), (gain_hbm, conv_gain), (cum_hbm, cum_gate))
        )
    ]
    for w in wcopies + ocopies + scopies:
        w.start()

    barrier = pltpu.get_barrier_semaphore()
    for d in range(1, 8):
        pl.semaphore_signal(
            barrier, inc=1, device_id=at_tp((t_me + d) % 8), device_id_type=MESH
        )
    for d in range(1, NX):
        pl.semaphore_signal(
            barrier, inc=1, device_id=at_sp(z * NX + (x + d) % NX), device_id_type=MESH
        )
    for d in (1, nz - 1):
        pl.semaphore_signal(
            barrier, inc=1, device_id=at_sp(((z + d) % nz) * NX + x), device_id_type=MESH
        )
    for d in (1, nsp - 1):
        pl.semaphore_signal(
            barrier, inc=1, device_id=at_sp((s_me + d) % nsp), device_id_type=MESH
        )

    for t in range(8):
        pl.semaphore_signal(
            barrier, inc=1, device_id=(zbar * NX + x, t), device_id_type=MESH
        )

    wide = tokens[...].astype(F32)
    factor = lax.rsqrt(jnp.mean(wide * wide, axis=1, keepdims=True) + 1e-06)
    nt[t_me] = (wide * factor * norm_gain[...]).astype(BF16)
    qp[:, 0, HEAD:, :] = jnp.ones((NX, HEAD, tok), BF16)
    qp[:, 1, :HEAD, :] = jnp.ones((NX, HEAD, tok), BF16)
    vp[:, HEAD:, :] = jnp.ones((2, VROWS - HEAD, tok), BF16)
    cpad[...] = jnp.zeros_like(cpad)
    mrow[...] = jnp.full_like(mrow, LOW)
    acc[...] = jnp.zeros_like(acc)

    pl.semaphore_wait(barrier, 7 + NX - 1 + 4 + 8)

    sib = y * 2 + (1 - c)
    tr = ((y + 1) % NY) * 2 + c
    tl = ((y + NY - 1) % NY) * 2 + c
    to = ((y + 2) % NY) * 2 + c
    lo, hi = pl.ds(0, half), pl.ds(half, half)

    def gather_over_tp(buf, ssem, rsem):
        n = buf.shape[1] // 2
        first, last = pl.ds(0, n), pl.ds(n, n)

        def gcopy(k, src, part, dev):
            ref = buf.at[src] if part is None else buf.at[src, part]
            return rcopy(ref, ref, ssem.at[k], rsem.at[k], at_tp(dev))

        return [
            gcopy(0, t_me, None, sib),
            gcopy(1, t_me, first, tr),
            gcopy(2, t_me, last, tr),
            gcopy(3, t_me, last, tl),
            gcopy(4, t_me, first, tl),
            gcopy(5, tl, None, sib),
            gcopy(6, tr, None, sib),
            gcopy(7, tl, first, tr),
            gcopy(8, tr, last, tl),
            gcopy(9, to, first, sib),
            gcopy(10, to, last, sib),
        ]

    g = gather_over_tp(nt, gsend, grecv)
    gw = gather_over_tp(wo, wosend, worecv)
    for k in (1, 3, 2, 4, 0):
        g[k].start()

    def sp_of(zz):
        return at_sp(zz * NX + x)

    def landed(t, piece):
        return t if piece is None else 4 + 4 * t + piece

    def kcopy(zb, t, zt, part=None, piece=None):
        ref = ks.at[zb] if part is None else ks.at[zb, part]
        return rcopy(ref, ref, ksend.at[t], krecv.at[landed(t, piece)], sp_of(zt))

    def vcopy(zb, t, zt, part=None, piece=None):
        ref = vs.at[zb] if part is None else vs.at[zb, :, part]
        return rcopy(ref, ref, vsend.at[t], vrecv.at[landed(t, piece)], sp_of(zt))

    def pair(i):
        return (y + 2 * NY - (2 * (i % 2) - 1) * ((i + 1) // 2)) % NY

    def pair_rows(i):
        return pl.ds(pl.multiple_of(pair(i) * 2 * rows, 2 * rows), 2 * rows)

    def place(t):
        dr = 2 * (t % 2) - 1
        return dr, (z + nz - dr * ((t + 1) // 2)) % nz

    def delivered(kind, t):
        up, s = t % 2 == 1, (t + 1) // 2
        if t == nz - 1:
            up = kind == "k"
        last = nz // 2 if up == (kind == "k") else nz // 2 - 1
        rows_at = []
        for zz in range(nz):
            zb = (zz - s if up else zz + s) % nz
            behind = [(zz + k if up else zz - k) % nz for k in range(last - s + 1)]
            if any(zb <= max(r, nz - 1 - r) for r in behind):
                rows_at.append(zz)
        return rows_at

    def among(kind, t, zz):
        found = False
        for r in delivered(kind, t):
            found = found | (zz == r)
        return found

    def piece_on(kind, piece):
        copy = kcopy if kind == "k" else vcopy
        part = pair_rows(piece)
        for t in (1, 2):
            dr, zb = place(t)
            zt = (z + nz + dr) % nz

            @pl.when(among(kind, t, z))
            def _(t=t, zb=zb, zt=zt):
                copy(zb, t, zt, part, piece).wait_recv()

            @pl.when(among(kind, t + 2, zt))
            def _(t=t, zb=zb, zt=zt):
                copy(zb, t + 2, zt, part).start()

    low_half, high_half = pl.ds(0, mid_tok), pl.ds(mid_tok, mid_tok)

    def qcopies(src, d, lanes, ssem, rsem):
        dev = at_sp(z * NX + (x + d) % NX)
        a = qp.at[src, 0, pl.ds(0, HEAD), lanes]
        b = qp.at[src, 1, pl.ds(HEAD, HEAD), lanes]
        return (
            rcopy(a, a, ssem.at[2 * d - 2], rsem.at[2 * d - 2], dev),
            rcopy(b, b, ssem.at[2 * d - 1], rsem.at[2 * d - 1], dev),
        )

    def qbcopies(src, lanes):
        dev = sp_of(zbar)
        return (
            rcopy(
                qb.at[pl.ds(0, HEAD), src],
                qp.at[x, 0, pl.ds(0, HEAD), lanes],
                qbsend.at[0],
                qbrecv.at[0],
                dev,
            ),
            rcopy(
                qb.at[pl.ds(HEAD, HEAD), src],
                qp.at[x, 1, pl.ds(HEAD, HEAD), lanes],
                qbsend.at[1],
                qbrecv.at[1],
                dev,
            ),
        )

    rcopy_rim = rcopy(
        gb.at[pl.ds(tok - 32, 32)], rim, msend.at[0], mrecv.at[0], at_sp((s_me + 1) % nsp)
    )
    for w in wcopies + scopies:
        w.wait()

    def project(i, carry):
        @pl.when(i == 0)
        def _():
            g[0].wait_recv()

        @pl.when(i == 1)
        def _():
            g[1].wait_recv()
            g[7].start()
            g[3].wait_recv()
            g[8].start()
            g[2].wait_recv()
            g[5].start()
            g[4].wait_recv()
            g[6].start()
            piece_on("k", 0)
            piece_on("v", 0)
            g[5].wait_recv()

        @pl.when(i == 2)
        def _():
            g[6].wait_recv()

        @pl.when(i == 3)
        def _():
            g[7].wait_recv()
            g[9].start()
            g[8].wait_recv()
            g[10].start()
            g[9].wait_recv()
            g[10].wait_recv()

        p = pair(i)
        lhs = nt[pl.ds(2 * p, 2)].reshape(2 * rows, depth)
        res = jnp.dot(lhs, wall[...], preferred_element_type=F32)
        here = pair_rows(i)
        opened = res[:, 384:640]
        gating = res[:, 640:896]
        gate = (opened / (1.0 + jnp.exp(-gating))).astype(BF16)
        gb[here, :] = gate
        cg[pl.ds(pl.multiple_of(p * 2 * rows + 32, 32), 2 * rows), :] = gate.astype(F32)
        ks[z, here, :] = res[:, 128:256].astype(BF16)
        vs[z, :, here] = res[:, 256:384].T.astype(BF16)
        qt = (res[:, :128] * HEAD ** (-0.5)).T.astype(BF16)

        spot = pl.ds(pl.multiple_of((p % 2) * 2 * rows, 2 * rows), 2 * rows)
        over = pl.ds(pl.multiple_of((p % 2) * 2 * rows + mid_tok, 2 * rows), 2 * rows)

        @pl.when(p // 2 == hb)
        def _():
            qb[:, spot] = qt
            for q in qbcopies(spot, over):
                q.start()

        @pl.when(p == NY - 1)
        def _():
            rcopy_rim.start()

        for t, zt in ((1, (z + 1) % nz), (2, (z + nz - 1) % nz)):

            @pl.when(among("k", t, zt))
            def _(t=t, zt=zt):
                kcopy(z, t, zt, here, i).start()

            @pl.when(among("v", t, zt))
            def _(t=t, zt=zt):
                vcopy(z, t, zt, here, i).start()

        @pl.when(p // 2 == ha)
        def _():
            qp[x, 0, :HEAD, spot] = qt[:HEAD]
            qp[x, 1, HEAD:, spot] = qt[HEAD:]
            for d in (1, 3, 2):
                for q in qcopies(x, d, spot, qsend, qrecv):
                    q.start()

        return carry

    lax.fori_loop(0, NY, project, 0)

    piece_on("k", 1)
    piece_on("v", 1)

    def conv_rows(i, carry):
        r0 = pl.multiple_of(i * 64, 64)
        win = cg[pl.ds(r0, 96), :]
        total = jnp.zeros((64, win.shape[1]), F32)
        for b in range(8):
            turned = win if b == 0 else pltpu.roll(win, 96 - b, 0)
            for a in range(5):
                k = 8 * a + b - 2
                if 0 <= k < 31:
                    total = total + conv_taps[k : k + 1, :] * turned[8 * a : 8 * a + 64]
        cv[pl.ds(r0, 64), :] = total
        square = total * total
        sq[pl.ds(r0, 64), :] = square[:, :128] + square[:, 128:]
        return carry

    lax.fori_loop(1, tok // 64, conv_rows, 0)

    cref = cum_gate[:, pl.ds(pl.multiple_of(z * NX * tok, 128), 128)][:, :1]

    def prepare(zb):
        ck = cum_gate[:, pl.ds(pl.multiple_of((zb * NX + x) * tok, 128), tok)]
        bias = cref - ck
        high = bias.astype(BF16).astype(F32)
        left = bias - high
        mid = left.astype(BF16).astype(F32)
        low = left - mid
        rowid = lax.broadcasted_iota(jnp.int32, (8, tok), 0)
        for h, r0 in ((0, HEAD), (1, 0)):
            tile = jnp.where(
                rowid == 0,
                high[h : h + 1],
                jnp.where(
                    rowid == 1, mid[h : h + 1], jnp.where(rowid == 2, low[h : h + 1], 0.0)
                ),
            )
            cpad[r0 : r0 + 8, :] = tile
        extra = cpad[...].T
        kf = ks[zb].astype(F32)
        lane = lax.broadcasted_iota(jnp.int32, (tok, 2 * HEAD), 1)
        kp[0] = jnp.where(lane < HEAD, kf, extra).astype(BF16)
        kp[1] = jnp.where(lane < HEAD, extra, kf).astype(BF16)
        vp[0, :HEAD, :] = vs[zb, :HEAD, :]
        vp[1, :HEAD, :] = vs[zb, HEAD:, :]

    def chunks(js, g, masked):
        lanes = pl.ds(pl.multiple_of(g * mid_tok, mid_tok), mid_tok)
        units = [(j, h) for j in js for h in range(2)]
        old = [mrow[j, h, :, lanes] for j, h in units]
        held = [acc[j, h, :, lanes] for j, h in units]
        sc = [jnp.dot(kp[h], qp[j, h, :, lanes], preferred_element_type=F32) for j, h in units]
        if masked:
            kpos = lax.broadcasted_iota(jnp.int32, sc[0].shape, 0)
            qpos = lax.broadcasted_iota(jnp.int32, sc[0].shape, 1)
            ahead = kpos - qpos - (ha + g * (hb - ha)) * mid_tok
            sc = [jnp.where(ahead <= (j - x) * tok, v, LOW) for v, (j, _) in zip(sc, units)]
        new = [jnp.maximum(o, jnp.max(v, axis=0, keepdims=True)) for o, v in zip(old, sc)]
        wts = [jnp.exp2((v - n) * LOG2E).astype(BF16) for n, v in zip(new, sc)]
        shrink = [jnp.exp2((o - n) * LOG2E) for o, n in zip(old, new)]
        out = [
            a * k + jnp.dot(vp[h], w, preferred_element_type=F32)
            for a, k, w, (_, h) in zip(held, shrink, wts, units)
        ]
        for n, o, (j, h) in zip(new, out, units):
            mrow[j, h, :, lanes] = n
            acc[j, h, :, lanes] = o

    def ocopies_of(d, lanes, k):
        dev = at_sp(z * NX + (x + d) % NX)
        return (
            rcopy(
                obuf.at[d - 1, :, lanes],
                orecv.at[d - 1, :, lanes],
                osend.at[2 * k + 4 * (d - 1)],
                orecv_sem.at[2 * k + 4 * (d - 1)],
                dev,
            ),
            rcopy(
                sbuf.at[d - 1, :, lanes],
                srecv.at[d - 1, :, lanes],
                osend.at[2 * k + 4 * (d - 1) + 1],
                orecv_sem.at[2 * k + 4 * (d - 1) + 1],
                dev,
            ),
        )

    def final_at(zz, gg):
        zq = nz - 1 - zz if gg else zz
        order = [(zz - (2 * (t % 2) - 1) * ((t + 1) // 2)) % nz for t in range(nz)]
        return max(t for t in range(nz) if order[t] <= zq)

    def finish(t, g):
        done = False
        for zz in range(nz):
            for gg in range(2):
                done = done | ((z == zz) & (g == gg) & (t == final_at(zz, gg)))

        @pl.when(done)
        def _():
            lanes = pl.ds(pl.multiple_of(g * mid_tok, mid_tok), mid_tok)
            for d in (2, 1, 3):
                j = (x + d) % NX
                for h in range(2):
                    obuf[d - 1, h * HEAD : (h + 1) * HEAD, lanes] = acc[j, h, :HEAD, lanes].astype(
                        BF16
                    )
                    sbuf[d - 1, h : h + 1, lanes] = mrow[j, h, :, lanes]
                    sbuf[d - 1, 2 + h : 3 + h, lanes] = acc[j, h, HEAD : HEAD + 1, lanes]
                for cp in ocopies_of(d, lanes, g):
                    cp.start()

    def whole(g):
        def some(i, carry):
            chunks(tuple(i * AT_ONCE + k for k in range(AT_ONCE)), g, False)
            return carry

        lax.fori_loop(0, NX // AT_ONCE, some, 0)

    def diagonal(g):
        chunks(tuple(range(NX)), g, True)

    def tile(t):
        _, zb = place(t)

        @pl.when((zb <= z) | (zb <= zbar))
        def _():
            prepare(zb)

            def group(i, carry):
                g = i + (z // (nz // 2)) * (1 - 2 * i)
                zq = z + g * (nz - 1 - 2 * z)

                @pl.when(zb < zq)
                def _():
                    whole(g)

                @pl.when(zb == zq)
                def _():
                    diagonal(g)

                @pl.when(zb <= zq)
                def _():
                    finish(t, g)

                return carry

            lax.fori_loop(0, 2, group, 0)

    def keys_on(t):
        dr, zb = place(t)
        zt = (z + nz + dr) % nz

        @pl.when(among("k", t, z))
        def _():
            kcopy(zb, t, zt).wait_recv()

        if t <= 5:

            @pl.when(among("k", t + 2, zt))
            def _():
                kcopy(zb, t + 2, zt).start()

    def values_on(t):
        dr, zb = place(t)
        zt = (z + nz + dr) % nz

        @pl.when(among("v", t, z))
        def _():
            vcopy(zb, t, zt).wait_recv()

        if t <= 4 or t == 6:
            on = t + 2 - t // 6

            @pl.when(among("v", on, zt))
            def _():
                vcopy(zb, on, zt).start()

    near = (z % 4) * (3 - z % 4) == 0
    late = (z == 5) | (z == 6)

    def relay():
        for q in qbcopies(low_half, high_half):
            q.wait_recv()
        for d in (1, 3, 2):
            for q in qcopies(x, d, high_half, qrsend, qrrecv):
                q.start()

    def relayed():
        for d in range(1, NX):
            for q in qcopies(x, d, high_half, qrsend, qrrecv):
                q.wait_recv()

    @pl.when(near)
    def _():
        relay()

    for kind, piece in (("k", 2), ("v", 2), ("k", 3), ("v", 3)):
        piece_on(kind, piece)

    def project_out(which, emit):
        lhs = xs[which].reshape(NY * rows, xs.shape[3])

        def columns(n, carry):
            cols = pl.ds(pl.multiple_of(n * 512, 512), 512)
            res = jnp.dot(lhs, wconv[:, cols], preferred_element_type=F32)
            emit(cols, res)
            return carry

        lax.fori_loop(0, depth // 512, columns, 0)

    def emit_sib(cols, res):
        sb[:, :, cols] = res.astype(BF16).reshape(NY, rows, 512)

    def emit_own(cols, res):
        po[:, :, cols] = res.reshape(NY, rows, 512)

    ybits = [(y + k) % NY for k in range(NY)]

    def xcopy(k, src, dst, dev):
        return rcopy(src, dst, xsend.at[k], xrecv.at[k], at_tp(dev))

    bcopies = [xcopy(k, sb.at[ybits[k]], rb.at[ybits[k]], sib) for k in range(NY)]

    def conv_part():
        for cc in ccopies:
            cc.wait_recv()
        total = csq[0]
        for t in range(1, 8):
            total = total + csq[t]
        scale = lax.rsqrt(total / (8.0 * conv_gain.shape[1]) + 1e-06)
        sq[...] = jnp.broadcast_to(scale, (128, tok)).T
        for i in range(8):
            r = pl.ds(i * rows, rows)
            factor = sq[r, :]
            for b in range(2):
                lanes = pl.ds(b * 128, 128)
                v = cv[r, lanes] * factor * conv_gain[:, lanes]
                v = v / (1.0 + jnp.exp(-v))
                xs[i % 2, i // 2, :, lanes] = v.astype(BF16)
        ocopies[1].wait()

        project_out(1 - c, emit_sib)
        for k in (2, 1, 3, 0):
            bcopies[k].start()
        project_out(c, emit_own)

    far_r = xcopy(4, t2.at[lo], r2r, tr)
    far_l = xcopy(5, t2.at[hi], r2l, tl)
    near_r = xcopy(6, sr.at[hi], frl.at[hi], tr)
    near_l = xcopy(7, sl.at[lo], frr.at[lo], tl)
    both_r = xcopy(8, sr.at[lo], frl.at[lo], tr)
    both_l = xcopy(9, sl.at[hi], frr.at[hi], tl)

    def scatter_first():
        bcopies[2].wait_recv()
        t2[...] = (po[ybits[2]] + rb[ybits[2]].astype(F32)).astype(BF16)
        far_r.start()
        far_l.start()
        bcopies[1].wait_recv()
        sr[hi, :] = (po[ybits[1], hi] + rb[ybits[1], hi].astype(F32)).astype(BF16)
        near_r.start()
        bcopies[3].wait_recv()
        sl[lo, :] = (po[ybits[3], lo] + rb[ybits[3], lo].astype(F32)).astype(BF16)
        near_l.start()

    def scatter_second():
        far_r.wait_recv()
        sr[lo, :] = (
            po[ybits[1], lo] + rb[ybits[1], lo].astype(F32) + r2r[...].astype(F32)
        ).astype(BF16)
        both_r.start()
        far_l.wait_recv()
        sl[hi, :] = (
            po[ybits[3], hi] + rb[ybits[3], hi].astype(F32) + r2l[...].astype(F32)
        ).astype(BF16)
        both_l.start()
        bcopies[0].wait_recv()
        po[y] = po[y] + rb[y].astype(F32)

    def weights_on():
        for got, on in ((1, 7), (3, 8), (2, 5), (4, 6)):
            gw[got].wait_recv()
            gw[on].start()

    def weights_last():
        for got, on in ((7, 9), (8, 10)):
            gw[got].wait_recv()
            gw[on].start()

    rcopy_rim.wait_recv()
    first = jnp.where(s_me > 0, 1.0, 0.0).astype(F32)
    cg[0:32, :] = rim[...].astype(F32) * first
    conv_rows(0, 0)
    part = jnp.sum(sq[...].T, axis=0, keepdims=True)
    csq[t_me] = part
    ccopies = []
    for d in range(1, 8):
        cc = rcopy(
            csq.at[t_me], csq.at[t_me], csend.at[d], crecv.at[d], at_tp((t_me + d) % 8)
        )
        cc.start()
        ccopies.append(cc)
    ocopies[0].wait()
    for k in (1, 3, 2, 4, 0):
        gw[k].start()

    @pl.when(jnp.logical_not(near | late))
    def _():
        relay()

    for d in range(1, NX):
        for q in qcopies(x, d, low_half, qsend, qrecv):
            q.wait_recv()
    prepare(z)
    diagonal(0)
    finish(0, 0)
    @pl.when(late)
    def _():
        relay()

    keys_on(3)
    keys_on(4)
    @pl.when(jnp.logical_not(late))
    def _():
        relayed()

    @pl.when(z < zbar)
    def _():
        whole(1)

    mid_row = nz // 2

    @pl.when(z <= mid_row)
    def _():
        values_on(3)
        values_on(4)

    swap = ((z + 4) // nz) * ((2 * nz - 2 - z) // nz)

    def step(i, carry):
        early = (i // 2 % 2) * (1 - i // 4)
        is_two, is_three = early * (1 - i % 2), early * (i % 2)
        t = i + swap * (is_two - is_three)
        tile(t)

        @pl.when(i == 1)
        def _():
            @pl.when(z > mid_row)
            def _():
                values_on(3)
                values_on(4)

            @pl.when(z <= mid_row)
            def _():
                keys_on(5)
                keys_on(6)

            conv_part()
            @pl.when(z > mid_row)
            def _():
                keys_on(5)
                keys_on(6)


        @pl.when(i == 2)
        def _():
            values_on(5)
            values_on(6)
            scatter_first()

        @pl.when((i == 3) & late)
        def _():
            relayed()

        @pl.when(i == 4)
        def _():
            weights_on()

        @pl.when(i == 6)
        def _():
            keys_on(7)
            values_on(7)
            scatter_second()

        return carry

    lax.fori_loop(1, nz, step, 0)


    for d in range(1, NX):
        for k, lanes in enumerate((low_half, high_half)):
            for cp in ocopies_of(d, lanes, k):
                cp.wait_recv()
    for h in range(2):
        best = mrow[x, h]
        for d in range(1, NX):
            best = jnp.maximum(best, srecv[d - 1, h : h + 1, :])
        share = jnp.exp2((mrow[x, h] - best) * LOG2E)
        summed = acc[x, h, HEAD : HEAD + 1, :] * share
        value = acc[x, h, :HEAD, :] * share
        for d in range(1, NX):
            share = jnp.exp2((srecv[d - 1, h : h + 1, :] - best) * LOG2E)
            summed = summed + srecv[d - 1, 2 + h : 3 + h, :] * share
            value = value + orecv[d - 1, h * HEAD : (h + 1) * HEAD, :].astype(F32) * share
        cpad[h * HEAD : (h + 1) * HEAD, :] = value / summed
        level = best + jnp.log(summed) - cref[h : h + 1]
        for zz, part, lanes, dst, at in (
            (z, ha, low_half, log_total, pl.multiple_of(ha * mid_tok, mid_tok)),
            (zbar, hb, high_half, lt_out, 0),
        ):
            here = pl.multiple_of((zz * NX + x) * tok + part * mid_tok, 128)
            dst[h : h + 1, pl.ds(at, mid_tok)] = (
                level[:, lanes.start : lanes.start + mid_tok]
                + cum_gate[:, pl.ds(here, mid_tok)][h : h + 1]
            )
    at_out[...] = cpad[...].T.astype(BF16).reshape(8, rows, 2 * HEAD)

    mine = at_in.at[:, pl.ds(pl.multiple_of(t_me * 2 * HEAD, 2 * HEAD), 2 * HEAD)]
    lcopy = rcopy(lt_out, lt_in, lsend.at[0], lrecv.at[0], sp_of(zbar))

    def acopy(k):
        zz, owner = (z, 4 * ha + k) if k < 4 else (zbar, 4 * hb + k - 4)
        return rcopy(at_out.at[k], mine, asend.at[k], arecv.at[t_me], (zz * NX + x, owner))

    for k in (4, 5, 6, 7, 0, 1, 2, 3):
        acopy(k).start()
    lcopy.start()

    weights_last()
    for k in (0, 5, 6, 9, 10):
        gw[k].wait_recv()
    near_r.wait_recv()
    near_l.wait_recv()
    both_r.wait_recv()
    both_l.wait_recv()
    po[y] = po[y] + frl[...].astype(F32) + frr[...].astype(F32)
    for t in range(8):
        rcopy(
            at_out.at[0],
            at_in.at[:, pl.ds(t * 2 * HEAD, 2 * HEAD)],
            asend.at[0],
            arecv.at[t],
            sp_of(zbar),
        ).wait_recv()

    lhs = at_in[...]

    lcopy.wait_recv()
    log_total[:, pl.ds(pl.multiple_of(hb * mid_tok, mid_tok), mid_tok)] = lt_in[0:2, :]

    def last(n, carry):
        cols = pl.ds(pl.multiple_of(n * 512, 512), 512)
        w = wo[:, :, cols].reshape(lhs.shape[1], 512)
        res = jnp.dot(lhs, w, preferred_element_type=F32)
        mixed[:, cols] = (po[y, :, cols] + res).astype(BF16)
        return carry

    lax.fori_loop(0, depth // 512, last, 0)

    for cp in g + gw:
        cp.wait_send()
    for t in range(1, 8):
        above, below = (z + 1) % nz, (z + nz - 1) % nz

        @pl.when(among("k", t, above if t % 2 else below))
        def _(t=t, above=above):
            kcopy(z, t, above).wait_send()

        @pl.when(among("v", t, above if t % 2 and t < nz - 1 else below))
        def _(t=t, above=above):
            vcopy(z, t, above).wait_send()

    for d in range(1, NX):
        for q in qcopies(x, d, low_half, qsend, qrecv) + qcopies(x, d, high_half, qrsend, qrrecv):
            q.wait_send()
    for q in qbcopies(low_half, high_half):
        q.wait_send()
    rcopy_rim.wait_send()
    for d in range(1, NX):
        for k, lanes in enumerate((low_half, high_half)):
            for cp in ocopies_of(d, lanes, k):
                cp.wait_send()
    for cp in ccopies + bcopies:
        cp.wait_send()
    for cp in (far_r, far_l, near_r, near_l, both_r, both_l, lcopy):
        cp.wait_send()
    for k in range(8):
        acopy(k).wait_send()


def per_device(*args):
    tokens = args[0]
    rows, depth = tokens.shape
    tok = rows * 8
    nz = lax.axis_size("sp") // NX
    att = args[2].shape[1]
    ch = args[5].shape[1]
    wide = 3 * att + 2 * ch
    ops = list(args)
    ops[1] = args[1][None]
    ops[8] = args[8][None]
    vmem = pl.BlockSpec(memory_space=pltpu.VMEM)
    hbm = pl.BlockSpec(memory_space=pltpu.HBM)
    specs = [vmem, vmem] + [hbm] * 10
    dma = pltpu.SemaphoreType.DMA
    scratch = [
        pltpu.VMEM(args[7].shape, F32),
        pltpu.VMEM((1, ch), F32),
        pltpu.VMEM(args[9].shape, F32),
        pltpu.VMEM((8, rows, depth), BF16),
        pltpu.VMEM((depth, wide), BF16),
        pltpu.VMEM((8, att, depth), BF16),
        pltpu.VMEM((ch, depth), BF16),
        pltpu.VMEM((NX, 2, att, tok), BF16),
        pltpu.VMEM((att, tok // 2), BF16),
        pltpu.VMEM((nz, tok, att), BF16),
        pltpu.VMEM((nz, att, tok), BF16),
        pltpu.VMEM((2, tok, att), BF16),
        pltpu.VMEM((2, VROWS, tok), BF16),
        pltpu.VMEM((att, tok), F32),
        pltpu.VMEM((NX, 2, 1, tok), F32),
        pltpu.VMEM((NX, 2, VROWS, tok), F32),
        pltpu.VMEM((NX - 1, att, tok), BF16),
        pltpu.VMEM((NX - 1, att, tok), BF16),
        pltpu.VMEM((NX - 1, 8, tok), F32),
        pltpu.VMEM((NX - 1, 8, tok), F32),
        pltpu.VMEM((tok, ch), BF16),
        pltpu.VMEM((32, ch), BF16),
        pltpu.VMEM((tok + 32, ch), F32),
        pltpu.VMEM((tok, ch), F32),
        pltpu.VMEM((tok, 128), F32),
        pltpu.VMEM((8, 1, tok), F32),
        pltpu.VMEM((2, NY, rows, ch), BF16),
        pltpu.VMEM((NY, rows, depth), BF16),
        pltpu.VMEM((NY, rows, depth), BF16),
        pltpu.VMEM((NY, rows, depth), F32),
        pltpu.VMEM((rows, depth), BF16),
        pltpu.VMEM((rows // 2, depth), BF16),
        pltpu.VMEM((rows // 2, depth), BF16),
        pltpu.VMEM((rows, depth), BF16),
        pltpu.VMEM((rows, depth), BF16),
        pltpu.VMEM((rows, depth), BF16),
        pltpu.VMEM((rows, depth), BF16),
        pltpu.VMEM((8, rows, att), BF16),
        pltpu.VMEM((rows, 8 * att), BF16),
        pltpu.VMEM((8, tok // 2), F32),
        pltpu.VMEM((8, tok // 2), F32),
    ] + [dma((n,)) for n in (10, 11, 11, 11, 11, 8, 16, 8, 16, 6, 6, 2, 2, 6, 6, 1, 1, 12, 12, 8, 8, 10, 10, 8, 8, 1, 1)]
    return pl.pallas_call(
        kernel,
        out_shape=(
            pltpu.VMEM((rows, depth), BF16),
            pltpu.VMEM((2, tok), F32),
        ),
        in_specs=specs,
        out_specs=(vmem, vmem),
        scratch_shapes=scratch,
        compiler_params=pltpu.CompilerParams(
            collective_id=0, has_side_effects=True, vmem_limit_bytes=58 * 1024 * 1024
        ),
        name="layer",
    )(*ops)


def solution(mesh):
    in_specs = (
        P(("sp", "tp"), None),
        P(),
        P(None, "tp"),
        P(None, "tp"),
        P(None, "tp"),
        P(None, "tp"),
        P(None, "tp"),
        P(None, "tp"),
        P("tp"),
        P("tp", None),
        P("tp", None),
        P("tp", None),
    )
    out_specs = (P(("sp", "tp"), None), P("tp", "sp"))
    return jax.shard_map(
        per_device, mesh=mesh, in_specs=in_specs, out_specs=out_specs, check_vma=False
    )
```

```python
import functools

import jax
import jax.numpy as jnp
from jax import lax
from jax.experimental import pallas as pl
from jax.experimental.pallas import tpu as pltpu
from jax.sharding import PartitionSpec as P

MESH = pl.DeviceIdType.MESH
F32 = jnp.float32
BF16 = jnp.bfloat16
HEAD = 64
NX = 4
NY = 4
LOW = -1e30
LOG2E = 1.4426950408889634
VROWS = 80
AT_ONCE = 4


def kernel(
    tokens,
    norm_gain,
    w_query,
    w_key,
    w_value,
    conv_in,
    conv_gate,
    taps_hbm,
    gain_hbm,
    cum_hbm,
    out_attn,
    out_conv,
    mixed,
    log_total,
    conv_taps,
    conv_gain,
    cum_gate,
    nt,
    wall,
    wo,
    wconv,
    qp,
    qb,
    ks,
    vs,
    kp,
    vp,
    cpad,
    mrow,
    acc,
    obuf,
    orecv,
    sbuf,
    srecv,
    gb,
    rim,
    cg,
    cv,
    sq,
    csq,
    xs,
    sb,
    rb,
    po,
    t2,
    r2r,
    r2l,
    sr,
    sl,
    frl,
    frr,
    at_out,
    at_in,
    lt_out,
    lt_in,
    wsem,
    gsend,
    grecv,
    wosend,
    worecv,
    ksend,
    krecv,
    vsend,
    vrecv,
    qsend,
    qrecv,
    qbsend,
    qbrecv,
    qrsend,
    qrrecv,
    msend,
    mrecv,
    osend,
    orecv_sem,
    csend,
    crecv,
    xsend,
    xrecv,
    asend,
    arecv,
    lsend,
    lrecv,
):
    s_me = lax.axis_index("sp")
    t_me = lax.axis_index("tp")
    nsp = lax.axis_size("sp")
    nz = nsp // NX
    z = s_me // NX
    x = s_me % NX
    y = t_me // 2
    c = t_me % 2
    rows = tokens.shape[0]
    half = rows // 2
    depth = tokens.shape[1]
    tok = rows * 8
    mid_tok = tok // 2
    zbar = nz - 1 - z
    hb = y // (NY // 2)
    ha = 1 - hb

    def at_tp(t):
        return (s_me, t)

    def at_sp(s):
        return (s, t_me)

    def rcopy(src, dst, ssem, rsem, dev):
        return pltpu.make_async_remote_copy(
            src_ref=src,
            dst_ref=dst,
            send_sem=ssem,
            recv_sem=rsem,
            device_id=dev,
            device_id_type=MESH,
        )

    wcopies = []
    at = 0
    for i, w in enumerate((w_key, w_value, w_query, conv_in, conv_gate)):
        n = w.shape[1]
        wcopies.append(pltpu.make_async_copy(w, wall.at[:, pl.ds(at, n)], wsem.at[i]))
        at += n
    ocopies = [
        pltpu.make_async_copy(out_attn, wo.at[t_me], wsem.at[5]),
        pltpu.make_async_copy(out_conv, wconv, wsem.at[6]),
    ]
    scopies = [
        pltpu.make_async_copy(src, dst, wsem.at[7 + i])
        for i, (src, dst) in enumerate(
            ((taps_hbm, conv_taps), (gain_hbm, conv_gain), (cum_hbm, cum_gate))
        )
    ]
    for w in wcopies + ocopies + scopies:
        w.start()

    barrier = pltpu.get_barrier_semaphore()
    for d in range(1, 8):
        pl.semaphore_signal(
            barrier, inc=1, device_id=at_tp((t_me + d) % 8), device_id_type=MESH
        )
    for d in range(1, NX):
        pl.semaphore_signal(
            barrier, inc=1, device_id=at_sp(z * NX + (x + d) % NX), device_id_type=MESH
        )
    for d in (1, nz - 1):
        pl.semaphore_signal(
            barrier, inc=1, device_id=at_sp(((z + d) % nz) * NX + x), device_id_type=MESH
        )
    for d in (1, nsp - 1):
        pl.semaphore_signal(
            barrier, inc=1, device_id=at_sp((s_me + d) % nsp), device_id_type=MESH
        )

    for t in range(8):
        pl.semaphore_signal(
            barrier, inc=1, device_id=(zbar * NX + x, t), device_id_type=MESH
        )

    wide = tokens[...].astype(F32)
    factor = lax.rsqrt(jnp.mean(wide * wide, axis=1, keepdims=True) + 1e-06)
    nt[t_me] = (wide * factor * norm_gain[...]).astype(BF16)
    qp[:, 0, HEAD:, :] = jnp.ones((NX, HEAD, tok), BF16)
    qp[:, 1, :HEAD, :] = jnp.ones((NX, HEAD, tok), BF16)
    vp[:, HEAD:, :] = jnp.ones((2, VROWS - HEAD, tok), BF16)
    cpad[...] = jnp.zeros_like(cpad)
    mrow[...] = jnp.full_like(mrow, LOW)
    acc[...] = jnp.zeros_like(acc)

    pl.semaphore_wait(barrier, 7 + NX - 1 + 4 + 8)

    sib = y * 2 + (1 - c)
    tr = ((y + 1) % NY) * 2 + c
    tl = ((y + NY - 1) % NY) * 2 + c
    to = ((y + 2) % NY) * 2 + c
    lo, hi = pl.ds(0, half), pl.ds(half, half)

    def gather_over_tp(buf, ssem, rsem):
        n = buf.shape[1] // 2
        first, last = pl.ds(0, n), pl.ds(n, n)

        def gcopy(k, src, part, dev):
            ref = buf.at[src] if part is None else buf.at[src, part]
            return rcopy(ref, ref, ssem.at[k], rsem.at[k], at_tp(dev))

        return [
            gcopy(0, t_me, None, sib),
            gcopy(1, t_me, first, tr),
            gcopy(2, t_me, last, tr),
            gcopy(3, t_me, last, tl),
            gcopy(4, t_me, first, tl),
            gcopy(5, tl, None, sib),
            gcopy(6, tr, None, sib),
            gcopy(7, tl, first, tr),
            gcopy(8, tr, last, tl),
            gcopy(9, to, first, sib),
            gcopy(10, to, last, sib),
        ]

    g = gather_over_tp(nt, gsend, grecv)
    gw = gather_over_tp(wo, wosend, worecv)
    for k in (1, 3, 2, 4, 0):
        g[k].start()

    def sp_of(zz):
        return at_sp(zz * NX + x)

    def landed(t, piece):
        return t if piece is None else 4 + 4 * t + piece

    def kcopy(zb, t, zt, part=None, piece=None):
        ref = ks.at[zb] if part is None else ks.at[zb, part]
        return rcopy(ref, ref, ksend.at[t], krecv.at[landed(t, piece)], sp_of(zt))

    def vcopy(zb, t, zt, part=None, piece=None):
        ref = vs.at[zb] if part is None else vs.at[zb, :, part]
        return rcopy(ref, ref, vsend.at[t], vrecv.at[landed(t, piece)], sp_of(zt))

    def pair(i):
        return (y + 2 * NY - (2 * (i % 2) - 1) * ((i + 1) // 2)) % NY

    def pair_rows(i):
        return pl.ds(pl.multiple_of(pair(i) * 2 * rows, 2 * rows), 2 * rows)

    def place(t):
        dr = 2 * (t % 2) - 1
        return dr, (z + nz - dr * ((t + 1) // 2)) % nz

    def delivered(kind, t):
        up, s = t % 2 == 1, (t + 1) // 2
        if t == nz - 1:
            up = kind == "k"
        last = nz // 2 if up == (kind == "k") else nz // 2 - 1
        rows_at = []
        for zz in range(nz):
            zb = (zz - s if up else zz + s) % nz
            behind = [(zz + k if up else zz - k) % nz for k in range(last - s + 1)]
            if any(zb <= max(r, nz - 1 - r) for r in behind):
                rows_at.append(zz)
        return rows_at

    def among(kind, t, zz):
        found = False
        for r in delivered(kind, t):
            found = found | (zz == r)
        return found

    def piece_on(kind, piece):
        copy = kcopy if kind == "k" else vcopy
        part = pair_rows(piece)
        for t in (1, 2):
            dr, zb = place(t)
            zt = (z + nz + dr) % nz

            @pl.when(among(kind, t, z))
            def _(t=t, zb=zb, zt=zt):
                copy(zb, t, zt, part, piece).wait_recv()

            @pl.when(among(kind, t + 2, zt))
            def _(t=t, zb=zb, zt=zt):
                copy(zb, t + 2, zt, part).start()

    low_half, high_half = pl.ds(0, mid_tok), pl.ds(mid_tok, mid_tok)

    def qcopies(src, d, lanes, ssem, rsem):
        dev = at_sp(z * NX + (x + d) % NX)
        a = qp.at[src, 0, pl.ds(0, HEAD), lanes]
        b = qp.at[src, 1, pl.ds(HEAD, HEAD), lanes]
        return (
            rcopy(a, a, ssem.at[2 * d - 2], rsem.at[2 * d - 2], dev),
            rcopy(b, b, ssem.at[2 * d - 1], rsem.at[2 * d - 1], dev),
        )

    def qbcopies(src, lanes):
        dev = sp_of(zbar)
        return (
            rcopy(
                qb.at[pl.ds(0, HEAD), src],
                qp.at[x, 0, pl.ds(0, HEAD), lanes],
                qbsend.at[0],
                qbrecv.at[0],
                dev,
            ),
            rcopy(
                qb.at[pl.ds(HEAD, HEAD), src],
                qp.at[x, 1, pl.ds(HEAD, HEAD), lanes],
                qbsend.at[1],
                qbrecv.at[1],
                dev,
            ),
        )

    rcopy_rim = rcopy(
        gb.at[pl.ds(tok - 32, 32)], rim, msend.at[0], mrecv.at[0], at_sp((s_me + 1) % nsp)
    )
    for w in wcopies + scopies:
        w.wait()

    def project(i, carry):
        @pl.when(i == 0)
        def _():
            g[0].wait_recv()

        @pl.when(i == 1)
        def _():
            g[1].wait_recv()
            g[7].start()
            g[3].wait_recv()
            g[8].start()
            g[2].wait_recv()
            g[5].start()
            g[4].wait_recv()
            g[6].start()
            piece_on("k", 0)
            piece_on("v", 0)
            g[5].wait_recv()

        @pl.when(i == 2)
        def _():
            g[6].wait_recv()

        @pl.when(i == 3)
        def _():
            g[7].wait_recv()
            g[9].start()
            g[8].wait_recv()
            g[10].start()
            g[9].wait_recv()
            g[10].wait_recv()

        p = pair(i)
        lhs = nt[pl.ds(2 * p, 2)].reshape(2 * rows, depth)
        here = pair_rows(i)
        kv = jnp.dot(lhs, wall[:, :256], preferred_element_type=F32)
        ks[z, here, :] = kv[:, :128].astype(BF16)
        vs[z, :, here] = kv[:, 128:].T.astype(BF16)
        for t, zt in ((1, (z + 1) % nz), (2, (z + nz - 1) % nz)):

            @pl.when(among("k", t, zt))
            def _(t=t, zt=zt):
                kcopy(z, t, zt, here, i).start()

            @pl.when(among("v", t, zt))
            def _(t=t, zt=zt):
                vcopy(z, t, zt, here, i).start()

        res = jnp.dot(lhs, wall[:, 256:], preferred_element_type=F32)
        opened = res[:, 128:384]
        gating = res[:, 384:640]
        gate = (opened / (1.0 + jnp.exp(-gating))).astype(BF16)
        gb[here, :] = gate
        cg[pl.ds(pl.multiple_of(pair(i) * 2 * rows + 32, 32), 2 * rows), :] = gate.astype(F32)
        qt = (res[:, :128] * HEAD ** (-0.5)).T.astype(BF16)

        spot = pl.ds(pl.multiple_of((p % 2) * 2 * rows, 2 * rows), 2 * rows)
        over = pl.ds(pl.multiple_of((p % 2) * 2 * rows + mid_tok, 2 * rows), 2 * rows)

        @pl.when(p // 2 == hb)
        def _():
            qb[:, spot] = qt
            for q in qbcopies(spot, over):
                q.start()

        @pl.when(p == NY - 1)
        def _():
            rcopy_rim.start()

        @pl.when(p // 2 == ha)
        def _():
            qp[x, 0, :HEAD, spot] = qt[:HEAD]
            qp[x, 1, HEAD:, spot] = qt[HEAD:]
            for d in (1, 3, 2):
                for q in qcopies(x, d, spot, qsend, qrecv):
                    q.start()

        return carry

    lax.fori_loop(0, NY, project, 0)

    piece_on("k", 1)
    piece_on("v", 1)

    def conv_rows(i, carry):
        r0 = pl.multiple_of(i * 64, 64)
        win = cg[pl.ds(r0, 96), :]
        total = jnp.zeros((64, win.shape[1]), F32)
        for b in range(8):
            turned = win if b == 0 else pltpu.roll(win, 96 - b, 0)
            for a in range(5):
                k = 8 * a + b - 2
                if 0 <= k < 31:
                    total = total + conv_taps[k : k + 1, :] * turned[8 * a : 8 * a + 64]
        cv[pl.ds(r0, 64), :] = total
        square = total * total
        sq[pl.ds(r0, 64), :] = square[:, :128] + square[:, 128:]
        return carry

    lax.fori_loop(1, tok // 64, conv_rows, 0)

    cref = cum_gate[:, pl.ds(pl.multiple_of(z * NX * tok, 128), 128)][:, :1]

    def prepare(zb):
        ck = cum_gate[:, pl.ds(pl.multiple_of((zb * NX + x) * tok, 128), tok)]
        bias = cref - ck
        high = bias.astype(BF16).astype(F32)
        left = bias - high
        mid = left.astype(BF16).astype(F32)
        low = left - mid
        rowid = lax.broadcasted_iota(jnp.int32, (8, tok), 0)
        for h, r0 in ((0, HEAD), (1, 0)):
            tile = jnp.where(
                rowid == 0,
                high[h : h + 1],
                jnp.where(
                    rowid == 1, mid[h : h + 1], jnp.where(rowid == 2, low[h : h + 1], 0.0)
                ),
            )
            cpad[r0 : r0 + 8, :] = tile
        extra = cpad[...].T
        kf = ks[zb].astype(F32)
        lane = lax.broadcasted_iota(jnp.int32, (tok, 2 * HEAD), 1)
        kp[0] = jnp.where(lane < HEAD, kf, extra).astype(BF16)
        kp[1] = jnp.where(lane < HEAD, extra, kf).astype(BF16)
        vp[0, :HEAD, :] = vs[zb, :HEAD, :]
        vp[1, :HEAD, :] = vs[zb, HEAD:, :]

    def chunks(js, g, masked):
        lanes = pl.ds(pl.multiple_of(g * mid_tok, mid_tok), mid_tok)
        units = [(j, h) for j in js for h in range(2)]
        old = [mrow[j, h, :, lanes] for j, h in units]
        held = [acc[j, h, :, lanes] for j, h in units]
        sc = [jnp.dot(kp[h], qp[j, h, :, lanes], preferred_element_type=F32) for j, h in units]
        if masked:
            kpos = lax.broadcasted_iota(jnp.int32, sc[0].shape, 0)
            qpos = lax.broadcasted_iota(jnp.int32, sc[0].shape, 1)
            ahead = kpos - qpos - (ha + g * (hb - ha)) * mid_tok
            sc = [jnp.where(ahead <= (j - x) * tok, v, LOW) for v, (j, _) in zip(sc, units)]
        new = [jnp.maximum(o, jnp.max(v, axis=0, keepdims=True)) for o, v in zip(old, sc)]
        wts = [jnp.exp2((v - n) * LOG2E).astype(BF16) for n, v in zip(new, sc)]
        shrink = [jnp.exp2((o - n) * LOG2E) for o, n in zip(old, new)]
        out = [
            a * k + jnp.dot(vp[h], w, preferred_element_type=F32)
            for a, k, w, (_, h) in zip(held, shrink, wts, units)
        ]
        for n, o, (j, h) in zip(new, out, units):
            mrow[j, h, :, lanes] = n
            acc[j, h, :, lanes] = o

    def ocopies_of(d, lanes, k):
        dev = at_sp(z * NX + (x + d) % NX)
        return (
            rcopy(
                obuf.at[d - 1, :, lanes],
                orecv.at[d - 1, :, lanes],
                osend.at[2 * k + 4 * (d - 1)],
                orecv_sem.at[2 * k + 4 * (d - 1)],
                dev,
            ),
            rcopy(
                sbuf.at[d - 1, :, lanes],
                srecv.at[d - 1, :, lanes],
                osend.at[2 * k + 4 * (d - 1) + 1],
                orecv_sem.at[2 * k + 4 * (d - 1) + 1],
                dev,
            ),
        )

    def final_at(zz, gg):
        zq = nz - 1 - zz if gg else zz
        order = [(zz - (2 * (t % 2) - 1) * ((t + 1) // 2)) % nz for t in range(nz)]
        return max(t for t in range(nz) if order[t] <= zq)

    def finish(t, g):
        done = False
        for zz in range(nz):
            for gg in range(2):
                done = done | ((z == zz) & (g == gg) & (t == final_at(zz, gg)))

        @pl.when(done)
        def _():
            lanes = pl.ds(pl.multiple_of(g * mid_tok, mid_tok), mid_tok)
            for d in (2, 1, 3):
                j = (x + d) % NX
                for h in range(2):
                    obuf[d - 1, h * HEAD : (h + 1) * HEAD, lanes] = acc[j, h, :HEAD, lanes].astype(
                        BF16
                    )
                    sbuf[d - 1, h : h + 1, lanes] = mrow[j, h, :, lanes]
                    sbuf[d - 1, 2 + h : 3 + h, lanes] = acc[j, h, HEAD : HEAD + 1, lanes]
                for cp in ocopies_of(d, lanes, g):
                    cp.start()

    def whole(g):
        def some(i, carry):
            chunks(tuple(i * AT_ONCE + k for k in range(AT_ONCE)), g, False)
            return carry

        lax.fori_loop(0, NX // AT_ONCE, some, 0)

    def diagonal(g):
        chunks(tuple(range(NX)), g, True)

    def tile(t):
        _, zb = place(t)

        @pl.when((zb <= z) | (zb <= zbar))
        def _():
            prepare(zb)

            def group(i, carry):
                g = i + (z // (nz // 2)) * (1 - 2 * i)
                zq = z + g * (nz - 1 - 2 * z)

                @pl.when(zb < zq)
                def _():
                    whole(g)

                @pl.when(zb == zq)
                def _():
                    diagonal(g)

                @pl.when(zb <= zq)
                def _():
                    finish(t, g)

                return carry

            lax.fori_loop(0, 2, group, 0)

    def keys_on(t):
        dr, zb = place(t)
        zt = (z + nz + dr) % nz

        @pl.when(among("k", t, z))
        def _():
            kcopy(zb, t, zt).wait_recv()

        if t <= 5:

            @pl.when(among("k", t + 2, zt))
            def _():
                kcopy(zb, t + 2, zt).start()

    def values_on(t):
        dr, zb = place(t)
        zt = (z + nz + dr) % nz

        @pl.when(among("v", t, z))
        def _():
            vcopy(zb, t, zt).wait_recv()

        if t <= 4 or t == 6:
            on = t + 2 - t // 6

            @pl.when(among("v", on, zt))
            def _():
                vcopy(zb, on, zt).start()

    near = (z % 4) * (3 - z % 4) == 0
    late = (z == 5) | (z == 6)

    def relay():
        for q in qbcopies(low_half, high_half):
            q.wait_recv()
        for d in (1, 3, 2):
            for q in qcopies(x, d, high_half, qrsend, qrrecv):
                q.start()

    def relayed():
        for d in range(1, NX):
            for q in qcopies(x, d, high_half, qrsend, qrrecv):
                q.wait_recv()

    @pl.when(near)
    def _():
        relay()

    for kind, piece in (("k", 2), ("v", 2), ("k", 3), ("v", 3)):
        piece_on(kind, piece)

    def project_out(which, emit):
        lhs = xs[which].reshape(NY * rows, xs.shape[3])

        def columns(n, carry):
            cols = pl.ds(pl.multiple_of(n * 512, 512), 512)
            res = jnp.dot(lhs, wconv[:, cols], preferred_element_type=F32)
            emit(cols, res)
            return carry

        lax.fori_loop(0, depth // 512, columns, 0)

    def emit_sib(cols, res):
        sb[:, :, cols] = res.astype(BF16).reshape(NY, rows, 512)

    def emit_own(cols, res):
        po[:, :, cols] = res.reshape(NY, rows, 512)

    ybits = [(y + k) % NY for k in range(NY)]

    def xcopy(k, src, dst, dev):
        return rcopy(src, dst, xsend.at[k], xrecv.at[k], at_tp(dev))

    bcopies = [xcopy(k, sb.at[ybits[k]], rb.at[ybits[k]], sib) for k in range(NY)]

    def conv_part():
        for cc in ccopies:
            cc.wait_recv()
        total = csq[0]
        for t in range(1, 8):
            total = total + csq[t]
        scale = lax.rsqrt(total / (8.0 * conv_gain.shape[1]) + 1e-06)
        sq[...] = jnp.broadcast_to(scale, (128, tok)).T
        for i in range(8):
            r = pl.ds(i * rows, rows)
            factor = sq[r, :]
            for b in range(2):
                lanes = pl.ds(b * 128, 128)
                v = cv[r, lanes] * factor * conv_gain[:, lanes]
                v = v / (1.0 + jnp.exp(-v))
                xs[i % 2, i // 2, :, lanes] = v.astype(BF16)
        ocopies[1].wait()

        project_out(1 - c, emit_sib)
        for k in (2, 1, 3, 0):
            bcopies[k].start()
        project_out(c, emit_own)

    far_r = xcopy(4, t2.at[lo], r2r, tr)
    far_l = xcopy(5, t2.at[hi], r2l, tl)
    near_r = xcopy(6, sr.at[hi], frl.at[hi], tr)
    near_l = xcopy(7, sl.at[lo], frr.at[lo], tl)
    both_r = xcopy(8, sr.at[lo], frl.at[lo], tr)
    both_l = xcopy(9, sl.at[hi], frr.at[hi], tl)

    def scatter_first():
        bcopies[2].wait_recv()
        t2[...] = (po[ybits[2]] + rb[ybits[2]].astype(F32)).astype(BF16)
        far_r.start()
        far_l.start()
        bcopies[1].wait_recv()
        sr[hi, :] = (po[ybits[1], hi] + rb[ybits[1], hi].astype(F32)).astype(BF16)
        near_r.start()
        bcopies[3].wait_recv()
        sl[lo, :] = (po[ybits[3], lo] + rb[ybits[3], lo].astype(F32)).astype(BF16)
        near_l.start()

    def scatter_second():
        far_r.wait_recv()
        sr[lo, :] = (
            po[ybits[1], lo] + rb[ybits[1], lo].astype(F32) + r2r[...].astype(F32)
        ).astype(BF16)
        both_r.start()
        far_l.wait_recv()
        sl[hi, :] = (
            po[ybits[3], hi] + rb[ybits[3], hi].astype(F32) + r2l[...].astype(F32)
        ).astype(BF16)
        both_l.start()
        bcopies[0].wait_recv()
        po[y] = po[y] + rb[y].astype(F32)

    def weights_on():
        for got, on in ((1, 7), (3, 8), (2, 5), (4, 6)):
            gw[got].wait_recv()
            gw[on].start()

    def weights_last():
        for got, on in ((7, 9), (8, 10)):
            gw[got].wait_recv()
            gw[on].start()

    rcopy_rim.wait_recv()
    first = jnp.where(s_me > 0, 1.0, 0.0).astype(F32)
    cg[0:32, :] = rim[...].astype(F32) * first
    conv_rows(0, 0)
    part = jnp.sum(sq[...].T, axis=0, keepdims=True)
    csq[t_me] = part
    ccopies = []
    for d in range(1, 8):
        cc = rcopy(
            csq.at[t_me], csq.at[t_me], csend.at[d], crecv.at[d], at_tp((t_me + d) % 8)
        )
        cc.start()
        ccopies.append(cc)
    ocopies[0].wait()
    for k in (1, 3, 2, 4, 0):
        gw[k].start()

    @pl.when(jnp.logical_not(near | late))
    def _():
        relay()

    for d in range(1, NX):
        for q in qcopies(x, d, low_half, qsend, qrecv):
            q.wait_recv()
    prepare(z)
    diagonal(0)
    finish(0, 0)
    @pl.when(late)
    def _():
        relay()

    keys_on(3)
    keys_on(4)
    @pl.when(jnp.logical_not(late))
    def _():
        relayed()

    @pl.when(z < zbar)
    def _():
        whole(1)

    mid_row = nz // 2

    @pl.when(z <= mid_row)
    def _():
        values_on(3)
        values_on(4)

    swap = ((z + 4) // nz) * ((2 * nz - 2 - z) // nz)

    def step(i, carry):
        early = (i // 2 % 2) * (1 - i // 4)
        is_two, is_three = early * (1 - i % 2), early * (i % 2)
        t = i + swap * (is_two - is_three)
        tile(t)

        @pl.when(i == 1)
        def _():
            @pl.when(z > mid_row)
            def _():
                values_on(3)
                values_on(4)

            @pl.when(z <= mid_row)
            def _():
                keys_on(5)
                keys_on(6)

            conv_part()
            @pl.when(z > mid_row)
            def _():
                keys_on(5)
                keys_on(6)


        @pl.when(i == 2)
        def _():
            values_on(5)
            values_on(6)
            scatter_first()

        @pl.when((i == 3) & late)
        def _():
            relayed()

        @pl.when(i == 4)
        def _():
            weights_on()

        @pl.when(i == 6)
        def _():
            keys_on(7)
            values_on(7)
            scatter_second()

        return carry

    lax.fori_loop(1, nz, step, 0)


    for d in range(1, NX):
        for k, lanes in enumerate((low_half, high_half)):
            for cp in ocopies_of(d, lanes, k):
                cp.wait_recv()
    for h in range(2):
        best = mrow[x, h]
        for d in range(1, NX):
            best = jnp.maximum(best, srecv[d - 1, h : h + 1, :])
        share = jnp.exp2((mrow[x, h] - best) * LOG2E)
        summed = acc[x, h, HEAD : HEAD + 1, :] * share
        value = acc[x, h, :HEAD, :] * share
        for d in range(1, NX):
            share = jnp.exp2((srecv[d - 1, h : h + 1, :] - best) * LOG2E)
            summed = summed + srecv[d - 1, 2 + h : 3 + h, :] * share
            value = value + orecv[d - 1, h * HEAD : (h + 1) * HEAD, :].astype(F32) * share
        cpad[h * HEAD : (h + 1) * HEAD, :] = value / summed
        level = best + jnp.log(summed) - cref[h : h + 1]
        for zz, part, lanes, dst, at in (
            (z, ha, low_half, log_total, pl.multiple_of(ha * mid_tok, mid_tok)),
            (zbar, hb, high_half, lt_out, 0),
        ):
            here = pl.multiple_of((zz * NX + x) * tok + part * mid_tok, 128)
            dst[h : h + 1, pl.ds(at, mid_tok)] = (
                level[:, lanes.start : lanes.start + mid_tok]
                + cum_gate[:, pl.ds(here, mid_tok)][h : h + 1]
            )
    at_out[...] = cpad[...].T.astype(BF16).reshape(8, rows, 2 * HEAD)

    mine = at_in.at[:, pl.ds(pl.multiple_of(t_me * 2 * HEAD, 2 * HEAD), 2 * HEAD)]
    lcopy = rcopy(lt_out, lt_in, lsend.at[0], lrecv.at[0], sp_of(zbar))

    def acopy(k):
        zz, owner = (z, 4 * ha + k) if k < 4 else (zbar, 4 * hb + k - 4)
        return rcopy(at_out.at[k], mine, asend.at[k], arecv.at[t_me], (zz * NX + x, owner))

    for k in (4, 5, 6, 7, 0, 1, 2, 3):
        acopy(k).start()
    lcopy.start()

    weights_last()
    for k in (0, 5, 6, 9, 10):
        gw[k].wait_recv()
    near_r.wait_recv()
    near_l.wait_recv()
    both_r.wait_recv()
    both_l.wait_recv()
    po[y] = po[y] + frl[...].astype(F32) + frr[...].astype(F32)
    def from_tp(t):
        return rcopy(
            at_out.at[0],
            at_in.at[:, pl.ds(pl.multiple_of(t * 2 * HEAD, 2 * HEAD), 2 * HEAD)],
            asend.at[0],
            arecv.at[t],
            sp_of(zbar),
        )

    def last(part, emit):
        for k in range(4):
            from_tp(4 * part + k).wait_recv()
        lhs = at_in[:, pl.ds(pl.multiple_of(part * 8 * HEAD, 8 * HEAD), 8 * HEAD)]

        def columns(n, carry):
            cols = pl.ds(pl.multiple_of(n * 512, 512), 512)
            w = wo[pl.ds(4 * part, 4), :, cols].reshape(8 * HEAD, 512)
            emit(cols, po[y, :, cols] + jnp.dot(lhs, w, preferred_element_type=F32))
            return carry

        lax.fori_loop(0, depth // 512, columns, 0)

    def keep(cols, value):
        po[y, :, cols] = value

    def put(cols, value):
        mixed[:, cols] = value.astype(BF16)

    last(ha, keep)
    last(hb, put)
    lcopy.wait_recv()
    log_total[:, pl.ds(pl.multiple_of(hb * mid_tok, mid_tok), mid_tok)] = lt_in[0:2, :]

    for cp in g + gw:
        cp.wait_send()
    for t in range(1, 8):
        above, below = (z + 1) % nz, (z + nz - 1) % nz

        @pl.when(among("k", t, above if t % 2 else below))
        def _(t=t, above=above):
            kcopy(z, t, above).wait_send()

        @pl.when(among("v", t, above if t % 2 and t < nz - 1 else below))
        def _(t=t, above=above):
            vcopy(z, t, above).wait_send()

    for d in range(1, NX):
        for q in qcopies(x, d, low_half, qsend, qrecv) + qcopies(x, d, high_half, qrsend, qrrecv):
            q.wait_send()
    for q in qbcopies(low_half, high_half):
        q.wait_send()
    rcopy_rim.wait_send()
    for d in range(1, NX):
        for k, lanes in enumerate((low_half, high_half)):
            for cp in ocopies_of(d, lanes, k):
                cp.wait_send()
    for cp in ccopies + bcopies:
        cp.wait_send()
    for cp in (far_r, far_l, near_r, near_l, both_r, both_l, lcopy):
        cp.wait_send()
    for k in range(8):
        acopy(k).wait_send()


def per_device(*args):
    tokens = args[0]
    rows, depth = tokens.shape
    tok = rows * 8
    nz = lax.axis_size("sp") // NX
    att = args[2].shape[1]
    ch = args[5].shape[1]
    wide = 3 * att + 2 * ch
    ops = list(args)
    ops[1] = args[1][None]
    ops[8] = args[8][None]
    vmem = pl.BlockSpec(memory_space=pltpu.VMEM)
    hbm = pl.BlockSpec(memory_space=pltpu.HBM)
    specs = [vmem, vmem] + [hbm] * 10
    dma = pltpu.SemaphoreType.DMA
    scratch = [
        pltpu.VMEM(args[7].shape, F32),
        pltpu.VMEM((1, ch), F32),
        pltpu.VMEM(args[9].shape, F32),
        pltpu.VMEM((8, rows, depth), BF16),
        pltpu.VMEM((depth, wide), BF16),
        pltpu.VMEM((8, att, depth), BF16),
        pltpu.VMEM((ch, depth), BF16),
        pltpu.VMEM((NX, 2, att, tok), BF16),
        pltpu.VMEM((att, tok // 2), BF16),
        pltpu.VMEM((nz, tok, att), BF16),
        pltpu.VMEM((nz, att, tok), BF16),
        pltpu.VMEM((2, tok, att), BF16),
        pltpu.VMEM((2, VROWS, tok), BF16),
        pltpu.VMEM((att, tok), F32),
        pltpu.VMEM((NX, 2, 1, tok), F32),
        pltpu.VMEM((NX, 2, VROWS, tok), F32),
        pltpu.VMEM((NX - 1, att, tok), BF16),
        pltpu.VMEM((NX - 1, att, tok), BF16),
        pltpu.VMEM((NX - 1, 8, tok), F32),
        pltpu.VMEM((NX - 1, 8, tok), F32),
        pltpu.VMEM((tok, ch), BF16),
        pltpu.VMEM((32, ch), BF16),
        pltpu.VMEM((tok + 32, ch), F32),
        pltpu.VMEM((tok, ch), F32),
        pltpu.VMEM((tok, 128), F32),
        pltpu.VMEM((8, 1, tok), F32),
        pltpu.VMEM((2, NY, rows, ch), BF16),
        pltpu.VMEM((NY, rows, depth), BF16),
        pltpu.VMEM((NY, rows, depth), BF16),
        pltpu.VMEM((NY, rows, depth), F32),
        pltpu.VMEM((rows, depth), BF16),
        pltpu.VMEM((rows // 2, depth), BF16),
        pltpu.VMEM((rows // 2, depth), BF16),
        pltpu.VMEM((rows, depth), BF16),
        pltpu.VMEM((rows, depth), BF16),
        pltpu.VMEM((rows, depth), BF16),
        pltpu.VMEM((rows, depth), BF16),
        pltpu.VMEM((8, rows, att), BF16),
        pltpu.VMEM((rows, 8 * att), BF16),
        pltpu.VMEM((8, tok // 2), F32),
        pltpu.VMEM((8, tok // 2), F32),
    ] + [dma((n,)) for n in (10, 11, 11, 11, 11, 8, 16, 8, 16, 6, 6, 2, 2, 6, 6, 1, 1, 12, 12, 8, 8, 10, 10, 8, 8, 1, 1)]
    return pl.pallas_call(
        kernel,
        out_shape=(
            pltpu.VMEM((rows, depth), BF16),
            pltpu.VMEM((2, tok), F32),
        ),
        in_specs=specs,
        out_specs=(vmem, vmem),
        scratch_shapes=scratch,
        compiler_params=pltpu.CompilerParams(
            collective_id=0, has_side_effects=True, vmem_limit_bytes=58 * 1024 * 1024
        ),
        name="layer",
    )(*ops)


def solution(mesh):
    in_specs = (
        P(("sp", "tp"), None),
        P(),
        P(None, "tp"),
        P(None, "tp"),
        P(None, "tp"),
        P(None, "tp"),
        P(None, "tp"),
        P(None, "tp"),
        P("tp"),
        P("tp", None),
        P("tp", None),
        P("tp", None),
    )
    out_specs = (P(("sp", "tp"), None), P("tp", "sp"))
    return jax.shard_map(
        per_device, mesh=mesh, in_specs=in_specs, out_specs=out_specs, check_vma=False
    )
```

```python
import functools

import jax
import jax.numpy as jnp
from jax import lax
from jax.experimental import pallas as pl
from jax.experimental.pallas import tpu as pltpu
from jax.sharding import PartitionSpec as P

MESH = pl.DeviceIdType.MESH
F32 = jnp.float32
BF16 = jnp.bfloat16
HEAD = 64
NX = 4
NY = 4
LOW = -1e30
LOG2E = 1.4426950408889634
VROWS = 80
AT_ONCE = 4


def kernel(
    tokens,
    norm_gain,
    w_query,
    w_key,
    w_value,
    conv_in,
    conv_gate,
    taps_hbm,
    gain_hbm,
    cum_hbm,
    out_attn,
    out_conv,
    mixed,
    log_total,
    conv_taps,
    conv_gain,
    cum_gate,
    nt,
    wall,
    wo,
    wconv,
    qp,
    qb,
    ks,
    vs,
    kp,
    vp,
    cpad,
    mrow,
    acc,
    obuf,
    orecv,
    sbuf,
    srecv,
    gb,
    rim,
    cg,
    cv,
    sq,
    csq,
    xs,
    sb,
    rb,
    po,
    t2,
    r2r,
    r2l,
    sr,
    sl,
    frl,
    frr,
    at_out,
    at_in,
    lt_out,
    lt_in,
    wsem,
    gsend,
    grecv,
    wosend,
    worecv,
    ksend,
    krecv,
    vsend,
    vrecv,
    qsend,
    qrecv,
    qbsend,
    qbrecv,
    qrsend,
    qrrecv,
    msend,
    mrecv,
    osend,
    orecv_sem,
    csend,
    crecv,
    xsend,
    xrecv,
    asend,
    arecv,
    lsend,
    lrecv,
):
    s_me = lax.axis_index("sp")
    t_me = lax.axis_index("tp")
    nsp = lax.axis_size("sp")
    nz = nsp // NX
    z = s_me // NX
    x = s_me % NX
    y = t_me // 2
    c = t_me % 2
    rows = tokens.shape[0]
    half = rows // 2
    depth = tokens.shape[1]
    tok = rows * 8
    mid_tok = tok // 2
    zbar = nz - 1 - z
    hb = y // (NY // 2)
    ha = 1 - hb

    def at_tp(t):
        return (s_me, t)

    def at_sp(s):
        return (s, t_me)

    def rcopy(src, dst, ssem, rsem, dev):
        return pltpu.make_async_remote_copy(
            src_ref=src,
            dst_ref=dst,
            send_sem=ssem,
            recv_sem=rsem,
            device_id=dev,
            device_id_type=MESH,
        )

    wcopies = []
    at = 0
    for i, w in enumerate((w_key, w_value, w_query, conv_in, conv_gate)):
        n = w.shape[1]
        wcopies.append(pltpu.make_async_copy(w, wall.at[:, pl.ds(at, n)], wsem.at[i]))
        at += n
    ocopies = [
        pltpu.make_async_copy(out_attn, wo.at[t_me], wsem.at[5]),
        pltpu.make_async_copy(out_conv, wconv, wsem.at[6]),
    ]
    scopies = [
        pltpu.make_async_copy(src, dst, wsem.at[7 + i])
        for i, (src, dst) in enumerate(
            ((taps_hbm, conv_taps), (gain_hbm, conv_gain), (cum_hbm, cum_gate))
        )
    ]
    for w in wcopies + ocopies + scopies:
        w.start()

    barrier = pltpu.get_barrier_semaphore()
    for d in range(1, 8):
        pl.semaphore_signal(
            barrier, inc=1, device_id=at_tp((t_me + d) % 8), device_id_type=MESH
        )
    for d in range(1, NX):
        pl.semaphore_signal(
            barrier, inc=1, device_id=at_sp(z * NX + (x + d) % NX), device_id_type=MESH
        )
    for d in (1, nz - 1):
        pl.semaphore_signal(
            barrier, inc=1, device_id=at_sp(((z + d) % nz) * NX + x), device_id_type=MESH
        )
    for d in (1, nsp - 1):
        pl.semaphore_signal(
            barrier, inc=1, device_id=at_sp((s_me + d) % nsp), device_id_type=MESH
        )

    for t in range(8):
        pl.semaphore_signal(
            barrier, inc=1, device_id=(zbar * NX + x, t), device_id_type=MESH
        )

    wide = tokens[...].astype(F32)
    factor = lax.rsqrt(jnp.mean(wide * wide, axis=1, keepdims=True) + 1e-06)
    nt[t_me] = (wide * factor * norm_gain[...]).astype(BF16)
    qp[:, 0, HEAD:, :] = jnp.ones((NX, HEAD, tok), BF16)
    qp[:, 1, :HEAD, :] = jnp.ones((NX, HEAD, tok), BF16)
    vp[:, HEAD:, :] = jnp.ones((2, VROWS - HEAD, tok), BF16)
    cpad[...] = jnp.zeros_like(cpad)
    mrow[...] = jnp.full_like(mrow, LOW)
    acc[...] = jnp.zeros_like(acc)

    pl.semaphore_wait(barrier, 7 + NX - 1 + 4 + 8)

    sib = y * 2 + (1 - c)
    tr = ((y + 1) % NY) * 2 + c
    tl = ((y + NY - 1) % NY) * 2 + c
    to = ((y + 2) % NY) * 2 + c
    lo, hi = pl.ds(0, half), pl.ds(half, half)

    def gather_over_tp(buf, ssem, rsem):
        n = buf.shape[1] // 2
        first, last = pl.ds(0, n), pl.ds(n, n)

        def gcopy(k, src, part, dev):
            ref = buf.at[src] if part is None else buf.at[src, part]
            return rcopy(ref, ref, ssem.at[k], rsem.at[k], at_tp(dev))

        return [
            gcopy(0, t_me, None, sib),
            gcopy(1, t_me, first, tr),
            gcopy(2, t_me, last, tr),
            gcopy(3, t_me, last, tl),
            gcopy(4, t_me, first, tl),
            gcopy(5, tl, None, sib),
            gcopy(6, tr, None, sib),
            gcopy(7, tl, first, tr),
            gcopy(8, tr, last, tl),
            gcopy(9, to, first, sib),
            gcopy(10, to, last, sib),
        ]

    g = gather_over_tp(nt, gsend, grecv)
    gw = gather_over_tp(wo, wosend, worecv)
    for k in (1, 3, 2, 4, 0):
        g[k].start()

    def sp_of(zz):
        return at_sp(zz * NX + x)

    def landed(t, piece):
        return t if piece is None else 4 + 4 * t + piece

    def kcopy(zb, t, zt, part=None, piece=None):
        ref = ks.at[zb] if part is None else ks.at[zb, part]
        return rcopy(ref, ref, ksend.at[t], krecv.at[landed(t, piece)], sp_of(zt))

    def vcopy(zb, t, zt, part=None, piece=None):
        ref = vs.at[zb] if part is None else vs.at[zb, :, part]
        return rcopy(ref, ref, vsend.at[t], vrecv.at[landed(t, piece)], sp_of(zt))

    def pair(i):
        return (y + 2 * NY - (2 * (i % 2) - 1) * ((i + 1) // 2)) % NY

    def pair_rows(i):
        return pl.ds(pl.multiple_of(pair(i) * 2 * rows, 2 * rows), 2 * rows)

    def place(t):
        dr = 2 * (t % 2) - 1
        return dr, (z + nz - dr * ((t + 1) // 2)) % nz

    def delivered(kind, t):
        up, s = t % 2 == 1, (t + 1) // 2
        if t == nz - 1:
            up = kind == "k"
        last = nz // 2 if up == (kind == "k") else nz // 2 - 1
        rows_at = []
        for zz in range(nz):
            zb = (zz - s if up else zz + s) % nz
            behind = [(zz + k if up else zz - k) % nz for k in range(last - s + 1)]
            if any(zb <= max(r, nz - 1 - r) for r in behind):
                rows_at.append(zz)
        return rows_at

    def among(kind, t, zz):
        found = False
        for r in delivered(kind, t):
            found = found | (zz == r)
        return found

    def piece_on(kind, piece):
        copy = kcopy if kind == "k" else vcopy
        part = pair_rows(piece)
        for t in (1, 2):
            dr, zb = place(t)
            zt = (z + nz + dr) % nz

            @pl.when(among(kind, t, z))
            def _(t=t, zb=zb, zt=zt):
                copy(zb, t, zt, part, piece).wait_recv()

            @pl.when(among(kind, t + 2, zt))
            def _(t=t, zb=zb, zt=zt):
                copy(zb, t + 2, zt, part).start()

    low_half, high_half = pl.ds(0, mid_tok), pl.ds(mid_tok, mid_tok)

    def qcopies(src, d, lanes, ssem, rsem):
        dev = at_sp(z * NX + (x + d) % NX)
        a = qp.at[src, 0, pl.ds(0, HEAD), lanes]
        b = qp.at[src, 1, pl.ds(HEAD, HEAD), lanes]
        return (
            rcopy(a, a, ssem.at[2 * d - 2], rsem.at[2 * d - 2], dev),
            rcopy(b, b, ssem.at[2 * d - 1], rsem.at[2 * d - 1], dev),
        )

    def qbcopies(src, lanes):
        dev = sp_of(zbar)
        return (
            rcopy(
                qb.at[pl.ds(0, HEAD), src],
                qp.at[x, 0, pl.ds(0, HEAD), lanes],
                qbsend.at[0],
                qbrecv.at[0],
                dev,
            ),
            rcopy(
                qb.at[pl.ds(HEAD, HEAD), src],
                qp.at[x, 1, pl.ds(HEAD, HEAD), lanes],
                qbsend.at[1],
                qbrecv.at[1],
                dev,
            ),
        )

    rcopy_rim = rcopy(
        gb.at[pl.ds(tok - 32, 32)], rim, msend.at[0], mrecv.at[0], at_sp((s_me + 1) % nsp)
    )
    for w in wcopies + scopies:
        w.wait()

    def project(i, carry):
        @pl.when(i == 0)
        def _():
            g[0].wait_recv()

        @pl.when(i == 1)
        def _():
            g[1].wait_recv()
            g[7].start()
            g[3].wait_recv()
            g[8].start()
            g[2].wait_recv()
            g[5].start()
            g[4].wait_recv()
            g[6].start()
            piece_on("k", 0)
            piece_on("v", 0)
            g[5].wait_recv()

        @pl.when(i == 2)
        def _():
            g[6].wait_recv()

        @pl.when(i == 3)
        def _():
            g[7].wait_recv()
            g[9].start()
            g[8].wait_recv()
            g[10].start()
            g[9].wait_recv()
            g[10].wait_recv()

        p = pair(i)
        lhs = nt[pl.ds(2 * p, 2)].reshape(2 * rows, depth)
        here = pair_rows(i)
        kv = jnp.dot(lhs, wall[:, :256], preferred_element_type=F32)
        ks[z, here, :] = kv[:, :128].astype(BF16)
        vs[z, :, here] = kv[:, 128:].T.astype(BF16)
        for t, zt in ((1, (z + 1) % nz), (2, (z + nz - 1) % nz)):

            @pl.when(among("k", t, zt))
            def _(t=t, zt=zt):
                kcopy(z, t, zt, here, i).start()

            @pl.when(among("v", t, zt))
            def _(t=t, zt=zt):
                vcopy(z, t, zt, here, i).start()

        res = jnp.dot(lhs, wall[:, 256:], preferred_element_type=F32)
        opened = res[:, 128:384]
        gating = res[:, 384:640]
        gate = (opened / (1.0 + jnp.exp(-gating))).astype(BF16)
        gb[here, :] = gate
        cg[pl.ds(pl.multiple_of(pair(i) * 2 * rows + 32, 32), 2 * rows), :] = gate.astype(F32)
        qt = (res[:, :128] * HEAD ** (-0.5)).T.astype(BF16)

        spot = pl.ds(pl.multiple_of((p % 2) * 2 * rows, 2 * rows), 2 * rows)
        over = pl.ds(pl.multiple_of((p % 2) * 2 * rows + mid_tok, 2 * rows), 2 * rows)

        @pl.when(p // 2 == hb)
        def _():
            qb[:, spot] = qt
            for q in qbcopies(spot, over):
                q.start()

        @pl.when(p == NY - 1)
        def _():
            rcopy_rim.start()

        @pl.when(p // 2 == ha)
        def _():
            qp[x, 0, :HEAD, spot] = qt[:HEAD]
            qp[x, 1, HEAD:, spot] = qt[HEAD:]
            for d in (1, 3, 2):
                for q in qcopies(x, d, spot, qsend, qrecv):
                    q.start()

        return carry

    lax.fori_loop(0, NY, project, 0)

    piece_on("k", 1)
    piece_on("v", 1)

    def conv_rows(i, carry):
        r0 = pl.multiple_of(i * 64, 64)
        win = cg[pl.ds(r0, 96), :]
        total = jnp.zeros((64, win.shape[1]), F32)
        for b in range(8):
            turned = win if b == 0 else pltpu.roll(win, 96 - b, 0)
            for a in range(5):
                k = 8 * a + b - 2
                if 0 <= k < 31:
                    total = total + conv_taps[k : k + 1, :] * turned[8 * a : 8 * a + 64]
        cv[pl.ds(r0, 64), :] = total
        square = total * total
        sq[pl.ds(r0, 64), :] = square[:, :128] + square[:, 128:]
        return carry

    lax.fori_loop(1, tok // 64, conv_rows, 0)

    cref = cum_gate[:, pl.ds(pl.multiple_of(z * NX * tok, 128), 128)][:, :1]

    def prepare(zb):
        ck = cum_gate[:, pl.ds(pl.multiple_of((zb * NX + x) * tok, 128), tok)]
        bias = cref - ck
        high = bias.astype(BF16).astype(F32)
        left = bias - high
        mid = left.astype(BF16).astype(F32)
        low = left - mid
        rowid = lax.broadcasted_iota(jnp.int32, (8, tok), 0)
        for h, r0 in ((0, HEAD), (1, 0)):
            tile = jnp.where(
                rowid == 0,
                high[h : h + 1],
                jnp.where(
                    rowid == 1, mid[h : h + 1], jnp.where(rowid == 2, low[h : h + 1], 0.0)
                ),
            )
            cpad[r0 : r0 + 8, :] = tile
        extra = cpad[...].T
        kf = ks[zb].astype(F32)
        lane = lax.broadcasted_iota(jnp.int32, (tok, 2 * HEAD), 1)
        kp[0] = jnp.where(lane < HEAD, kf, extra).astype(BF16)
        kp[1] = jnp.where(lane < HEAD, extra, kf).astype(BF16)
        vp[0, :HEAD, :] = vs[zb, :HEAD, :]
        vp[1, :HEAD, :] = vs[zb, HEAD:, :]

    def chunks(js, g, masked):
        lanes = pl.ds(pl.multiple_of(g * mid_tok, mid_tok), mid_tok)
        units = [(j, h) for j in js for h in range(2)]
        old = [mrow[j, h, :, lanes] for j, h in units]
        held = [acc[j, h, :, lanes] for j, h in units]
        sc = [jnp.dot(kp[h], qp[j, h, :, lanes], preferred_element_type=F32) for j, h in units]
        if masked:
            kpos = lax.broadcasted_iota(jnp.int32, sc[0].shape, 0)
            qpos = lax.broadcasted_iota(jnp.int32, sc[0].shape, 1)
            ahead = kpos - qpos - (ha + g * (hb - ha)) * mid_tok
            sc = [jnp.where(ahead <= (j - x) * tok, v, LOW) for v, (j, _) in zip(sc, units)]
        new = [jnp.maximum(o, jnp.max(v, axis=0, keepdims=True)) for o, v in zip(old, sc)]
        wts = [jnp.exp2((v - n) * LOG2E).astype(BF16) for n, v in zip(new, sc)]
        shrink = [jnp.exp2((o - n) * LOG2E) for o, n in zip(old, new)]
        out = [
            a * k + jnp.dot(vp[h], w, preferred_element_type=F32)
            for a, k, w, (_, h) in zip(held, shrink, wts, units)
        ]
        for n, o, (j, h) in zip(new, out, units):
            mrow[j, h, :, lanes] = n
            acc[j, h, :, lanes] = o

    def ocopies_of(d, lanes, k):
        dev = at_sp(z * NX + (x + d) % NX)
        return (
            rcopy(
                obuf.at[d - 1, :, lanes],
                orecv.at[d - 1, :, lanes],
                osend.at[2 * k + 4 * (d - 1)],
                orecv_sem.at[2 * k + 4 * (d - 1)],
                dev,
            ),
            rcopy(
                sbuf.at[d - 1, :, lanes],
                srecv.at[d - 1, :, lanes],
                osend.at[2 * k + 4 * (d - 1) + 1],
                orecv_sem.at[2 * k + 4 * (d - 1) + 1],
                dev,
            ),
        )

    def final_at(zz, gg):
        zq = nz - 1 - zz if gg else zz
        order = [(zz - (2 * (t % 2) - 1) * ((t + 1) // 2)) % nz for t in range(nz)]
        return max(t for t in range(nz) if order[t] <= zq)

    def finish(t, g):
        done = False
        for zz in range(nz):
            for gg in range(2):
                done = done | ((z == zz) & (g == gg) & (t == final_at(zz, gg)))

        @pl.when(done)
        def _():
            lanes = pl.ds(pl.multiple_of(g * mid_tok, mid_tok), mid_tok)
            for d in (2, 1, 3):
                j = (x + d) % NX
                for h in range(2):
                    obuf[d - 1, h * HEAD : (h + 1) * HEAD, lanes] = acc[j, h, :HEAD, lanes].astype(
                        BF16
                    )
                    sbuf[d - 1, h : h + 1, lanes] = mrow[j, h, :, lanes]
                    sbuf[d - 1, 2 + h : 3 + h, lanes] = acc[j, h, HEAD : HEAD + 1, lanes]
                for cp in ocopies_of(d, lanes, g):
                    cp.start()

    def whole(g):
        def some(i, carry):
            chunks(tuple(i * AT_ONCE + k for k in range(AT_ONCE)), g, False)
            return carry

        lax.fori_loop(0, NX // AT_ONCE, some, 0)

    def diagonal(g):
        chunks(tuple(range(NX)), g, True)

    def tile(t):
        _, zb = place(t)

        @pl.when((zb <= z) | (zb <= zbar))
        def _():
            prepare(zb)

            def group(i, carry):
                g = i + (z // (nz // 2)) * (1 - 2 * i)
                zq = z + g * (nz - 1 - 2 * z)

                @pl.when(zb < zq)
                def _():
                    whole(g)

                @pl.when(zb == zq)
                def _():
                    diagonal(g)

                @pl.when(zb <= zq)
                def _():
                    finish(t, g)

                return carry

            lax.fori_loop(0, 2, group, 0)

    def keys_on(t):
        dr, zb = place(t)
        zt = (z + nz + dr) % nz

        @pl.when(among("k", t, z))
        def _():
            kcopy(zb, t, zt).wait_recv()

        if t <= 5:

            @pl.when(among("k", t + 2, zt))
            def _():
                kcopy(zb, t + 2, zt).start()

    def values_on(t):
        dr, zb = place(t)
        zt = (z + nz + dr) % nz

        @pl.when(among("v", t, z))
        def _():
            vcopy(zb, t, zt).wait_recv()

        if t <= 4 or t == 6:
            on = t + 2 - t // 6

            @pl.when(among("v", on, zt))
            def _():
                vcopy(zb, on, zt).start()

    near = (z % 4) * (3 - z % 4) == 0
    late = (z == 5) | (z == 6)

    def relay():
        for q in qbcopies(low_half, high_half):
            q.wait_recv()
        for d in (1, 3, 2):
            for q in qcopies(x, d, high_half, qrsend, qrrecv):
                q.start()

    def relayed():
        for d in range(1, NX):
            for q in qcopies(x, d, high_half, qrsend, qrrecv):
                q.wait_recv()

    @pl.when(near)
    def _():
        relay()

    for kind, piece in (("k", 2), ("v", 2), ("k", 3), ("v", 3)):
        piece_on(kind, piece)

    def project_out(which, emit):
        lhs = xs[which].reshape(NY * rows, xs.shape[3])

        def columns(n, carry):
            cols = pl.ds(pl.multiple_of(n * 512, 512), 512)
            res = jnp.dot(lhs, wconv[:, cols], preferred_element_type=F32)
            emit(cols, res)
            return carry

        lax.fori_loop(0, depth // 512, columns, 0)

    def emit_sib(cols, res):
        sb[:, :, cols] = res.astype(BF16).reshape(NY, rows, 512)

    def emit_own(cols, res):
        po[:, :, cols] = res.reshape(NY, rows, 512)

    ybits = [(y + k) % NY for k in range(NY)]

    def xcopy(k, src, dst, dev):
        return rcopy(src, dst, xsend.at[k], xrecv.at[k], at_tp(dev))

    bcopies = [xcopy(k, sb.at[ybits[k]], rb.at[ybits[k]], sib) for k in range(NY)]

    def conv_part():
        for cc in ccopies:
            cc.wait_recv()
        total = csq[0]
        for t in range(1, 8):
            total = total + csq[t]
        scale = lax.rsqrt(total / (8.0 * conv_gain.shape[1]) + 1e-06)
        sq[...] = jnp.broadcast_to(scale, (128, tok)).T
        for i in range(8):
            r = pl.ds(i * rows, rows)
            factor = sq[r, :]
            for b in range(2):
                lanes = pl.ds(b * 128, 128)
                v = cv[r, lanes] * factor * conv_gain[:, lanes]
                v = v / (1.0 + jnp.exp(-v))
                xs[i % 2, i // 2, :, lanes] = v.astype(BF16)
        ocopies[1].wait()

        project_out(1 - c, emit_sib)
        for k in (2, 1, 3, 0):
            bcopies[k].start()
        project_out(c, emit_own)

    far_r = xcopy(4, t2.at[lo], r2r, tr)
    far_l = xcopy(5, t2.at[hi], r2l, tl)
    near_r = xcopy(6, sr.at[hi], frl.at[hi], tr)
    near_l = xcopy(7, sl.at[lo], frr.at[lo], tl)
    both_r = xcopy(8, sr.at[lo], frl.at[lo], tr)
    both_l = xcopy(9, sl.at[hi], frr.at[hi], tl)

    def scatter_first():
        bcopies[2].wait_recv()
        t2[...] = (po[ybits[2]] + rb[ybits[2]].astype(F32)).astype(BF16)
        far_r.start()
        far_l.start()
        bcopies[1].wait_recv()
        sr[hi, :] = (po[ybits[1], hi] + rb[ybits[1], hi].astype(F32)).astype(BF16)
        near_r.start()
        bcopies[3].wait_recv()
        sl[lo, :] = (po[ybits[3], lo] + rb[ybits[3], lo].astype(F32)).astype(BF16)
        near_l.start()

    def scatter_second():
        far_r.wait_recv()
        sr[lo, :] = (
            po[ybits[1], lo] + rb[ybits[1], lo].astype(F32) + r2r[...].astype(F32)
        ).astype(BF16)
        both_r.start()
        far_l.wait_recv()
        sl[hi, :] = (
            po[ybits[3], hi] + rb[ybits[3], hi].astype(F32) + r2l[...].astype(F32)
        ).astype(BF16)
        both_l.start()
        bcopies[0].wait_recv()
        po[y] = po[y] + rb[y].astype(F32)

    def weights_on():
        for got, on in ((1, 7), (3, 8), (2, 5), (4, 6)):
            gw[got].wait_recv()
            gw[on].start()

    def weights_last():
        for got, on in ((7, 9), (8, 10)):
            gw[got].wait_recv()
            gw[on].start()

    rcopy_rim.wait_recv()
    first = jnp.where(s_me > 0, 1.0, 0.0).astype(F32)
    cg[0:32, :] = rim[...].astype(F32) * first
    conv_rows(0, 0)
    part = jnp.sum(sq[...].T, axis=0, keepdims=True)
    csq[t_me] = part
    ccopies = []
    for d in range(1, 8):
        cc = rcopy(
            csq.at[t_me], csq.at[t_me], csend.at[d], crecv.at[d], at_tp((t_me + d) % 8)
        )
        cc.start()
        ccopies.append(cc)
    ocopies[0].wait()
    for k in (1, 3, 2, 4, 0):
        gw[k].start()

    @pl.when(jnp.logical_not(near | late))
    def _():
        relay()

    for d in range(1, NX):
        for q in qcopies(x, d, low_half, qsend, qrecv):
            q.wait_recv()
    prepare(z)
    diagonal(0)
    finish(0, 0)
    @pl.when(late)
    def _():
        relay()

    keys_on(3)
    keys_on(4)
    @pl.when(jnp.logical_not(late))
    def _():
        relayed()

    @pl.when(z < zbar)
    def _():
        whole(1)

    mid_row = nz // 2

    @pl.when(z <= mid_row)
    def _():
        values_on(3)
        values_on(4)

    swap = ((z + 4) // nz) * ((2 * nz - 2 - z) // nz)

    def step(i, carry):
        early = (i // 2 % 2) * (1 - i // 4)
        is_two, is_three = early * (1 - i % 2), early * (i % 2)
        t = i + swap * (is_two - is_three)
        tile(t)

        @pl.when(i == 1)
        def _():
            @pl.when(z > mid_row)
            def _():
                values_on(3)
                values_on(4)

            @pl.when(z <= mid_row)
            def _():
                keys_on(5)
                keys_on(6)

            conv_part()
            @pl.when(z > mid_row)
            def _():
                keys_on(5)
                keys_on(6)


        @pl.when(i == 2)
        def _():
            values_on(5)
            values_on(6)
            scatter_first()

        @pl.when((i == 3) & late)
        def _():
            relayed()

        @pl.when(i == 4)
        def _():
            weights_on()

        @pl.when(i == 6)
        def _():
            keys_on(7)
            values_on(7)
            scatter_second()

        return carry

    lax.fori_loop(1, nz, step, 0)


    for d in range(1, NX):
        for k, lanes in enumerate((low_half, high_half)):
            for cp in ocopies_of(d, lanes, k):
                cp.wait_recv()
    for h in range(2):
        best = mrow[x, h]
        for d in range(1, NX):
            best = jnp.maximum(best, srecv[d - 1, h : h + 1, :])
        share = jnp.exp2((mrow[x, h] - best) * LOG2E)
        summed = acc[x, h, HEAD : HEAD + 1, :] * share
        value = acc[x, h, :HEAD, :] * share
        for d in range(1, NX):
            share = jnp.exp2((srecv[d - 1, h : h + 1, :] - best) * LOG2E)
            summed = summed + srecv[d - 1, 2 + h : 3 + h, :] * share
            value = value + orecv[d - 1, h * HEAD : (h + 1) * HEAD, :].astype(F32) * share
        cpad[h * HEAD : (h + 1) * HEAD, :] = value / summed
        level = best + jnp.log(summed) - cref[h : h + 1]
        for zz, part, lanes, dst, at in (
            (z, ha, low_half, log_total, pl.multiple_of(ha * mid_tok, mid_tok)),
            (zbar, hb, high_half, lt_out, 0),
        ):
            here = pl.multiple_of((zz * NX + x) * tok + part * mid_tok, 128)
            dst[h : h + 1, pl.ds(at, mid_tok)] = (
                level[:, lanes.start : lanes.start + mid_tok]
                + cum_gate[:, pl.ds(here, mid_tok)][h : h + 1]
            )
    at_out[...] = cpad[...].T.astype(BF16).reshape(8, rows, 2 * HEAD)

    mine = at_in.at[:, pl.ds(pl.multiple_of(t_me * 2 * HEAD, 2 * HEAD), 2 * HEAD)]
    lcopy = rcopy(lt_out, lt_in, lsend.at[0], lrecv.at[0], sp_of(zbar))

    def acopy(k):
        zz, owner = (z, 4 * ha + k) if k < 4 else (zbar, 4 * hb + k - 4)
        return rcopy(at_out.at[k], mine, asend.at[k], arecv.at[t_me], (zz * NX + x, owner))

    for k in (4, 5, 6, 7, 0, 1, 2, 3):
        acopy(k).start()
    lcopy.start()

    weights_last()
    for k in (0, 5, 6, 9, 10):
        gw[k].wait_recv()
    near_r.wait_recv()
    near_l.wait_recv()
    both_r.wait_recv()
    both_l.wait_recv()
    po[y] = po[y] + frl[...].astype(F32) + frr[...].astype(F32)
    def from_tp(t):
        return rcopy(
            at_out.at[0],
            at_in.at[:, pl.ds(pl.multiple_of(t * 2 * HEAD, 2 * HEAD), 2 * HEAD)],
            asend.at[0],
            arecv.at[t],
            sp_of(zbar),
        )

    def last(part, emit):
        for k in range(4):
            from_tp(4 * part + k).wait_recv()
        lhs = at_in[:, pl.ds(pl.multiple_of(part * 8 * HEAD, 8 * HEAD), 8 * HEAD)]

        def columns(n, carry):
            cols = pl.ds(pl.multiple_of(n * 512, 512), 512)
            w = wo[pl.ds(4 * part, 4), :, cols].reshape(8 * HEAD, 512)
            emit(cols, po[y, :, cols] + jnp.dot(lhs, w, preferred_element_type=F32))
            return carry

        lax.fori_loop(0, depth // 512, columns, 0)

    def keep(cols, value):
        po[y, :, cols] = value

    def put(cols, value):
        mixed[:, cols] = value.astype(BF16)

    last(ha, keep)
    last(hb, put)
    lcopy.wait_recv()
    log_total[:, pl.ds(pl.multiple_of(hb * mid_tok, mid_tok), mid_tok)] = lt_in[0:2, :]

    for cp in g + gw:
        cp.wait_send()
    for t in range(1, 8):
        above, below = (z + 1) % nz, (z + nz - 1) % nz

        @pl.when(among("k", t, above if t % 2 else below))
        def _(t=t, above=above):
            kcopy(z, t, above).wait_send()

        @pl.when(among("v", t, above if t % 2 and t < nz - 1 else below))
        def _(t=t, above=above):
            vcopy(z, t, above).wait_send()

    for d in range(1, NX):
        for q in qcopies(x, d, low_half, qsend, qrecv) + qcopies(x, d, high_half, qrsend, qrrecv):
            q.wait_send()
    for q in qbcopies(low_half, high_half):
        q.wait_send()
    rcopy_rim.wait_send()
    for d in range(1, NX):
        for k, lanes in enumerate((low_half, high_half)):
            for cp in ocopies_of(d, lanes, k):
                cp.wait_send()
    for cp in ccopies + bcopies:
        cp.wait_send()
    for cp in (far_r, far_l, near_r, near_l, both_r, both_l, lcopy):
        cp.wait_send()
    for k in range(8):
        acopy(k).wait_send()


def per_device(*args):
    tokens = args[0]
    rows, depth = tokens.shape
    tok = rows * 8
    nz = lax.axis_size("sp") // NX
    att = args[2].shape[1]
    ch = args[5].shape[1]
    wide = 3 * att + 2 * ch
    ops = list(args)
    ops[1] = args[1][None]
    ops[8] = args[8][None]
    vmem = pl.BlockSpec(memory_space=pltpu.VMEM)
    hbm = pl.BlockSpec(memory_space=pltpu.HBM)
    specs = [vmem, vmem] + [hbm] * 10
    dma = pltpu.SemaphoreType.DMA
    scratch = [
        pltpu.VMEM(args[7].shape, F32),
        pltpu.VMEM((1, ch), F32),
        pltpu.VMEM(args[9].shape, F32),
        pltpu.VMEM((8, rows, depth), BF16),
        pltpu.VMEM((depth, wide), BF16),
        pltpu.VMEM((8, att, depth), BF16),
        pltpu.VMEM((ch, depth), BF16),
        pltpu.VMEM((NX, 2, att, tok), BF16),
        pltpu.VMEM((att, tok // 2), BF16),
        pltpu.VMEM((nz, tok, att), BF16),
        pltpu.VMEM((nz, att, tok), BF16),
        pltpu.VMEM((2, tok, att), BF16),
        pltpu.VMEM((2, VROWS, tok), BF16),
        pltpu.VMEM((att, tok), F32),
        pltpu.VMEM((NX, 2, 1, tok), F32),
        pltpu.VMEM((NX, 2, VROWS, tok), F32),
        pltpu.VMEM((NX - 1, att, tok), BF16),
        pltpu.VMEM((NX - 1, att, tok), BF16),
        pltpu.VMEM((NX - 1, 4, tok), F32),
        pltpu.VMEM((NX - 1, 4, tok), F32),
        pltpu.VMEM((tok, ch), BF16),
        pltpu.VMEM((32, ch), BF16),
        pltpu.VMEM((tok + 32, ch), F32),
        pltpu.VMEM((tok, ch), F32),
        pltpu.VMEM((tok, 128), F32),
        pltpu.VMEM((8, 1, tok), F32),
        pltpu.VMEM((2, NY, rows, ch), BF16),
        pltpu.VMEM((NY, rows, depth), BF16),
        pltpu.VMEM((NY, rows, depth), BF16),
        pltpu.VMEM((NY, rows, depth), F32),
        pltpu.VMEM((rows, depth), BF16),
        pltpu.VMEM((rows // 2, depth), BF16),
        pltpu.VMEM((rows // 2, depth), BF16),
        pltpu.VMEM((rows, depth), BF16),
        pltpu.VMEM((rows, depth), BF16),
        pltpu.VMEM((rows, depth), BF16),
        pltpu.VMEM((rows, depth), BF16),
        pltpu.VMEM((8, rows, att), BF16),
        pltpu.VMEM((rows, 8 * att), BF16),
        pltpu.VMEM((8, tok // 2), F32),
        pltpu.VMEM((8, tok // 2), F32),
    ] + [dma((n,)) for n in (10, 11, 11, 11, 11, 8, 16, 8, 16, 6, 6, 2, 2, 6, 6, 1, 1, 12, 12, 8, 8, 10, 10, 8, 8, 1, 1)]
    return pl.pallas_call(
        kernel,
        out_shape=(
            pltpu.VMEM((rows, depth), BF16),
            pltpu.VMEM((2, tok), F32),
        ),
        in_specs=specs,
        out_specs=(vmem, vmem),
        scratch_shapes=scratch,
        compiler_params=pltpu.CompilerParams(
            collective_id=0, has_side_effects=True, vmem_limit_bytes=58 * 1024 * 1024
        ),
        name="layer",
    )(*ops)


def solution(mesh):
    in_specs = (
        P(("sp", "tp"), None),
        P(),
        P(None, "tp"),
        P(None, "tp"),
        P(None, "tp"),
        P(None, "tp"),
        P(None, "tp"),
        P(None, "tp"),
        P("tp"),
        P("tp", None),
        P("tp", None),
        P("tp", None),
    )
    out_specs = (P(("sp", "tp"), None), P("tp", "sp"))
    return jax.shard_map(
        per_device, mesh=mesh, in_specs=in_specs, out_specs=out_specs, check_vma=False
    )
```
